32 devices in a mesh: sp: 4 (over y, x), tp: 8 (over z, core).
Axes of the slice: x: 2, y: 2, z: 4, core: 2. Of those that a mesh axis runs over, the one named last changes fastest.
Arguments:
- upstream: bfloat16 [1024, 4096], P('sp', 'tp'), may hold values from -6 to 6
- stream: bfloat16 [1024, 4096], P('sp', 'tp'), may hold values from -400 to 400
- norm_gain: float32 [4096], P('tp'), may hold values from 0.1 to 1.9
- routes: int32 [1024, 2], P('sp'), may hold values from 0 to 3, all different within a row; in each aligned block of 256 rows (0 to 255, 256 to 511, ...) at most 192 rows name the same one
- route_weights: float32 [1024, 2], P('sp'), may hold values from 0.1 to 1
- w_gate: bfloat16 [4, 4096, 2048], P('sp', None, 'tp'), may hold values from -0.09375 to 0.09375
- w_up: bfloat16 [4, 4096, 2048], P('sp', None, 'tp'), may hold values from -0.09375 to 0.09375
- w_down: bfloat16 [4, 2048, 4096], P('sp', 'tp'), may hold values from -0.125 to 0.125
- value_in: bfloat16 [1024, 2048], P('sp', 'tp'), may hold values from -6 to 6
- gate_in: bfloat16 [1024, 2048], P('sp', 'tp'), may hold values from -6 to 6
- conv_pre: bfloat16 [1024, 2048], P('sp', 'tp'), may hold values from -200 to 200
- ln_gain: float32 [2048], P('tp'), may hold values from 0.1 to 1.9
- conv_taps: float32 [31, 2048], P(None, 'tp'), may hold values from -1 to 1
- w_out: bfloat16 [2048, 4096], P('tp'), may hold values from -0.125 to 0.125
Outputs:
- grad_gate: float32 [4, 4096, 2048], P('sp', None, 'tp')
- grad_up: float32 [4, 4096, 2048], P('sp', None, 'tp')
- grad_down: float32 [4, 2048, 4096], P('sp', 'tp')
- grad_out: float32 [2048, 4096], P('tp', 'sp')
- value_grad: bfloat16 [1024, 2048], P('sp', 'tp')
- gate_grad: bfloat16 [1024, 2048], P('sp', 'tp')
The draws below stay inside these ranges and needn't reach their ends.
Inputs may be any that keep to these rules, and one draw needn't show every extreme that they name: `routes`: each token names two different experts. Among the tokens of one index of sp no expert is named more than 192 times, and in every draw some expert exactly 192 times.
All inputs are finite; a program needn't handle non-finite values.
Results may differ from the reference program's by a relative error of at most 0.0071.
Values may be sent and summed in bfloat16 or wider, within the bound.
A program may use at most 128 MiB of HBM per device.

```python
import math
import jax
import jax.numpy as jnp
import numpy as np
from jax import lax

D = 4096
C = 2048
FF = 2048
TAPS = 31
TOK_DEV = 256
TOKENS = 1024
EXPERTS = 4
CAP = 192
N_SP = 4


def draw_stream(key, part):
    subkeys = jax.random.split(jax.random.fold_in(key, 11), 3)
    random_part = jnp.clip(jax.random.normal(subkeys[0], (TOKENS, D), jnp.float32), -6.0, 6.0)
    row_scale = jnp.exp(jax.random.uniform(subkeys[1], (TOKENS, 1), jnp.float32, 0.0, math.log(10.0)))
    rising = jnp.exp(math.log(10.0) * (jnp.arange(D, dtype=jnp.float32) + 0.5) / D)
    jitter = jnp.exp(jax.random.uniform(subkeys[2], (D,), jnp.float32, -0.3, 0.3))
    column_scale = rising * jitter
    return (random_part * row_scale * column_scale[None, :] / 3.0).astype(jnp.bfloat16)


def draw_conv_pre(key, part):
    subkeys = jax.random.split(jax.random.fold_in(key, 23), 4)
    random_part = jnp.clip(jax.random.normal(subkeys[0], (TOKENS, C), jnp.float32), -6.0, 6.0)
    row_scale = jnp.exp(jax.random.uniform(subkeys[1], (TOKENS, 1), jnp.float32, 0.0, math.log(4.0)))
    rising = jnp.exp(math.log(10.0) * (jnp.arange(C, dtype=jnp.float32) + 0.5) / C)
    jitter = jnp.exp(jax.random.uniform(subkeys[2], (C,), jnp.float32, -0.3, 0.3))
    column_scale = rising * jitter
    row_offset = 1.5 * jnp.clip(jax.random.normal(subkeys[3], (TOKENS, 1), jnp.float32), -3.0, 3.0)
    return ((random_part * column_scale[None, :] / 3.0 + row_offset) * row_scale).astype(jnp.bfloat16)


def with_spikes(entries, rng, source, target, blocks, factor):
    def block_of(position):
        return (jnp.arange(entries.shape[position]) // (entries.shape[position] // blocks)).reshape((-1,) + (1,) * (entries.ndim - 1 - position))

    first = jax.random.permutation(rng, blocks)[block_of(target)]
    other_side = (block_of(target) + blocks // 2) % blocks
    return jnp.where((block_of(source) == first) | (block_of(source) == other_side), factor * entries, entries)


def block_levels(own_key, dims, pieces, low, top_value):
    def one(position, blocks):
        draws = jax.random.uniform(jax.random.fold_in(jax.random.fold_in(own_key, 6), position), (blocks,), jnp.float32, low / len(pieces), top_value / len(pieces))
        return jnp.repeat(jnp.exp(draws), dims[position] // blocks).reshape((-1,) + (1,) * (len(dims) - position - 1))

    gain = one(*pieces[0])
    for cut in pieces[1:]:
        gain = gain * one(*cut)
    return gain


def assign_block(key, own, number, rows, count, top, reach, slope):
    sequence = jax.random.permutation(key, count)
    packed, common = shares(count, rows * top, reach, slope, True), shares(count, rows * top, reach, slope, False)
    places = jnp.arange(count)

    def named(sizes, turn):
        used = int((sizes > 0).sum())
        fixed = max(1, used // 4)
        shifted = fixed + (places - fixed + turn * (used - fixed)) % max(1, count - fixed)
        return jnp.zeros((count,), jnp.int32).at[sequence[jnp.where(places < fixed, places, shifted)]].set(jnp.asarray(sizes, jnp.int32))

    sizes = jnp.where(number % 4 == 0, named(packed, number // 4), named(common, number - number // 4 - 1))
    mixed = jax.random.permutation(jax.random.fold_in(own, 3), count)
    source_of, receiver = mixed[0:count // 2 * 2:2], mixed[1:count // 2 * 2:2]
    room = jnp.minimum(sizes[source_of] - 1, reach - sizes[receiver]) // 2
    room = jnp.where((source_of == sequence[0]) | (receiver == sequence[0]) | (sizes[receiver] == 0), 0, jnp.maximum(room, 0))
    shifted = jax.random.randint(jax.random.fold_in(own, 4), (count // 2,), 0, 1 << 20) % (room + 1)
    sizes = sizes.at[source_of].add(-shifted).at[receiver].add(shifted)
    labels = jnp.searchsorted(jnp.cumsum(sizes), jnp.arange(rows * top), side="right").astype(jnp.int32)
    listing = labels.reshape(top, rows).T
    listing = listing[jax.random.permutation(jax.random.fold_in(own, 1), rows)]
    turn = jax.random.randint(jax.random.fold_in(own, 2), (rows, 1), 0, top)
    return jnp.take_along_axis(listing, (jnp.arange(top)[None, :] + turn) % top, axis=1)


def shares(number_of, total, reach, lean, full):
    loads = [(1 << 20) // math.isqrt(grade ** lean) + 1 for grade in range(1, number_of + 1)]
    largest = reach if full else min(reach, max(-(-total // number_of), total * loads[0] // sum(loads)))
    least = 1 if total - largest >= number_of - 1 else 0
    holding, rest = [largest] + [least] * (number_of - 1), total - largest - least * (number_of - 1)
    while rest > 0:
        candidates = [i for i in range(1, number_of) if holding[i] < largest] or [i for i in range(1, number_of) if holding[i] < reach]
        whole, left = sum([loads[i] for i in candidates]), rest
        for i in candidates:
            addition = min(reach - holding[i], max(1, left * loads[i] // whole), rest)
            holding[i] = holding[i] + addition
            rest = rest - addition
    return np.array(holding)


def scatter_about(own_key, extent, width, limit, pieces=(), kind=jnp.bfloat16):
    values = jax.random.normal(own_key, extent, jnp.float32) * width
    if len(pieces) > 0:
        values = block_levels(own_key, extent, pieces, -0.22, 0.18) * values
    return jnp.clip(values, min=-limit, max=limit).astype(kind)


def bell_draw_with(own_key, extent, scale, most, cuts, heavy, held_as=jnp.bfloat16):
    drawn = scale * jax.random.normal(own_key, extent, jnp.float32)
    if cuts:
        drawn = drawn * block_levels(own_key, extent, cuts, -0.22, 0.18)
    return jnp.clip(with_spikes(drawn, jax.random.fold_in(own_key, 3), *heavy), -most, most).astype(held_as)


def setup_inputs(seed: int = 0) -> dict:
    splits = jax.random.split(jax.random.key(seed), 15)
    upstream = bell_draw_with(splits[0], (TOKENS, D), 1.0, 6.0, ((0, 4), (1, 8)), (0, 1, 8, 2.0))
    stream = draw_stream(jax.random.fold_in(splits[14], 71), 0)
    norm_gain = jnp.clip(1.0 + 0.18 * jax.random.normal(splits[2], (D,), jnp.float32), 0.1, 1.9)
    routes_keys = jax.random.split(jax.random.fold_in(splits[3], 1), TOKENS // TOK_DEV)
    routes_turns = jax.random.permutation(jax.random.fold_in(splits[3], 3), TOKENS // TOK_DEV)
    routes = jax.vmap(lambda own, number: assign_block(jax.random.fold_in(splits[3], 2), own, number, TOK_DEV, EXPERTS, 2, CAP, 1))(routes_keys, routes_turns).reshape((TOKENS, 2))
    route_weights = jnp.clip(jnp.exp(math.log(1.0) - 2.3025851 * jax.random.uniform(splits[4], (TOKENS, 2), jnp.float32) ** block_levels(splits[4], (TOKENS, 2), ((0, 4),), -0.2, 0.2)), 0.1, 1.0)
    w_gate = scatter_about(splits[5], (EXPERTS, D, FF), D ** -0.5, 0.09375, ((0, 4), (2, 8)))
    w_up = scatter_about(splits[6], (EXPERTS, D, FF), D ** -0.5, 0.09375, ((0, 4), (2, 8)))
    w_down = scatter_about(splits[7], (EXPERTS, FF, D), FF ** -0.5, 0.125, ((0, 4), (1, 8)))
    value_in = scatter_about(splits[8], (TOKENS, C), 1.0, 6.0, ((0, 4), (1, 8)))
    gate_in = scatter_about(splits[9], (TOKENS, C), 1.5, 6.0, ((0, 4), (1, 8)))
    conv_pre = draw_conv_pre(jax.random.fold_in(splits[14], 71), 0)
    ln_gain = jnp.clip(1.0 + 0.18 * jax.random.normal(splits[11], (C,), jnp.float32), 0.1, 1.9)
    conv_taps = scatter_about(splits[12], (TAPS, C), TAPS ** -0.5, 1.0, ((1, 8),), jnp.float32)
    w_out = scatter_about(splits[13], (C, D), C ** -0.5, 0.125, ((0, 8),))
    return dict(upstream=upstream, stream=stream, norm_gain=norm_gain, routes=routes, route_weights=route_weights, w_gate=w_gate, w_up=w_up, w_down=w_down, value_in=value_in, gate_in=gate_in, conv_pre=conv_pre, ln_gain=ln_gain, conv_taps=conv_taps, w_out=w_out)


EPSILON = 1e-06

def silu_slope(values):
    logistic = jax.nn.sigmoid(values)
    return logistic * (1.0 + values * (1.0 - logistic))

def reference(upstream, stream, norm_gain, routes, route_weights, w_gate, w_up, w_down, value_in, gate_in, conv_pre, ln_gain, conv_taps, w_out):
    tokens, model_width = stream.shape
    experts = w_gate.shape[0]
    channels = conv_pre.shape[1]
    tap_count = conv_taps.shape[0]
    capacity = 3 * TOK_DEV // N_SP
    expert_rows = N_SP * capacity
    residual = stream.astype(jnp.float32)
    inverse = lax.rsqrt(lax.optimization_barrier(jnp.mean(residual * residual, axis=1, keepdims=True)) + EPSILON)
    normed = (norm_gain[None, :] * residual * inverse).astype(jnp.bfloat16)
    flat_experts = routes.reshape(-1)
    one_hot = (flat_experts[:, None] == jnp.arange(experts, dtype=jnp.int32)[None, :]).astype(jnp.int32)
    blocked = one_hot.reshape(N_SP, 2 * TOK_DEV, experts)
    earlier = (jnp.cumsum(blocked, axis=1) - blocked) * blocked
    slot_rank = lax.optimization_barrier(jnp.sum(earlier, axis=2)).reshape(-1)
    source = jnp.arange(2 * tokens, dtype=jnp.int32) // (2 * TOK_DEV)
    slot_index = flat_experts * expert_rows + source * capacity + slot_rank
    token_of = jnp.full((experts * expert_rows,), tokens, jnp.int32).at[slot_index].set(jnp.arange(2 * tokens, dtype=jnp.int32) // 2)
    weight_of = jnp.zeros((experts * expert_rows,), jnp.float32).at[slot_index].set(route_weights.reshape(-1))
    normed_pad = jnp.concatenate([normed, jnp.zeros((1, model_width), jnp.bfloat16)], axis=0)
    upstream_pad = jnp.concatenate([upstream, jnp.zeros((1, model_width), jnp.bfloat16)], axis=0)

    def one_expert(operands):
        indices, weights, gate_mat, upper_mat, down_mat = operands
        inputs = normed_pad[indices]
        cotangent = (weights[:, None] * upstream_pad[indices].astype(jnp.float32)).astype(jnp.bfloat16)
        gate_pre = jnp.dot(inputs, gate_mat, preferred_element_type=jnp.float32)
        upper_pre = jnp.dot(inputs, upper_mat, preferred_element_type=jnp.float32)
        active = (jax.nn.silu(gate_pre) * upper_pre).astype(jnp.bfloat16)
        active_back = jnp.dot(cotangent, down_mat.T, preferred_element_type=jnp.float32)
        gate_back = (active_back * upper_pre * silu_slope(gate_pre)).astype(jnp.bfloat16)
        upper_back = (active_back * jax.nn.silu(gate_pre)).astype(jnp.bfloat16)
        grad_gate = jnp.dot(inputs.T, gate_back, preferred_element_type=jnp.float32)
        grad_up = jnp.dot(inputs.T, upper_back, preferred_element_type=jnp.float32)
        grad_down = jnp.dot(active.T, cotangent, preferred_element_type=jnp.float32)
        input_back = (jnp.dot(gate_back, gate_mat.T, preferred_element_type=jnp.float32) + jnp.dot(upper_back, upper_mat.T, preferred_element_type=jnp.float32)).astype(jnp.bfloat16)
        return (grad_gate, grad_up, grad_down, input_back)
    grad_gate, grad_up, grad_down, input_back = lax.map(one_expert, (token_of.reshape(experts, expert_rows), weight_of.reshape(experts, expert_rows), w_gate, w_up, w_down))
    token_back = jnp.zeros((tokens + 1, model_width), jnp.float32).at[token_of].add(input_back.reshape(-1, model_width).astype(jnp.float32))[:tokens]
    gained = norm_gain[None, :] * token_back
    inner_sum = lax.optimization_barrier(jnp.sum(gained * residual, axis=1, keepdims=True))
    norm_back = inverse * gained - residual * inverse ** 3 * inner_sum / model_width
    stream_grad = (upstream.astype(jnp.float32) + norm_back).astype(jnp.bfloat16)
    conv_vals = conv_pre.astype(jnp.float32)
    mean_val = lax.optimization_barrier(jnp.mean(conv_vals, axis=1, keepdims=True))
    variance = lax.optimization_barrier(jnp.mean(conv_vals * conv_vals, axis=1, keepdims=True)) - mean_val * mean_val
    inv_std = lax.rsqrt(variance + EPSILON)
    centred = (conv_vals - mean_val) * inv_std
    scaled = centred * ln_gain[None, :]
    mixed_out = jax.nn.silu(scaled).astype(jnp.bfloat16)
    grad_out = jnp.dot(mixed_out.T, stream_grad, preferred_element_type=jnp.float32)
    mixed_back = jnp.dot(stream_grad, w_out.T, preferred_element_type=jnp.float32)
    norm_in = mixed_back * silu_slope(scaled) * ln_gain[None, :]
    conv_back = inv_std * (norm_in - lax.optimization_barrier(jnp.mean(norm_in, axis=1, keepdims=True)) - centred * lax.optimization_barrier(jnp.mean(norm_in * centred, axis=1, keepdims=True)))
    padded = jnp.concatenate([conv_back, jnp.zeros((tap_count - 1, channels), jnp.float32)], axis=0)
    glu_back = jnp.zeros((tokens, channels), jnp.float32)
    for tap_index in range(tap_count):
        offset = tap_count - 1 - tap_index
        glu_back = glu_back + conv_taps[tap_index][None, :] * padded[offset:offset + tokens]
    gate_sigma = jax.nn.sigmoid(gate_in.astype(jnp.float32))
    value_grad = (glu_back * gate_sigma).astype(jnp.bfloat16)
    gate_grad = (glu_back * value_in.astype(jnp.float32) * gate_sigma * (1.0 - gate_sigma)).astype(jnp.bfloat16)
    return (grad_gate, grad_up, grad_down, grad_out, value_grad, gate_grad)
```

```python
import functools

import jax
import jax.numpy as jnp
from jax import lax
from jax.experimental import pallas as pl
from jax.experimental.pallas import tpu as pltpu
from jax.sharding import PartitionSpec as P


EPSILON = 1e-06
VMEM_LIMIT = 60 * 2**20


def shifted(block, axis, distance):
    devices = range(lax.axis_size(axis))
    route = [(i - distance, i) for i in devices if i - distance in devices]
    return lax.ppermute(block, axis, route)


def group_sum_kernel(axis, group, own_ref, out_ref, landed, send_sems, recv_sems):
    me = lax.axis_index(axis)
    barrier = pltpu.get_barrier_semaphore()
    for step in range(1, group):
        pl.semaphore_signal(
            barrier,
            inc=1,
            device_id={axis: lax.rem(me + step, group)},
            device_id_type=pl.DeviceIdType.MESH,
        )
    pl.semaphore_wait(barrier, group - 1)
    copies = []
    for step in range(1, group):
        copy = pltpu.make_async_remote_copy(
            src_ref=own_ref,
            dst_ref=landed.at[step - 1],
            send_sem=send_sems.at[step - 1],
            recv_sem=recv_sems.at[step - 1],
            device_id={axis: lax.rem(me + step, group)},
            device_id_type=pl.DeviceIdType.MESH,
        )
        copy.start()
        copies.append(copy)
    for copy in copies:
        copy.wait()
    total = own_ref[...]
    for step in range(1, group):
        total = total + landed[step - 1]
    out_ref[...] = total


def group_sum(vectors, axis, collective_id):
    block = jnp.stack(vectors, axis=0)
    group = lax.axis_size(axis)
    summed = pl.pallas_call(
        functools.partial(group_sum_kernel, axis, group),
        out_shape=jax.ShapeDtypeStruct(block.shape, block.dtype),
        in_specs=[pl.BlockSpec(memory_space=pltpu.VMEM)],
        out_specs=pl.BlockSpec(memory_space=pltpu.VMEM),
        scratch_shapes=[
            pltpu.VMEM((group - 1,) + block.shape, block.dtype),
            pltpu.SemaphoreType.DMA((group - 1,)),
            pltpu.SemaphoreType.DMA((group - 1,)),
        ],
        compiler_params=pltpu.CompilerParams(
            collective_id=collective_id, has_side_effects=True
        ),
        cost_estimate=pl.CostEstimate(
            flops=group * block.size, bytes_accessed=400 * block.size * 4, transcendentals=0
        ),
        name="group_sum",
    )(block)
    return tuple(summed[row] for row in range(len(vectors)))


def silu_slope(values):
    logistic = jax.nn.sigmoid(values)
    return logistic * (1.0 + values * (1.0 - logistic))


def per_device(
    upstream,
    stream,
    norm_gain,
    routes,
    route_weights,
    w_gate,
    w_up,
    w_down,
    value_in,
    gate_in,
    conv_pre,
    ln_gain,
    conv_taps,
    w_out,
):
    tok_rows, width_part = stream.shape
    token_groups = lax.axis_size("sp")
    width_groups = lax.axis_size("tp")
    model_width = width_part * width_groups
    channels = conv_pre.shape[1] * width_groups
    tap_count = conv_taps.shape[0]
    capacity = 3 * tok_rows // token_groups
    experts = w_gate.shape[0] * token_groups
    slot_count = experts * capacity
    expert_rows = token_groups * capacity
    flat_experts = routes.reshape(-1)
    one_hot = (flat_experts[:, None] == jnp.arange(experts, dtype=jnp.int32)[None, :]).astype(
        jnp.int32
    )
    slot_rank = jnp.sum((jnp.cumsum(one_hot, axis=0) - one_hot) * one_hot, axis=1)
    slot_index = (flat_experts * capacity + slot_rank).reshape(tok_rows, 2)
    slot_ids = jnp.arange(slot_count, dtype=jnp.int32)[:, None]
    first_hit = slot_ids == slot_index[None, :, 0]
    second_hit = slot_ids == slot_index[None, :, 1]
    any_hit = jnp.logical_or(first_hit, second_hit)
    picker = any_hit.astype(jnp.bfloat16)
    slot_weight = jnp.sum(
        jnp.where(first_hit, route_weights[None, :, 0], 0.0)
        + jnp.where(second_hit, route_weights[None, :, 1], 0.0),
        axis=1,
    )
    token_iota = jnp.arange(tok_rows, dtype=jnp.int32)[None, :]
    slot_token = jnp.where(
        jnp.any(any_hit, axis=1), jnp.sum(jnp.where(any_hit, token_iota, 0), axis=1), tok_rows
    )
    columns = stream.shape[1]
    spare = jnp.zeros((1, columns), jnp.bfloat16)
    upstream_pad = jnp.concatenate([upstream, spare], axis=0)
    cotangent = (upstream_pad[slot_token].astype(jnp.float32) * slot_weight[:, None]).astype(
        jnp.bfloat16
    )
    sent_cotangent = cotangent.reshape(experts, capacity, columns)
    part_cotangent = lax.all_to_all(
        sent_cotangent, "sp", split_axis=0, concat_axis=0, tiled=True
    ).reshape(expert_rows, width_part)
    part_cotangent, stream_late, conv_late = lax.optimization_barrier(
        (part_cotangent, stream, conv_pre)
    )
    cotangent = lax.all_gather(part_cotangent, "tp", axis=1, tiled=True)
    residual = stream_late.astype(jnp.float32)
    conv_vals = conv_late.astype(jnp.float32)
    row_squares, conv_total, conv_squares = group_sum(
        (
            jnp.sum(residual * residual, axis=1),
            jnp.sum(conv_vals, axis=1),
            jnp.sum(conv_vals * conv_vals, axis=1),
        ),
        "tp",
        0,
    )
    inverse = lax.rsqrt(row_squares / model_width + EPSILON)[:, None]
    normed = (norm_gain[None, :] * residual * inverse).astype(jnp.bfloat16)
    normed_pad = jnp.concatenate([normed, spare], axis=0)
    inputs = normed_pad[slot_token]
    sent_inputs = inputs.reshape(experts, capacity, columns)
    part_inputs = lax.all_to_all(sent_inputs, "sp", split_axis=0, concat_axis=0, tiled=True)
    inputs = lax.all_gather(
        part_inputs.reshape(expert_rows, width_part), "tp", axis=1, tiled=True
    )
    gate_mat = w_gate[0]
    upper_mat = w_up[0]
    down_mat = w_down[0]
    gate_pre = jnp.dot(inputs, gate_mat, preferred_element_type=jnp.float32)
    upper_pre = jnp.dot(inputs, upper_mat, preferred_element_type=jnp.float32)
    active = (jax.nn.silu(gate_pre) * upper_pre).astype(jnp.bfloat16)
    active_back = lax.dot_general(
        cotangent, down_mat, (((1,), (1,)), ((), ())), preferred_element_type=jnp.float32
    )
    gate_back = (active_back * upper_pre * silu_slope(gate_pre)).astype(jnp.bfloat16)
    upper_back = (active_back * jax.nn.silu(gate_pre)).astype(jnp.bfloat16)
    grad_gate = lax.dot_general(
        inputs, gate_back, (((0,), (0,)), ((), ())), preferred_element_type=jnp.float32
    )
    grad_up = lax.dot_general(
        inputs, upper_back, (((0,), (0,)), ((), ())), preferred_element_type=jnp.float32
    )
    grad_down = lax.dot_general(
        active, cotangent, (((0,), (0,)), ((), ())), preferred_element_type=jnp.float32
    )
    input_part = lax.dot_general(
        gate_back, gate_mat, (((1,), (1,)), ((), ())), preferred_element_type=jnp.float32
    ) + lax.dot_general(
        upper_back, upper_mat, (((1,), (1,)), ((), ())), preferred_element_type=jnp.float32
    )
    input_back = lax.psum_scatter(
        input_part.astype(jnp.bfloat16), "tp", scatter_dimension=1, tiled=True
    )
    input_back, grad_gate, grad_up, grad_down = lax.optimization_barrier(
        (input_back, grad_gate, grad_up, grad_down)
    )
    returned = lax.all_to_all(
        input_back.reshape(token_groups, capacity, width_part),
        "sp",
        split_axis=0,
        concat_axis=0,
        tiled=True,
    )
    returned = returned.reshape(slot_count, width_part)
    token_back = lax.dot_general(
        picker, returned, (((0,), (0,)), ((), ())), preferred_element_type=jnp.float32
    )
    gained = norm_gain[None, :] * token_back
    (inner_sum,) = group_sum((jnp.sum(gained * residual, axis=1),), "tp", 1)
    norm_back = inverse * gained - residual * inverse**3 * (inner_sum / model_width)[:, None]
    stream_grad = (upstream.astype(jnp.float32) + norm_back).astype(jnp.bfloat16)
    full_grad = lax.all_gather(stream_grad, "tp", axis=1, tiled=True)
    mean_val = (conv_total / channels)[:, None]
    variance = (conv_squares / channels)[:, None] - mean_val * mean_val
    inv_std = lax.rsqrt(variance + EPSILON)
    centred = (conv_vals - mean_val) * inv_std
    scaled = centred * ln_gain[None, :]
    mixed_out = jax.nn.silu(scaled).astype(jnp.bfloat16)
    grad_rows = lax.dot_general(
        full_grad, mixed_out, (((0,), (0,)), ((), ())), preferred_element_type=jnp.float32
    ).astype(jnp.bfloat16)
    grad_out = (
        lax.psum_scatter(grad_rows, "sp", scatter_dimension=0, tiled=True).astype(jnp.float32).T
    )
    mixed_back = lax.dot_general(
        full_grad, w_out, (((1,), (1,)), ((), ())), preferred_element_type=jnp.float32
    )
    norm_in = mixed_back * silu_slope(scaled) * ln_gain[None, :]
    norm_total, norm_cross = group_sum(
        (jnp.sum(norm_in, axis=1), jnp.sum(norm_in * centred, axis=1)), "tp", 2
    )
    conv_back = inv_std * (
        norm_in - (norm_total / channels)[:, None] - centred * (norm_cross / channels)[:, None]
    )
    next_rim = shifted(conv_back[: tap_count - 1], "sp", -1)
    padded = jnp.concatenate([conv_back, next_rim], axis=0)
    glu_back = jnp.zeros(conv_back.shape, jnp.float32)
    for tap_index in range(tap_count):
        offset = tap_count - 1 - tap_index
        glu_back = glu_back + conv_taps[tap_index][None, :] * padded[offset : offset + tok_rows]
    gate_sigma = jax.nn.sigmoid(gate_in.astype(jnp.float32))
    value_grad = (glu_back * gate_sigma).astype(jnp.bfloat16)
    gate_grad = (glu_back * value_in.astype(jnp.float32) * gate_sigma * (1.0 - gate_sigma)).astype(
        jnp.bfloat16
    )
    return (grad_gate[None], grad_up[None], grad_down[None], grad_out, value_grad, gate_grad)


MESH_ID = pl.DeviceIdType.MESH


def remote(src, dst, send_sem, recv_sem, sp_index, tp_index):
    return pltpu.make_async_remote_copy(
        src_ref=src,
        dst_ref=dst,
        send_sem=send_sem,
        recv_sem=recv_sem,
        device_id={"sp": sp_index, "tp": tp_index},
        device_id_type=MESH_ID,
    )


def greet(devices):
    barrier = pltpu.get_barrier_semaphore()
    for sp_index, tp_index in devices:
        pl.semaphore_signal(
            barrier,
            inc=1,
            device_id={"sp": sp_index, "tp": tp_index},
            device_id_type=MESH_ID,
        )
    pl.semaphore_wait(barrier, len(devices))


def places():
    sp = lax.axis_index("sp")
    tp = lax.axis_index("tp")
    chip, core = tp // 2, tp % 2
    side = 1 - 2 * (sp % 2)
    lift = 2 - 4 * (sp // 2)
    across, along = sp + side, sp + lift
    corner = 3 - sp
    hops = (
        chip,
        chip + 1 - 2 * (chip % 2),
        chip + 2 - 4 * (chip // 2),
        3 - chip,
    )
    return sp, tp, chip, core, across, along, corner, hops


def to_column(row):
    count = row.shape[1]
    down = lax.broadcasted_iota(jnp.int32, (count, count), 0)
    over = lax.broadcasted_iota(jnp.int32, (count, count), 1)
    return jnp.sum(jnp.where(down == over, row, 0.0), axis=1, keepdims=True)


def to_row(column):
    count = column.shape[0]
    down = lax.broadcasted_iota(jnp.int32, (count, count), 0)
    over = lax.broadcasted_iota(jnp.int32, (count, count), 1)
    return jnp.sum(jnp.where(down == over, column, 0.0), axis=0, keepdims=True)


def dot_nt(left, right):
    return lax.dot_general(
        left, right, (((1,), (1,)), ((), ())), preferred_element_type=jnp.float32
    )


def dot_tn(left, right):
    return lax.dot_general(
        left, right, (((0,), (0,)), ((), ())), preferred_element_type=jnp.float32
    )


def expert_kernel(
    width,
    gs_ref,
    up_ref,
    stat_ref,
    wrow_ref,
    wg_hbm,
    wu_hbm,
    wd_hbm,
    rows_s,
    rows_u,
    hidden,
    active,
    keep,
    send_x,
    send_y,
    stat_out,
    wgu,
    wd,
    mate_w,
    mate_h,
    acc,
    back,
    stat_in,
    inv_out,
    inv_in,
    w_in,
    z_send,
    piece_recv,
    xy_send,
    relay_send,
    mate_send,
    mate_recv,
    stat_send,
    stat_recv,
    inv_send,
    inv_recv,
    w_send,
    w_recv,
    mw_sems,
    mh_send,
    mh_recv,
    local_sems,
):
    sp, tp, chip, core, across, along, corner, hops = places()
    mate = tp + 1 - 2 * core
    tokens, columns = gs_ref.shape
    part = wd_hbm.shape[0]
    tp_count = 8
    peers = [lax.rem(tp + step, tp_count) for step in range(1, tp_count)]
    others = (across, along, corner)
    owns = (gs_ref, up_ref)
    rows = (rows_s, rows_u)

    loads = [
        pltpu.make_async_copy(wg_hbm, wgu.at[:, :, :, pl.ds(0, part)], local_sems.at[0]),
        pltpu.make_async_copy(wu_hbm, wgu.at[:, :, :, pl.ds(part, part)], local_sems.at[1]),
        pltpu.make_async_copy(wd_hbm, wd, local_sems.at[2]),
        pltpu.make_async_copy(gs_ref, rows_s.at[sp, core, chip], local_sems.at[3]),
        pltpu.make_async_copy(up_ref, rows_u.at[sp, core, chip], local_sems.at[4]),
    ]
    for load in loads:
        load.start()
    greet([(sp, peer) for peer in peers] + [(other, tp) for other in others])

    pending = []

    def go(copy):
        copy.start()
        pending.append(copy)

    for i, peer in enumerate(peers):
        go(remote(stat_ref, stat_in.at[tp], stat_send.at[i], stat_recv.at[tp], sp, peer))
    for i, other in enumerate(others):
        go(remote(wrow_ref.at[other], w_in.at[sp], w_send.at[i], w_recv.at[sp], other, tp))

    def send_piece(kind, step, source):
        place = hops[step]
        for way, target in enumerate((across, along)):
            go(
                remote(
                    source,
                    rows[kind].at[sp, core, place],
                    xy_send.at[kind, step, way],
                    piece_recv.at[kind, sp, place],
                    target,
                    tp,
                )
            )

    for kind in (0, 1):
        for step in (1, 2, 3):
            go(
                remote(
                    owns[kind],
                    rows[kind].at[sp, core, chip],
                    z_send.at[kind, step - 1],
                    piece_recv.at[kind, sp, chip],
                    sp,
                    2 * hops[step] + core,
                )
            )
        send_piece(kind, 0, owns[kind])

    def await_piece(kind, origin, step):
        slot = rows[kind].at[origin, core, hops[step]]
        remote(
            slot,
            slot,
            mate_send.at[kind, origin],
            piece_recv.at[kind, origin, hops[step]],
            sp,
            mate,
        ).wait_recv()

    def relay(kind, step):
        origin, target = (across, along) if step % 2 == 0 else (along, across)
        await_piece(kind, origin, step)
        slot = rows[kind].at[origin, core, hops[step]]
        go(
            remote(
                slot,
                slot,
                relay_send.at[kind, step],
                piece_recv.at[kind, origin, hops[step]],
                target,
                tp,
            )
        )

    def share(kind, origin):
        slot = rows[kind].at[origin, core]
        go(
            remote(
                slot, slot, mate_send.at[kind, origin], mate_recv.at[kind, origin], sp, mate
            )
        )

    def await_share(kind, origin):
        slot = rows[kind].at[origin, 1 - core]
        remote(
            slot, slot, mate_send.at[kind, origin], mate_recv.at[kind, origin], sp, mate
        ).wait_recv()

    for load in loads:
        load.wait()
    go(
        remote(
            wgu.at[:, 1 - core], mate_w, mw_sems.at[0], mw_sems.at[1], sp, mate
        )
    )
    acc[...] = jnp.zeros(acc.shape, jnp.float32)
    back[...] = jnp.zeros(back.shape, jnp.float32)
    w_in[sp] = wrow_ref[sp]

    total = stat_ref[...]
    for peer in peers:
        remote(
            stat_in.at[peer], stat_in.at[peer], stat_send.at[0], stat_recv.at[peer], sp, peer
        ).wait_recv()
        total = total + stat_in[peer]
    stat_out[...] = total
    inverse_row = lax.rsqrt(total[0:1] / width + EPSILON)
    inv_out[...] = jnp.broadcast_to(inverse_row, inv_out.shape)
    inv_in[sp] = jnp.broadcast_to(inverse_row, inv_out.shape)
    for i, other in enumerate(others):
        go(remote(inv_out, inv_in.at[sp], inv_send.at[i], inv_recv.at[sp], other, tp))

    def forward(origin):
        def body(index, carry):
            half, place = index // 4, lax.rem(index, 4)
            acc[origin] += jnp.dot(
                rows_s[origin, half, place],
                wgu[place, half],
                preferred_element_type=jnp.float32,
            )
            return carry

        lax.fori_loop(0, tp_count, body, 0)

    def backward(origin, half):
        def body(place, carry):
            start = pl.multiple_of((2 * place + half) * columns, columns)
            back[origin] += dot_nt(rows_u[origin, half, place], wd[:, pl.ds(start, columns)])
            return carry

        lax.fori_loop(0, 4, body, 0)

    chunk = 64

    def activate(origin):
        inverse = to_column(inv_in[origin, 0:1])
        weight = to_column(w_in[origin, 0:1])
        for begin in range(0, tokens, chunk):
            end = begin + chunk
            pre = acc[origin, begin:end] * inverse[begin:end]
            gate, upper = pre[:, :part], pre[:, part:]
            cot = back[origin, begin:end] * weight[begin:end]
            logistic = 1.0 / (1.0 + jnp.exp(-gate))
            silu = gate * logistic
            slope = logistic * (1.0 + gate * (1.0 - logistic))
            active[origin, begin:end] = (silu * upper * weight[begin:end]).astype(jnp.bfloat16)
            back_inv = cot * inverse[begin:end]
            hidden[origin, begin:end, :part] = (back_inv * upper * slope).astype(jnp.bfloat16)
            hidden[origin, begin:end, part:] = (back_inv * silu).astype(jnp.bfloat16)
        go(
            remote(
                hidden.at[origin],
                mate_h.at[origin],
                mh_send.at[origin],
                mh_recv.at[origin],
                sp,
                mate,
            )
        )

    def spread(origin, low, high):
        remote(
            mate_h.at[origin],
            mate_h.at[origin],
            mh_send.at[origin],
            mh_recv.at[origin],
            sp,
            mate,
        ).wait_recv()

        for target, first in ((low, 0), (high, 2)):

            def body(i, carry, target=target, first=first):
                place = first + i
                part_sum = dot_nt(hidden[origin], wgu[place, core]) + dot_nt(
                    mate_h[origin], mate_w[place]
                )
                target[i] = part_sum.astype(jnp.bfloat16)
                return carry

            lax.fori_loop(0, 2, body, 0)

    def arrive(kind, step):
        await_piece(kind, sp, step)
        send_piece(kind, step, rows[kind].at[sp, core, hops[step]])

    arrive(0, 1)
    relay(0, 0)
    arrive(0, 2)
    relay(1, 0)
    arrive(0, 3)
    relay(0, 1)
    share(0, sp)
    arrive(1, 1)
    relay(0, 2)
    await_share(0, sp)
    forward(sp)
    arrive(1, 2)
    relay(0, 3)
    for step in (1, 3):
        await_piece(0, across, step)
    share(0, across)
    for step in (0, 2):
        await_piece(0, along, step)
    share(0, along)
    arrive(1, 3)
    relay(1, 1)
    share(1, sp)
    await_share(0, across)
    forward(across)
    await_share(0, along)
    forward(along)
    relay(1, 2)
    for step in (0, 1, 2, 3):
        await_piece(0, corner, step)
    share(0, corner)
    await_share(1, sp)
    backward(sp, 0)
    backward(sp, 1)
    await_share(0, corner)
    forward(corner)
    relay(1, 3)
    for other in others:
        for sems, landing in ((inv_recv, inv_in), (w_recv, w_in)):
            remote(
                landing.at[other], landing.at[other], inv_send.at[0], sems.at[other], sp, mate
            ).wait_recv()
    activate(sp)
    for step in (1, 3):
        await_piece(1, across, step)
    share(1, across)
    for step in (0, 2):
        await_piece(1, along, step)
    share(1, along)
    remote(mate_w, mate_w, mw_sems.at[0], mw_sems.at[1], sp, mate).wait_recv()
    await_share(1, across)
    backward(across, 0)
    backward(across, 1)
    activate(across)
    await_share(1, along)
    backward(along, 0)
    backward(along, 1)
    activate(along)
    row_of = sp // 2
    col_of = lax.rem(sp, 2)
    spread(sp, keep.at[0, row_of], keep.at[1, col_of])
    spread(across, send_x.at[row_of], keep.at[1, 1 - col_of])
    spread(along, keep.at[0, 1 - row_of], send_y.at[col_of])
    for step in (0, 1, 2, 3):
        await_piece(1, corner, step)
    share(1, corner)
    backward(corner, core)
    await_share(1, corner)
    backward(corner, 1 - core)
    activate(corner)
    spread(corner, send_x.at[1 - row_of], send_y.at[1 - col_of])
    for copy in pending:
        copy.wait_send()


def grads_kernel(rows_s, rows_u, hidden, active, gate_out, up_out, down_out, tall, wide, sems):
    columns = rows_s.shape[4]
    part = active.shape[2]
    pieces = 8

    def copies(piece, slot):
        span = pl.ds(pl.multiple_of(piece * columns, columns), columns)
        return (
            pltpu.make_async_copy(
                tall.at[slot, :, pl.ds(0, part)], gate_out.at[span], sems.at[slot, 0]
            ),
            pltpu.make_async_copy(
                tall.at[slot, :, pl.ds(part, part)], up_out.at[span], sems.at[slot, 1]
            ),
            pltpu.make_async_copy(wide.at[slot], down_out.at[:, span], sems.at[slot, 2]),
        )

    def body(piece, carry):
        slot = lax.rem(piece, 2)
        half, place = lax.rem(piece, 2), piece // 2

        @pl.when(piece >= 2)
        def _():
            for copy in copies(piece - 2, slot):
                copy.wait()

        for origin in range(4):
            tall_term = dot_tn(rows_s[origin, half, place], hidden[origin])
            wide_term = dot_tn(active[origin], rows_u[origin, half, place])
            if origin == 0:
                tall[slot] = tall_term
                wide[slot] = wide_term
            else:
                tall[slot] += tall_term
                wide[slot] += wide_term
        for copy in copies(piece, slot):
            copy.start()
        return carry

    lax.fori_loop(0, pieces, body, 0)
    for piece in (pieces - 2, pieces - 1):
        for copy in copies(piece, piece % 2):
            copy.wait()


def return_kernel(
    width,
    channels,
    keep,
    got_x,
    got_y,
    up_ref,
    stream_ref,
    gain_ref,
    inv_ref,
    mixed_ref,
    slope_ref,
    centred_ref,
    invstd_ref,
    w_hbm,
    conv_out,
    grads,
    mixed,
    w_out,
    turn_out,
    turn_in,
    z_out,
    z_in,
    own_sum,
    note_out,
    note_in,
    tail_out,
    tail_in,
    full,
    rim_in,
    mix_send,
    mix_recv,
    turn_send,
    turn_recv,
    z_send,
    z_recv,
    note_send,
    note_recv,
    tail_send,
    tail_recv,
    full_send,
    full_recv,
    mate_send,
    mate_recv,
    grad_send,
    grad_recv,
    gmate_send,
    gmate_recv,
    rim_sems,
    local_sems,
):
    sp, tp, chip, core, across, along, corner, hops = places()
    mate = tp + 1 - 2 * core
    tp_count = 8
    tokens, columns = up_ref.shape
    row_of = sp // 2
    col_of = lax.rem(sp, 2)
    peers = [lax.rem(tp + step, tp_count) for step in range(1, tp_count)]
    others = (across, along, corner)
    load = pltpu.make_async_copy(w_hbm, w_out, local_sems.at[0])
    load.start()
    own_mixed = pltpu.make_async_copy(mixed_ref, mixed.at[sp], local_sems.at[1])
    own_mixed.start()
    greet([(sp, peer) for peer in peers] + [(other, tp) for other in others])
    pending = []

    def go(copy):
        copy.start()
        pending.append(copy)

    turns = ((0, 1 - row_of, row_of, got_x, along), (1, 1 - col_of, col_of, got_y, across))
    for i in range(2):
        for group, far, near, got, target in turns:
            turn_out[group, i] = (
                keep[group, far, i].astype(jnp.float32) + got[far, i].astype(jnp.float32)
            ).astype(jnp.bfloat16)
            go(
                remote(
                    turn_out.at[group, i],
                    turn_in.at[group, i],
                    turn_send.at[group, i],
                    turn_recv.at[group, i],
                    target,
                    tp,
                )
            )
    for i, other in enumerate(others):
        go(remote(mixed_ref, mixed.at[sp], mix_send.at[i], mix_recv.at[sp], other, tp))
    for i in range(2):
        for group, far, near, got, target in turns:
            place = 2 * group + i
            remote(
                turn_in.at[group, i],
                turn_in.at[group, i],
                turn_send.at[group, i],
                turn_recv.at[group, i],
                target,
                tp,
            ).wait_recv()
            summed = (
                keep[group, near, i].astype(jnp.float32)
                + got[near, i].astype(jnp.float32)
                + turn_in[group, i].astype(jnp.float32)
            )

            @pl.when(chip == place)
            def _(summed=summed):
                own_sum[...] = summed

            @pl.when(chip != place)
            def _(summed=summed, place=place):
                z_out[place] = summed.astype(jnp.bfloat16)
                remote(
                    z_out.at[place],
                    z_in.at[chip],
                    z_send.at[place],
                    z_recv.at[chip],
                    sp,
                    2 * place + core,
                ).start()

    for step in (1, 2, 3):
        place = hops[step]
        remote(
            z_out.at[place], z_in.at[place], z_send.at[place], z_recv.at[place], sp, mate
        ).wait()

    gain = gain_ref[...]
    chunk = 64
    for begin in range(0, tokens, chunk):
        end = begin + chunk
        own_sum[begin:end] = gain * (
            own_sum[begin:end]
            + z_in[hops[1], begin:end].astype(jnp.float32)
            + z_in[hops[2], begin:end].astype(jnp.float32)
            + z_in[hops[3], begin:end].astype(jnp.float32)
        )
    inner = jnp.sum(own_sum[...] * stream_ref[...].astype(jnp.float32), axis=1, keepdims=True)
    inner_row = to_row(inner)
    note_out[...] = jnp.broadcast_to(inner_row, note_out.shape)
    for i, peer in enumerate(peers):
        go(remote(note_out, note_in.at[tp], note_send.at[i], note_recv.at[tp], sp, peer))
    for peer in peers:
        remote(
            note_in.at[peer], note_in.at[peer], note_send.at[0], note_recv.at[peer], sp, peer
        ).wait_recv()
        inner_row = inner_row + note_in[peer, 0:1]
    inverse = inv_ref[...]
    factor = inverse * inverse * to_column(inner_row) / width
    for begin in range(0, tokens, chunk):
        end = begin + chunk
        full[core, chip, begin:end] = (
            up_ref[begin:end].astype(jnp.float32)
            + own_sum[begin:end]
            - stream_ref[begin:end].astype(jnp.float32) * factor[begin:end]
        ).astype(jnp.bfloat16)
    slot = full.at[core, chip]
    for step in (1, 2, 3):
        go(
            remote(
                slot,
                slot,
                full_send.at[step - 1],
                full_recv.at[chip],
                sp,
                2 * hops[step] + core,
            )
        )

    def fan(step):
        place = hops[step]
        slot = full.at[core, place]
        if step > 0:
            remote(slot, slot, full_send.at[0], full_recv.at[place], sp, mate).wait_recv()
        remote(slot, slot, mate_send.at[place], mate_recv.at[place], sp, mate).start()

        @pl.when(place != sp)
        def _():
            remote(
                slot, grads.at[sp, core], grad_send.at[place], grad_recv.at[sp], place, tp
            ).start()

    load.wait()

    def mixed_term(half, place):
        start = pl.multiple_of((2 * place + half) * columns, columns)
        return dot_nt(full[half, place], w_out[:, pl.ds(start, columns)])

    mixed_back = None
    for step in range(4):
        fan(step)
        term = mixed_term(core, hops[step])
        mixed_back = term if mixed_back is None else mixed_back + term
    for step in range(4):
        place = hops[step]
        slot = full.at[1 - core, place]
        remote(slot, slot, mate_send.at[place], mate_recv.at[place], sp, mate).wait_recv()
        mixed_back = mixed_back + mixed_term(1 - core, place)
    norm_in = mixed_back * slope_ref[...]
    centred = centred_ref[...]
    sums = jnp.concatenate(
        [
            to_row(jnp.sum(norm_in, axis=1, keepdims=True)),
            to_row(jnp.sum(norm_in * centred, axis=1, keepdims=True)),
            jnp.zeros((6, tokens), jnp.float32),
        ],
        axis=0,
    )
    tail_out[...] = sums
    for i, peer in enumerate(peers):
        go(remote(tail_out, tail_in.at[tp], tail_send.at[i], tail_recv.at[tp], sp, peer))
    for peer in peers:
        remote(
            tail_in.at[peer], tail_in.at[peer], tail_send.at[0], tail_recv.at[peer], sp, peer
        ).wait_recv()
        sums = sums + tail_in[peer]
    conv_out[0:tokens] = invstd_ref[...] * (
        norm_in - to_column(sums[0:1]) / channels - centred * (to_column(sums[1:2]) / channels)
    )
    rim = rim_in.shape[0]
    before = lax.rem(sp + 3, 4)
    go(
        remote(
            conv_out.at[pl.ds(0, rim)], rim_in, rim_sems.at[0], rim_sems.at[1], before, tp
        )
    )
    for half in range(2):
        grads[sp, half] = full[half, sp]
    for other in others:
        slot = grads.at[other, core]
        remote(slot, slot, grad_send.at[0], grad_recv.at[other], other, tp).wait_recv()
        go(remote(slot, slot, gmate_send.at[other], gmate_recv.at[other], sp, mate))
    own_mixed.wait()
    for other in others:
        slot = mixed.at[other]
        remote(slot, slot, mix_send.at[0], mix_recv.at[other], other, tp).wait_recv()
    for other in others:
        slot = grads.at[other, 1 - core]
        remote(slot, slot, gmate_send.at[other], gmate_recv.at[other], sp, mate).wait_recv()
    remote(rim_in, rim_in, rim_sems.at[0], rim_sems.at[1], before, tp).wait_recv()
    last = (sp < 3).astype(jnp.float32)
    conv_out[tokens : tokens + rim] = rim_in[...] * last
    for step in range(4):
        place = hops[step]
        slot = full.at[core, place]
        remote(slot, slot, mate_send.at[place], mate_recv.at[place], sp, mate).wait_send()

        @pl.when(place != sp)
        def _(slot=slot, place=place):
            remote(
                slot, grads.at[sp, core], grad_send.at[place], grad_recv.at[sp], place, tp
            ).wait_send()

    for copy in pending:
        copy.wait_send()


def finish_kernel(conv, taps, value_in, gate_in, grads, mixed, grad_out, value_out, gate_out):
    tokens, part = value_in.shape
    tap_count = taps.shape[0]
    columns = grads.shape[3]
    for half in range(2):
        total = dot_tn(mixed[0], grads[0, half])
        for origin in range(1, 4):
            total = total + dot_tn(mixed[origin], grads[origin, half])
        grad_out[:, half * columns : (half + 1) * columns] = total
    glu = jnp.zeros((tokens, part), jnp.float32)
    for residue in range(8):
        rolled = None
        for offset in range(residue, tap_count, 8):
            base = offset - residue
            tap = taps[tap_count - 1 - offset : tap_count - offset]
            term = tap * conv[base : base + tokens + 8]
            rolled = term if rolled is None else rolled + term
        glu = glu + rolled[residue : residue + tokens]
    sigma = 1.0 / (1.0 + jnp.exp(-gate_in[...].astype(jnp.float32)))
    value_out[...] = (glu * sigma).astype(jnp.bfloat16)
    gate_out[...] = (
        glu * value_in[...].astype(jnp.float32) * sigma * (1.0 - sigma)
    ).astype(jnp.bfloat16)


def fused_device(
    upstream,
    stream,
    norm_gain,
    routes,
    route_weights,
    w_gate,
    w_up,
    w_down,
    value_in,
    gate_in,
    conv_pre,
    ln_gain,
    conv_taps,
    w_out,
):
    tokens, columns = stream.shape
    tp_count = lax.axis_size("tp")
    sp_count = lax.axis_size("sp")
    chips = tp_count // 2
    width = columns * tp_count
    part = w_gate.shape[2]
    channel_part = conv_pre.shape[1]
    channels = channel_part * tp_count
    bf16, f32 = jnp.bfloat16, jnp.float32
    vmem = pl.BlockSpec(memory_space=pltpu.VMEM)
    anywhere = pl.BlockSpec(memory_space=pl.ANY)
    dma = pltpu.SemaphoreType.DMA
    shape = jax.ShapeDtypeStruct

    residual = stream.astype(f32)
    scaled_stream = (norm_gain[None, :] * residual).astype(bf16)
    conv_vals = conv_pre.astype(f32)
    stats = jnp.stack(
        [
            jnp.sum(residual * residual, axis=1),
            jnp.sum(conv_vals, axis=1),
            jnp.sum(conv_vals * conv_vals, axis=1),
        ]
        + [jnp.zeros((tokens,), f32)] * 5,
        axis=0,
    )
    expert_ids = jnp.arange(sp_count, dtype=jnp.int32)
    weights = jnp.sum(
        jnp.where(routes[None] == expert_ids[:, None, None], route_weights[None], 0.0), axis=2
    )
    weight_rows = jnp.broadcast_to(weights[:, None, :], (sp_count, 8, tokens))
    piece = (chips, 2, columns, part)
    rows_shape = (sp_count, 2, chips, tokens, columns)
    outs = pl.pallas_call(
        functools.partial(expert_kernel, width),
        out_shape=(
            shape(rows_shape, bf16),
            shape(rows_shape, bf16),
            shape((sp_count, tokens, 2 * part), bf16),
            shape((sp_count, tokens, part), bf16),
            shape((2, 2, 2, tokens, columns), bf16),
            shape((2, 2, tokens, columns), bf16),
            shape((2, 2, tokens, columns), bf16),
            shape((8, tokens), f32),
        ),
        in_specs=[vmem, vmem, vmem, vmem, anywhere, anywhere, anywhere],
        out_specs=[vmem] * 8,
        scratch_shapes=[
            pltpu.VMEM((chips, 2, columns, 2 * part), bf16),
            pltpu.VMEM((part, width), bf16),
            pltpu.VMEM((chips, columns, 2 * part), bf16),
            pltpu.VMEM((sp_count, tokens, 2 * part), bf16),
            pltpu.VMEM((sp_count, tokens, 2 * part), f32),
            pltpu.VMEM((sp_count, tokens, part), f32),
            pltpu.VMEM((tp_count, 8, tokens), f32),
            pltpu.VMEM((8, tokens), f32),
            pltpu.VMEM((sp_count, 8, tokens), f32),
            pltpu.VMEM((sp_count, 8, tokens), f32),
            dma((2, 3)),
            dma((2, sp_count, chips)),
            dma((2, chips, 2)),
            dma((2, chips)),
            dma((2, sp_count)),
            dma((2, sp_count)),
            dma((tp_count - 1,)),
            dma((tp_count,)),
            dma((3,)),
            dma((sp_count,)),
            dma((3,)),
            dma((sp_count,)),
            dma((2,)),
            dma((sp_count,)),
            dma((sp_count,)),
            dma((5,)),
        ],
        compiler_params=pltpu.CompilerParams(
            collective_id=3, has_side_effects=True, vmem_limit_bytes=VMEM_LIMIT
        ),
        cost_estimate=pl.CostEstimate(
            flops=10**10, bytes_accessed=10**8, transcendentals=0
        ),
        name="expert_gather",
    )(
        scaled_stream,
        upstream,
        stats,
        weight_rows,
        w_gate[0].reshape(piece),
        w_up[0].reshape(piece),
        w_down[0],
    )
    rows_s, rows_u, hidden, active, keep, send_x, send_y, totals = outs

    def swap(block, step):
        route = [(i, i + step if (i // step) % 2 == 0 else i - step) for i in range(sp_count)]
        return lax.ppermute(block, "sp", route)

    got_x = swap(send_x, 1)
    got_y = swap(send_y, 2)

    grad_gate, grad_up, grad_down = pl.pallas_call(
        grads_kernel,
        out_shape=(shape((width, part), f32), shape((width, part), f32), shape((part, width), f32)),
        in_specs=[vmem] * 4,
        out_specs=[anywhere] * 3,
        scratch_shapes=[
            pltpu.VMEM((2, columns, 2 * part), f32),
            pltpu.VMEM((2, part, columns), f32),
            dma((2, 3)),
        ],
        compiler_params=pltpu.CompilerParams(vmem_limit_bytes=VMEM_LIMIT),
        cost_estimate=pl.CostEstimate(
            flops=6 * width * part * tokens * sp_count,
            bytes_accessed=40 * 2**20,
            transcendentals=0,
        ),
        name="weight_grads",
    )(rows_s, rows_u, hidden, active)

    inverse = lax.rsqrt(totals[0] / width + EPSILON)[:, None]
    mean_val = (totals[1] / channels)[:, None]
    variance = (totals[2] / channels)[:, None] - mean_val * mean_val
    inv_std = lax.rsqrt(variance + EPSILON)
    centred = (conv_vals - mean_val) * inv_std
    scaled = centred * ln_gain[None, :]
    mixed_out = jax.nn.silu(scaled).astype(bf16)
    slope = silu_slope(scaled) * ln_gain[None, :]
    rim = -(-(conv_taps.shape[0] - 1) // 8) * 8
    conv_back, grads, mixed = pl.pallas_call(
        functools.partial(return_kernel, width, channels),
        out_shape=(
            shape((tokens + rim, channel_part), f32),
            shape((sp_count, 2, tokens, columns), bf16),
            shape((sp_count, tokens, channel_part), bf16),
        ),
        in_specs=[vmem] * 11 + [anywhere],
        out_specs=[vmem] * 3,
        scratch_shapes=[
            pltpu.VMEM(w_out.shape, bf16),
            pltpu.VMEM((2, 2, tokens, columns), bf16),
            pltpu.VMEM((2, 2, tokens, columns), bf16),
            pltpu.VMEM((chips, tokens, columns), bf16),
            pltpu.VMEM((chips, tokens, columns), bf16),
            pltpu.VMEM((tokens, columns), f32),
            pltpu.VMEM((8, tokens), f32),
            pltpu.VMEM((tp_count, 8, tokens), f32),
            pltpu.VMEM((8, tokens), f32),
            pltpu.VMEM((tp_count, 8, tokens), f32),
            pltpu.VMEM((2, chips, tokens, columns), bf16),
            pltpu.VMEM((rim, channel_part), f32),
            dma((3,)),
            dma((sp_count,)),
            dma((2, 2)),
            dma((2, 2)),
            dma((chips,)),
            dma((chips,)),
            dma((tp_count - 1,)),
            dma((tp_count,)),
            dma((tp_count - 1,)),
            dma((tp_count,)),
            dma((3,)),
            dma((chips,)),
            dma((chips,)),
            dma((chips,)),
            dma((sp_count,)),
            dma((sp_count,)),
            dma((sp_count,)),
            dma((sp_count,)),
            dma((2,)),
            dma((2,)),
        ],
        compiler_params=pltpu.CompilerParams(
            collective_id=4, has_side_effects=True, vmem_limit_bytes=VMEM_LIMIT
        ),
        cost_estimate=pl.CostEstimate(
            flops=10**10, bytes_accessed=10**8, transcendentals=0
        ),
        name="return_path",
    )(
        keep,
        got_x,
        got_y,
        upstream,
        stream,
        norm_gain[None, :],
        inverse,
        mixed_out,
        slope,
        centred,
        inv_std,
        w_out,
    )
    grad_out, value_grad, gate_grad = pl.pallas_call(
        finish_kernel,
        out_shape=(
            shape((channel_part, 2 * columns), f32),
            shape((tokens, channel_part), bf16),
            shape((tokens, channel_part), bf16),
        ),
        in_specs=[vmem] * 6,
        out_specs=[vmem] * 3,
        compiler_params=pltpu.CompilerParams(vmem_limit_bytes=VMEM_LIMIT),
        cost_estimate=pl.CostEstimate(
            flops=10**9, bytes_accessed=10**7, transcendentals=0
        ),
        name="finish",
    )(conv_back, conv_taps, value_in, gate_in, grads, mixed)
    return (grad_gate[None], grad_up[None], grad_down[None], grad_out, value_grad, gate_grad)


def solution(mesh):
    planar = mesh.shape["sp"] == 4 and mesh.shape["tp"] == 2 * mesh.shape["sp"]
    return jax.shard_map(
        fused_device if planar else per_device,
        mesh=mesh,
        in_specs=(
            P("sp", "tp"),
            P("sp", "tp"),
            P("tp"),
            P("sp", None),
            P("sp", None),
            P("sp", None, "tp"),
            P("sp", None, "tp"),
            P("sp", "tp", None),
            P("sp", "tp"),
            P("sp", "tp"),
            P("sp", "tp"),
            P("tp"),
            P(None, "tp"),
            P("tp", None),
        ),
        out_specs=(
            P("sp", None, "tp"),
            P("sp", None, "tp"),
            P("sp", "tp", None),
            P("tp", "sp"),
            P("sp", "tp"),
            P("sp", "tp"),
        ),
        check_vma=False,
    )
```

```python
import functools

import jax
import jax.numpy as jnp
from jax import lax
from jax.experimental import pallas as pl
from jax.experimental.pallas import tpu as pltpu
from jax.sharding import PartitionSpec as P


EPSILON = 1e-06
VMEM_LIMIT = 60 * 2**20


def shifted(block, axis, distance):
    devices = range(lax.axis_size(axis))
    route = [(i - distance, i) for i in devices if i - distance in devices]
    return lax.ppermute(block, axis, route)


def group_sum_kernel(axis, group, own_ref, out_ref, landed, send_sems, recv_sems):
    me = lax.axis_index(axis)
    barrier = pltpu.get_barrier_semaphore()
    for step in range(1, group):
        pl.semaphore_signal(
            barrier,
            inc=1,
            device_id={axis: lax.rem(me + step, group)},
            device_id_type=pl.DeviceIdType.MESH,
        )
    pl.semaphore_wait(barrier, group - 1)
    copies = []
    for step in range(1, group):
        copy = pltpu.make_async_remote_copy(
            src_ref=own_ref,
            dst_ref=landed.at[step - 1],
            send_sem=send_sems.at[step - 1],
            recv_sem=recv_sems.at[step - 1],
            device_id={axis: lax.rem(me + step, group)},
            device_id_type=pl.DeviceIdType.MESH,
        )
        copy.start()
        copies.append(copy)
    for copy in copies:
        copy.wait()
    total = own_ref[...]
    for step in range(1, group):
        total = total + landed[step - 1]
    out_ref[...] = total


def group_sum(vectors, axis, collective_id):
    block = jnp.stack(vectors, axis=0)
    group = lax.axis_size(axis)
    summed = pl.pallas_call(
        functools.partial(group_sum_kernel, axis, group),
        out_shape=jax.ShapeDtypeStruct(block.shape, block.dtype),
        in_specs=[pl.BlockSpec(memory_space=pltpu.VMEM)],
        out_specs=pl.BlockSpec(memory_space=pltpu.VMEM),
        scratch_shapes=[
            pltpu.VMEM((group - 1,) + block.shape, block.dtype),
            pltpu.SemaphoreType.DMA((group - 1,)),
            pltpu.SemaphoreType.DMA((group - 1,)),
        ],
        compiler_params=pltpu.CompilerParams(
            collective_id=collective_id, has_side_effects=True
        ),
        cost_estimate=pl.CostEstimate(
            flops=group * block.size, bytes_accessed=400 * block.size * 4, transcendentals=0
        ),
        name="group_sum",
    )(block)
    return tuple(summed[row] for row in range(len(vectors)))


def silu_slope(values):
    logistic = jax.nn.sigmoid(values)
    return logistic * (1.0 + values * (1.0 - logistic))


def per_device(
    upstream,
    stream,
    norm_gain,
    routes,
    route_weights,
    w_gate,
    w_up,
    w_down,
    value_in,
    gate_in,
    conv_pre,
    ln_gain,
    conv_taps,
    w_out,
):
    tok_rows, width_part = stream.shape
    token_groups = lax.axis_size("sp")
    width_groups = lax.axis_size("tp")
    model_width = width_part * width_groups
    channels = conv_pre.shape[1] * width_groups
    tap_count = conv_taps.shape[0]
    capacity = 3 * tok_rows // token_groups
    experts = w_gate.shape[0] * token_groups
    slot_count = experts * capacity
    expert_rows = token_groups * capacity
    flat_experts = routes.reshape(-1)
    one_hot = (flat_experts[:, None] == jnp.arange(experts, dtype=jnp.int32)[None, :]).astype(
        jnp.int32
    )
    slot_rank = jnp.sum((jnp.cumsum(one_hot, axis=0) - one_hot) * one_hot, axis=1)
    slot_index = (flat_experts * capacity + slot_rank).reshape(tok_rows, 2)
    slot_ids = jnp.arange(slot_count, dtype=jnp.int32)[:, None]
    first_hit = slot_ids == slot_index[None, :, 0]
    second_hit = slot_ids == slot_index[None, :, 1]
    any_hit = jnp.logical_or(first_hit, second_hit)
    picker = any_hit.astype(jnp.bfloat16)
    slot_weight = jnp.sum(
        jnp.where(first_hit, route_weights[None, :, 0], 0.0)
        + jnp.where(second_hit, route_weights[None, :, 1], 0.0),
        axis=1,
    )
    token_iota = jnp.arange(tok_rows, dtype=jnp.int32)[None, :]
    slot_token = jnp.where(
        jnp.any(any_hit, axis=1), jnp.sum(jnp.where(any_hit, token_iota, 0), axis=1), tok_rows
    )
    columns = stream.shape[1]
    spare = jnp.zeros((1, columns), jnp.bfloat16)
    upstream_pad = jnp.concatenate([upstream, spare], axis=0)
    cotangent = (upstream_pad[slot_token].astype(jnp.float32) * slot_weight[:, None]).astype(
        jnp.bfloat16
    )
    sent_cotangent = cotangent.reshape(experts, capacity, columns)
    part_cotangent = lax.all_to_all(
        sent_cotangent, "sp", split_axis=0, concat_axis=0, tiled=True
    ).reshape(expert_rows, width_part)
    part_cotangent, stream_late, conv_late = lax.optimization_barrier(
        (part_cotangent, stream, conv_pre)
    )
    cotangent = lax.all_gather(part_cotangent, "tp", axis=1, tiled=True)
    residual = stream_late.astype(jnp.float32)
    conv_vals = conv_late.astype(jnp.float32)
    row_squares, conv_total, conv_squares = group_sum(
        (
            jnp.sum(residual * residual, axis=1),
            jnp.sum(conv_vals, axis=1),
            jnp.sum(conv_vals * conv_vals, axis=1),
        ),
        "tp",
        0,
    )
    inverse = lax.rsqrt(row_squares / model_width + EPSILON)[:, None]
    normed = (norm_gain[None, :] * residual * inverse).astype(jnp.bfloat16)
    normed_pad = jnp.concatenate([normed, spare], axis=0)
    inputs = normed_pad[slot_token]
    sent_inputs = inputs.reshape(experts, capacity, columns)
    part_inputs = lax.all_to_all(sent_inputs, "sp", split_axis=0, concat_axis=0, tiled=True)
    inputs = lax.all_gather(
        part_inputs.reshape(expert_rows, width_part), "tp", axis=1, tiled=True
    )
    gate_mat = w_gate[0]
    upper_mat = w_up[0]
    down_mat = w_down[0]
    gate_pre = jnp.dot(inputs, gate_mat, preferred_element_type=jnp.float32)
    upper_pre = jnp.dot(inputs, upper_mat, preferred_element_type=jnp.float32)
    active = (jax.nn.silu(gate_pre) * upper_pre).astype(jnp.bfloat16)
    active_back = lax.dot_general(
        cotangent, down_mat, (((1,), (1,)), ((), ())), preferred_element_type=jnp.float32
    )
    gate_back = (active_back * upper_pre * silu_slope(gate_pre)).astype(jnp.bfloat16)
    upper_back = (active_back * jax.nn.silu(gate_pre)).astype(jnp.bfloat16)
    grad_gate = lax.dot_general(
        inputs, gate_back, (((0,), (0,)), ((), ())), preferred_element_type=jnp.float32
    )
    grad_up = lax.dot_general(
        inputs, upper_back, (((0,), (0,)), ((), ())), preferred_element_type=jnp.float32
    )
    grad_down = lax.dot_general(
        active, cotangent, (((0,), (0,)), ((), ())), preferred_element_type=jnp.float32
    )
    input_part = lax.dot_general(
        gate_back, gate_mat, (((1,), (1,)), ((), ())), preferred_element_type=jnp.float32
    ) + lax.dot_general(
        upper_back, upper_mat, (((1,), (1,)), ((), ())), preferred_element_type=jnp.float32
    )
    input_back = lax.psum_scatter(
        input_part.astype(jnp.bfloat16), "tp", scatter_dimension=1, tiled=True
    )
    input_back, grad_gate, grad_up, grad_down = lax.optimization_barrier(
        (input_back, grad_gate, grad_up, grad_down)
    )
    returned = lax.all_to_all(
        input_back.reshape(token_groups, capacity, width_part),
        "sp",
        split_axis=0,
        concat_axis=0,
        tiled=True,
    )
    returned = returned.reshape(slot_count, width_part)
    token_back = lax.dot_general(
        picker, returned, (((0,), (0,)), ((), ())), preferred_element_type=jnp.float32
    )
    gained = norm_gain[None, :] * token_back
    (inner_sum,) = group_sum((jnp.sum(gained * residual, axis=1),), "tp", 1)
    norm_back = inverse * gained - residual * inverse**3 * (inner_sum / model_width)[:, None]
    stream_grad = (upstream.astype(jnp.float32) + norm_back).astype(jnp.bfloat16)
    full_grad = lax.all_gather(stream_grad, "tp", axis=1, tiled=True)
    mean_val = (conv_total / channels)[:, None]
    variance = (conv_squares / channels)[:, None] - mean_val * mean_val
    inv_std = lax.rsqrt(variance + EPSILON)
    centred = (conv_vals - mean_val) * inv_std
    scaled = centred * ln_gain[None, :]
    mixed_out = jax.nn.silu(scaled).astype(jnp.bfloat16)
    grad_rows = lax.dot_general(
        full_grad, mixed_out, (((0,), (0,)), ((), ())), preferred_element_type=jnp.float32
    ).astype(jnp.bfloat16)
    grad_out = (
        lax.psum_scatter(grad_rows, "sp", scatter_dimension=0, tiled=True).astype(jnp.float32).T
    )
    mixed_back = lax.dot_general(
        full_grad, w_out, (((1,), (1,)), ((), ())), preferred_element_type=jnp.float32
    )
    norm_in = mixed_back * silu_slope(scaled) * ln_gain[None, :]
    norm_total, norm_cross = group_sum(
        (jnp.sum(norm_in, axis=1), jnp.sum(norm_in * centred, axis=1)), "tp", 2
    )
    conv_back = inv_std * (
        norm_in - (norm_total / channels)[:, None] - centred * (norm_cross / channels)[:, None]
    )
    next_rim = shifted(conv_back[: tap_count - 1], "sp", -1)
    padded = jnp.concatenate([conv_back, next_rim], axis=0)
    glu_back = jnp.zeros(conv_back.shape, jnp.float32)
    for tap_index in range(tap_count):
        offset = tap_count - 1 - tap_index
        glu_back = glu_back + conv_taps[tap_index][None, :] * padded[offset : offset + tok_rows]
    gate_sigma = jax.nn.sigmoid(gate_in.astype(jnp.float32))
    value_grad = (glu_back * gate_sigma).astype(jnp.bfloat16)
    gate_grad = (glu_back * value_in.astype(jnp.float32) * gate_sigma * (1.0 - gate_sigma)).astype(
        jnp.bfloat16
    )
    return (grad_gate[None], grad_up[None], grad_down[None], grad_out, value_grad, gate_grad)


MESH_ID = pl.DeviceIdType.MESH


def remote(src, dst, send_sem, recv_sem, sp_index, tp_index):
    return pltpu.make_async_remote_copy(
        src_ref=src,
        dst_ref=dst,
        send_sem=send_sem,
        recv_sem=recv_sem,
        device_id={"sp": sp_index, "tp": tp_index},
        device_id_type=MESH_ID,
    )


def signal(devices):
    barrier = pltpu.get_barrier_semaphore()
    for sp_index, tp_index in devices:
        pl.semaphore_signal(
            barrier,
            inc=1,
            device_id={"sp": sp_index, "tp": tp_index},
            device_id_type=MESH_ID,
        )


def await_signals(count):
    pl.semaphore_wait(pltpu.get_barrier_semaphore(), count)


def places():
    sp = lax.axis_index("sp")
    tp = lax.axis_index("tp")
    chip, core = tp // 2, tp % 2
    side = 1 - 2 * (sp % 2)
    lift = 2 - 4 * (sp // 2)
    across, along = sp + side, sp + lift
    corner = 3 - sp
    hops = (
        chip,
        chip + 1 - 2 * (chip % 2),
        2 - chip // 2,
        3 - 3 * (chip // 2),
    )
    return sp, tp, chip, core, across, along, corner, hops


def to_column(row):
    count = row.shape[1]
    down = lax.broadcasted_iota(jnp.int32, (count, count), 0)
    over = lax.broadcasted_iota(jnp.int32, (count, count), 1)
    return jnp.sum(jnp.where(down == over, row, 0.0), axis=1, keepdims=True)


def to_row(column):
    count = column.shape[0]
    down = lax.broadcasted_iota(jnp.int32, (count, count), 0)
    over = lax.broadcasted_iota(jnp.int32, (count, count), 1)
    return jnp.sum(jnp.where(down == over, column, 0.0), axis=0, keepdims=True)


def dot_nt(left, right):
    return lax.dot_general(
        left, right, (((1,), (1,)), ((), ())), preferred_element_type=jnp.float32
    )


def dot_tn(left, right):
    return lax.dot_general(
        left, right, (((0,), (0,)), ((), ())), preferred_element_type=jnp.float32
    )


def expert_kernel(
    width,
    stream_ref,
    up_ref,
    gain_ref,
    routes_ref,
    weights_ref,
    conv_ref,
    wg_hbm,
    wu_hbm,
    wd_hbm,
    rows_s_out,
    rows_u_out,
    hidden_out,
    active_out,
    keep_out,
    far_x_out,
    far_y_out,
    near_x_out,
    near_y_out,
    stat_out,
    rows_s,
    rows_u,
    hidden,
    active,
    keep,
    send_x,
    send_y,
    gs_ref,
    stat_ref,
    wrow_ref,
    wgu,
    wd,
    mate_w,
    mate_h,
    acc,
    back,
    stat_in,
    inv_out,
    inv_in,
    w_in,
    z_send,
    piece_recv,
    xy_send,
    relay_send,
    mate_send,
    mate_recv,
    last_send,
    last_recv,
    c_send,
    near_send,
    near_recv,
    stat_send,
    stat_recv,
    inv_send,
    inv_recv,
    w_send,
    w_recv,
    mw_sems,
    mh_send,
    mh_recv,
    local_sems,
    rows_sems,
    small_sems,
):
    sp, tp, chip, core, across, along, corner, hops = places()
    mate = tp + 1 - 2 * core
    tokens, columns = gs_ref.shape
    part = wd_hbm.shape[0]
    sp_count, tp_count = 4, 8
    row_of = sp // 2
    col_of = lax.rem(sp, 2)
    peers = [lax.rem(tp + step, tp_count) for step in range(1, tp_count)]
    others = (across, along, corner)
    owns = (gs_ref, up_ref)
    rows = (rows_s, rows_u)
    rows_out = (rows_s_out, rows_u_out)

    signal([(sp, peer) for peer in peers] + [(other, tp) for other in others])
    loads = [
        pltpu.make_async_copy(up_ref, rows_u.at[sp, core, chip], local_sems.at[3]),
        pltpu.make_async_copy(wg_hbm, wgu.at[:, :, :, pl.ds(0, part)], local_sems.at[0]),
        pltpu.make_async_copy(wu_hbm, wgu.at[:, :, :, pl.ds(part, part)], local_sems.at[1]),
        pltpu.make_async_copy(wd_hbm, wd, local_sems.at[2]),
    ]
    for load in loads:
        load.start()
    own_rows = pltpu.make_async_copy(gs_ref, rows_s.at[sp, core, chip], local_sems.at[4])

    gain = gain_ref[...]
    squares = []
    for begin in range(0, tokens, 64):
        block = stream_ref[begin : begin + 64].astype(jnp.float32)
        gs_ref[begin : begin + 64] = (gain * block).astype(jnp.bfloat16)
        squares.append(jnp.sum(block * block, axis=1, keepdims=True))
    conv_vals = conv_ref[...].astype(jnp.float32)
    stat_ref[...] = jnp.concatenate(
        [
            to_row(jnp.concatenate(squares, axis=0)),
            to_row(jnp.sum(conv_vals, axis=1, keepdims=True)),
            to_row(jnp.sum(conv_vals * conv_vals, axis=1, keepdims=True)),
            jnp.zeros((5, tokens), jnp.float32),
        ],
        axis=0,
    )
    for expert in range(sp_count):
        row = jnp.sum(
            jnp.where(routes_ref[...] == expert, weights_ref[...], 0.0), axis=0, keepdims=True
        )
        wrow_ref[expert] = jnp.broadcast_to(row, (8, tokens))
    await_signals(len(peers) + len(others))
    own_rows.start()

    pending = []
    stores = []

    def go(copy):
        copy.start()
        pending.append(copy)

    def store(source, target, sem):
        copy = pltpu.make_async_copy(source, target, sem)
        copy.start()
        stores.append(copy)

    for i, peer in enumerate(peers):
        go(remote(stat_ref, stat_in.at[tp], stat_send.at[i], stat_recv.at[tp], sp, peer))
    for i, other in enumerate(others):
        go(remote(wrow_ref.at[other], w_in.at[sp], w_send.at[i], w_recv.at[sp], other, tp))

    def send_piece(kind, step, source):
        place = hops[step]
        for way, target in enumerate((across, along)):
            go(
                remote(
                    source,
                    rows[kind].at[sp, core, place],
                    xy_send.at[kind, step, way],
                    piece_recv.at[kind, sp, place],
                    target,
                    tp,
                )
            )

    edge = lax.rem(chip + 1, 4) // 2 == 0
    middle = jnp.logical_not(edge)

    def z_copy(kind, origin, step, send_sem, source=None):
        slot = rows[kind].at[origin, core, chip]
        return remote(
            slot if source is None else source,
            slot,
            send_sem,
            piece_recv.at[kind, origin, chip],
            sp,
            2 * hops[step] + core,
        )

    def pass_copy(kind, origin, send_sem):
        slot = rows[kind].at[origin, core, hops[2]]
        return remote(
            slot,
            slot,
            send_sem,
            piece_recv.at[kind, origin, hops[2]],
            sp,
            2 * hops[1] + core,
        )

    for kind in (0, 1):
        for step in (1, 2):
            go(z_copy(kind, sp, step, z_send.at[kind, step - 1], owns[kind]))

        @pl.when(edge)
        def _(kind=kind):
            z_copy(kind, sp, 3, z_send.at[kind, 2], owns[kind]).start()

        send_piece(kind, 0, owns[kind])

    def await_piece(kind, origin, step):
        slot = rows[kind].at[origin, core, hops[step]]
        remote(
            slot,
            slot,
            mate_send.at[kind, origin],
            piece_recv.at[kind, origin, hops[step]],
            sp,
            mate,
        ).wait_recv()

    def relay(kind, step):
        origin, target = (across, along) if step % 2 == 0 else (along, across)
        await_piece(kind, origin, step)
        slot = rows[kind].at[origin, core, hops[step]]
        go(
            remote(
                slot,
                slot,
                relay_send.at[kind, step],
                piece_recv.at[kind, origin, hops[step]],
                target,
                tp,
            )
        )

    def share(kind, origin):
        slot = rows[kind].at[origin, core]
        go(
            remote(
                slot, slot, mate_send.at[kind, origin], mate_recv.at[kind, origin], sp, mate
            )
        )
        store(slot, rows_out[kind].at[origin, core], rows_sems.at[kind, origin, 0])

    def await_share(kind, origin):
        slot = rows[kind].at[origin, 1 - core]
        remote(
            slot, slot, mate_send.at[kind, origin], mate_recv.at[kind, origin], sp, mate
        ).wait_recv()
        store(slot, rows_out[kind].at[origin, 1 - core], rows_sems.at[kind, origin, 1])

    acc[...] = jnp.zeros(acc.shape, jnp.float32)
    back[...] = jnp.zeros(back.shape, jnp.float32)
    w_in[sp] = wrow_ref[sp]

    total = stat_ref[...]
    for peer in peers:
        remote(
            stat_in.at[peer], stat_in.at[peer], stat_send.at[0], stat_recv.at[peer], sp, peer
        ).wait_recv()
        total = total + stat_in[peer]
    stat_out[...] = total
    inverse_row = lax.rsqrt(total[0:1] / width + EPSILON)
    inv_out[...] = jnp.broadcast_to(inverse_row, inv_out.shape)
    inv_in[sp] = jnp.broadcast_to(inverse_row, inv_out.shape)
    for i, other in enumerate(others):
        go(remote(inv_out, inv_in.at[sp], inv_send.at[i], inv_recv.at[sp], other, tp))

    def forward(origin):
        def body(index, carry):
            half, place = index // 4, lax.rem(index, 4)
            acc[origin] += jnp.dot(
                rows_s[origin, half, place],
                wgu[place, half],
                preferred_element_type=jnp.float32,
            )
            return carry

        lax.fori_loop(0, tp_count, body, 0)

    def backward_piece(origin, half, place):
        start = pl.multiple_of((2 * place + half) * columns, columns)
        back[origin] += dot_nt(rows_u[origin, half, place], wd[:, pl.ds(start, columns)])

    def backward(origin):
        def body(index, carry):
            backward_piece(origin, index // 4, lax.rem(index, 4))
            return carry

        lax.fori_loop(0, tp_count, body, 0)

    chunk = 64

    def activate(origin):
        inverse = to_column(inv_in[origin, 0:1])
        weight = to_column(w_in[origin, 0:1])
        for begin in range(0, tokens, chunk):
            end = begin + chunk
            pre = acc[origin, begin:end] * inverse[begin:end]
            gate, upper = pre[:, :part], pre[:, part:]
            cot = back[origin, begin:end] * weight[begin:end]
            logistic = 1.0 / (1.0 + jnp.exp(-gate))
            silu = gate * logistic
            slope = logistic * (1.0 + gate * (1.0 - logistic))
            active[origin, begin:end] = (silu * upper * weight[begin:end]).astype(jnp.bfloat16)
            back_inv = cot * inverse[begin:end]
            hidden[origin, begin:end, :part] = (back_inv * upper * slope).astype(jnp.bfloat16)
            hidden[origin, begin:end, part:] = (back_inv * silu).astype(jnp.bfloat16)
        go(
            remote(
                hidden.at[origin],
                mate_h.at[origin],
                mh_send.at[origin],
                mh_recv.at[origin],
                sp,
                mate,
            )
        )

    def spread(origin, low, high):
        remote(
            mate_h.at[origin],
            mate_h.at[origin],
            mh_send.at[origin],
            mh_recv.at[origin],
            sp,
            mate,
        ).wait_recv()
        store(hidden.at[origin], hidden_out.at[origin], small_sems.at[0, origin])
        store(active.at[origin], active_out.at[origin], small_sems.at[1, origin])

        for target, first in ((low, 0), (high, 2)):

            def body(i, carry, target=target, first=first):
                place = first + i
                part_sum = dot_nt(hidden[origin], wgu[place, core]) + dot_nt(
                    mate_h[origin], mate_w[place]
                )
                target[i] = part_sum.astype(jnp.bfloat16)
                return carry

            lax.fori_loop(0, 2, body, 0)

    def pass_on(kind, origin, send_sem):
        @pl.when(middle)
        def _():
            pass_copy(kind, origin, send_sem).start()

    def arrive(kind, step):
        await_piece(kind, sp, step)
        if step == 2:
            pass_on(kind, sp, z_send.at[kind, 2])
        send_piece(kind, step, rows[kind].at[sp, core, hops[step]])

    def corner_out(kind):
        await_piece(kind, corner, 0)
        go(z_copy(kind, corner, 1, c_send.at[kind, 0]))

        @pl.when(middle)
        def _():
            z_copy(kind, corner, 2, c_send.at[kind, 1]).start()

    def corner_in(kind):
        await_piece(kind, corner, 2)
        pass_on(kind, corner, c_send.at[kind, 2])

    relay(0, 0)
    arrive(0, 1)
    relay(1, 0)
    arrive(0, 2)
    corner_out(0)
    arrive(0, 3)
    own_rows.wait()
    for load in loads:
        load.wait()
    share(0, sp)
    go(remote(wgu.at[:, 1 - core], mate_w, mw_sems.at[0], mw_sems.at[1], sp, mate))
    corner_out(1)
    arrive(1, 1)
    await_share(0, sp)
    forward(sp)
    arrive(1, 2)
    corner_in(0)
    arrive(1, 3)
    share(1, sp)
    relay(0, 3)
    for step in (1, 2, 3):
        await_piece(0, across, step)
    share(0, across)
    for step in (0, 1, 2):
        await_piece(0, along, step)
    share(0, along)
    await_share(1, sp)
    backward(sp)
    corner_in(1)
    await_share(0, across)
    forward(across)
    await_share(0, along)
    forward(along)
    for other in others:
        for sems, landing in ((inv_recv, inv_in), (w_recv, w_in)):
            remote(
                landing.at[other], landing.at[other], inv_send.at[0], sems.at[other], sp, mate
            ).wait_recv()
    activate(sp)
    relay(1, 3)
    for step in (1, 3):
        await_piece(0, corner, step)
    share(0, corner)
    await_share(0, corner)
    forward(corner)
    for step in (1, 2, 3):
        await_piece(1, across, step)
    share(1, across)
    for step in (0, 1, 2):
        await_piece(1, along, step)
    share(1, along)
    remote(mate_w, mate_w, mw_sems.at[0], mw_sems.at[1], sp, mate).wait_recv()
    await_share(1, across)
    backward(across)
    activate(across)
    await_share(1, along)
    backward(along)
    activate(along)
    spread(across, send_x.at[0], keep.at[1, 1 - col_of])
    for i in range(2):
        go(
            remote(
                send_x.at[0, i], near_x_out.at[i], near_send.at[0, i], near_recv.at[0, i], across, tp
            )
        )
    store(keep.at[1, 1 - col_of], keep_out.at[1, 1 - col_of], small_sems.at[2, 0])
    spread(along, keep.at[0, 1 - row_of], send_y.at[0])
    for i in range(2):
        go(
            remote(
                send_y.at[0, i], near_y_out.at[i], near_send.at[1, i], near_recv.at[1, i], along, tp
            )
        )
    store(keep.at[0, 1 - row_of], keep_out.at[0, 1 - row_of], small_sems.at[2, 1])
    spread(sp, keep.at[0, row_of], keep.at[1, col_of])
    store(keep.at[0, row_of], keep_out.at[0, row_of], small_sems.at[2, 2])
    store(keep.at[1, col_of], keep_out.at[1, col_of], small_sems.at[2, 3])
    for step in (0, 1, 2, 3):
        place = hops[step]
        if step in (1, 3):
            await_piece(1, corner, step)
        slot = rows_u.at[corner, core, place]
        go(remote(slot, slot, last_send.at[place], last_recv.at[place], sp, mate))
        backward_piece(corner, core, place)
    store(rows_u.at[corner, core], rows_u_out.at[corner, core], rows_sems.at[1, corner, 0])
    for step in (0, 1, 2, 3):
        place = hops[step]
        slot = rows_u.at[corner, 1 - core, place]
        remote(slot, slot, last_send.at[place], last_recv.at[place], sp, mate).wait_recv()
        backward_piece(corner, 1 - core, place)
    store(rows_u.at[corner, 1 - core], rows_u_out.at[corner, 1 - core], rows_sems.at[1, corner, 1])
    activate(corner)
    spread(corner, send_x.at[1], send_y.at[1])
    store(send_x.at[1], far_x_out, small_sems.at[3, 0])
    store(send_y.at[1], far_y_out, small_sems.at[3, 1])
    for side, landing in enumerate((near_x_out, near_y_out)):
        for i in range(2):
            remote(
                landing.at[i], landing.at[i], near_send.at[side, i], near_recv.at[side, i], sp, mate
            ).wait_recv()
    for copy in stores:
        copy.wait()
    for copy in pending:
        copy.wait_send()
    for kind in (0, 1):

        @pl.when(edge)
        def _(kind=kind):
            z_copy(kind, sp, 3, z_send.at[kind, 2], owns[kind]).wait_send()

        @pl.when(middle)
        def _(kind=kind):
            pass_copy(kind, sp, z_send.at[kind, 2]).wait_send()
            z_copy(kind, corner, 2, c_send.at[kind, 1]).wait_send()
            pass_copy(kind, corner, c_send.at[kind, 2]).wait_send()


def grads_kernel(rows_s, rows_u, hidden, active, gate_out, up_out, down_out, tall, wide, sems):
    columns = rows_s.shape[4]
    part = active.shape[2]
    pieces = 8

    def copies(piece, slot):
        span = pl.ds(pl.multiple_of(piece * columns, columns), columns)
        return (
            pltpu.make_async_copy(
                tall.at[slot, :, pl.ds(0, part)], gate_out.at[span], sems.at[slot, 0]
            ),
            pltpu.make_async_copy(
                tall.at[slot, :, pl.ds(part, part)], up_out.at[span], sems.at[slot, 1]
            ),
            pltpu.make_async_copy(wide.at[slot], down_out.at[:, span], sems.at[slot, 2]),
        )

    def body(piece, carry):
        slot = lax.rem(piece, 2)
        half, place = lax.rem(piece, 2), piece // 2

        @pl.when(piece >= 2)
        def _():
            for copy in copies(piece - 2, slot):
                copy.wait()

        for origin in range(4):
            tall_term = dot_tn(rows_s[origin, half, place], hidden[origin])
            wide_term = dot_tn(active[origin], rows_u[origin, half, place])
            if origin == 0:
                tall[slot] = tall_term
                wide[slot] = wide_term
            else:
                tall[slot] += tall_term
                wide[slot] += wide_term
        for copy in copies(piece, slot):
            copy.start()
        return carry

    lax.fori_loop(0, pieces, body, 0)
    for piece in (pieces - 2, pieces - 1):
        for copy in copies(piece, piece % 2):
            copy.wait()


def return_kernel(
    width,
    channels,
    keep_hbm,
    far_x_hbm,
    far_y_hbm,
    near_x_hbm,
    near_y_hbm,
    up_ref,
    stream_ref,
    gain_ref,
    stat_ref,
    conv_ref,
    ln_ref,
    w_hbm,
    conv_out,
    grads,
    mixed,
    w_out,
    keep,
    far,
    near,
    mixed_ref,
    slope_ref,
    centred_ref,
    turn_out,
    turn_in,
    z_out,
    z_in,
    over_in,
    over_sum,
    own_sum,
    mixed_back,
    note_out,
    note_in,
    tail_out,
    tail_in,
    full,
    rim_in,
    mix_send,
    mix_recv,
    turn_send,
    turn_recv,
    z_send,
    z_recv,
    over_recv,
    note_send,
    note_recv,
    tail_send,
    tail_recv,
    full_send,
    full_recv,
    mate_send,
    mate_recv,
    grad_send,
    grad_recv,
    gmate_send,
    gmate_recv,
    rim_sems,
    local_sems,
):
    sp, tp, chip, core, across, along, corner, hops = places()
    mate = tp + 1 - 2 * core
    tp_count = 8
    tokens, columns = up_ref.shape
    row_of = sp // 2
    col_of = lax.rem(sp, 2)
    peers = [lax.rem(tp + step, tp_count) for step in range(1, tp_count)]
    others = (across, along, corner)
    signal([(sp, peer) for peer in peers] + [(other, tp) for other in others])
    pulls = [
        pltpu.make_async_copy(source, target, local_sems.at[2 + i])
        for i, (source, target) in enumerate(
            (
                (far_x_hbm, far.at[0]),
                (far_y_hbm, far.at[1]),
                (keep_hbm, keep),
                (near_x_hbm, near.at[0]),
                (near_y_hbm, near.at[1]),
            )
        )
    ]
    for pull in pulls:
        pull.start()
    load = pltpu.make_async_copy(w_hbm, w_out, local_sems.at[0])
    load.start()
    inverse = to_column(lax.rsqrt(stat_ref[0:1] / width + EPSILON))
    mean_row = stat_ref[1:2] / channels
    inv_std = to_column(lax.rsqrt(stat_ref[2:3] / channels - mean_row * mean_row + EPSILON))
    mean_val = to_column(mean_row)
    ln_gain = ln_ref[...]
    for begin in range(0, tokens, 64):
        end = begin + 64
        block = (conv_ref[begin:end].astype(jnp.float32) - mean_val[begin:end]) * inv_std[
            begin:end
        ]
        scaled = block * ln_gain
        logistic = 1.0 / (1.0 + jnp.exp(-scaled))
        centred_ref[begin:end] = block
        mixed_ref[begin:end] = (scaled * logistic).astype(jnp.bfloat16)
        slope_ref[begin:end] = logistic * (1.0 + scaled * (1.0 - logistic)) * ln_gain
    await_signals(len(peers) + len(others))
    own_mixed = pltpu.make_async_copy(mixed_ref, mixed.at[sp], local_sems.at[1])
    own_mixed.start()
    for pull in pulls:
        pull.wait()
    pending = []

    def go(copy):
        copy.start()
        pending.append(copy)

    edge = lax.rem(chip + 1, 4) // 2 == 0
    middle = jnp.logical_not(edge)
    halves = 2
    half_rows = tokens // halves
    spans = [pl.ds(h * half_rows, half_rows) for h in range(halves)]

    def turn_copy(group, i, h):
        return remote(
            turn_out.at[group, i, spans[h]],
            turn_in.at[group, i, spans[h]],
            turn_send.at[group, i, h],
            turn_recv.at[group, i, h],
            (along, across)[group] if isinstance(group, int) else sp,
            tp,
        )

    for h in range(halves):
        for i in range(2):
            for group, off in ((0, 1 - row_of), (1, 1 - col_of)):
                turn_out[group, i, spans[h]] = (
                    keep[group, off, i, spans[h]].astype(jnp.float32)
                    + far[group, i, spans[h]].astype(jnp.float32)
                ).astype(jnp.bfloat16)
                go(turn_copy(group, i, h))
    for i, other in enumerate(others):
        go(remote(mixed_ref, mixed.at[sp], mix_send.at[i], mix_recv.at[sp], other, tp))

    def plane_sum(place, h):
        group, i = place // 2, lax.rem(place, 2)
        own = row_of + group * (col_of - row_of)
        remote(
            turn_in.at[group, i, spans[h]],
            turn_in.at[group, i, spans[h]],
            turn_send.at[group, i, h],
            turn_recv.at[group, i, h],
            sp,
            mate,
        ).wait_recv()
        return (
            keep[group, own, i, spans[h]].astype(jnp.float32)
            + near[group, i, spans[h]].astype(jnp.float32)
            + turn_in[group, i, spans[h]].astype(jnp.float32)
        )

    def z_copy(step, h):
        return remote(
            z_out.at[step, h],
            z_in.at[chip, h],
            z_send.at[step, h],
            z_recv.at[chip, h],
            sp,
            2 * hops[step] + core,
        )

    def over_copy(h):
        return remote(
            z_out.at[2, h], over_in.at[h], z_send.at[2, h], over_recv.at[h], sp, 2 * hops[1] + core
        )

    def await_z(step, h):
        slot = z_in.at[hops[step], h]
        remote(slot, slot, z_send.at[0, h], z_recv.at[hops[step], h], sp, mate).wait_recv()

    def reduce_out(h):
        summed = plane_sum(hops[2], h)

        @pl.when(edge)
        def _():
            z_out[2, h] = summed.astype(jnp.bfloat16)
            over_copy(h).start()

        @pl.when(middle)
        def _():
            over_sum[h] = summed

        for step in (3, 1):
            z_out[step, h] = plane_sum(hops[step], h).astype(jnp.bfloat16)
            go(z_copy(step, h))
        own_sum[spans[h]] = plane_sum(chip, h)

    def reduce_over(h):
        @pl.when(middle)
        def _():
            slot = over_in.at[h]
            remote(slot, slot, z_send.at[2, h], over_recv.at[h], sp, mate).wait_recv()
            z_out[2, h] = (over_sum[h] + over_in[h].astype(jnp.float32)).astype(jnp.bfloat16)
            z_copy(2, h).start()

    gain = gain_ref[...]
    inner_rows = []

    def reduce_in(h):
        for step in (1, 2):
            await_z(step, h)
        total = (
            own_sum[spans[h]]
            + z_in[hops[1], h].astype(jnp.float32)
            + z_in[hops[2], h].astype(jnp.float32)
        )
        own_sum[spans[h]] = total

        @pl.when(edge)
        def _():
            await_z(3, h)
            own_sum[spans[h]] += z_in[hops[3], h].astype(jnp.float32)

        gained = gain * own_sum[spans[h]]
        own_sum[spans[h]] = gained
        row = to_row(
            jnp.sum(gained * stream_ref[spans[h]].astype(jnp.float32), axis=1, keepdims=True)
        )
        inner_rows.append(row)
        note_out[h] = jnp.broadcast_to(row, note_out.shape[1:])
        for i, peer in enumerate(peers):
            go(
                remote(
                    note_out.at[h], note_in.at[tp, h], note_send.at[i, h], note_recv.at[tp, h], sp, peer
                )
            )

    def full_slot(place, h, half=None):
        return full.at[core if half is None else half, place, spans[h]]

    def full_copy(step, h):
        slot = full_slot(chip, h)
        return remote(
            slot, slot, full_send.at[step - 1, h], full_recv.at[chip, h], sp, 2 * hops[step] + core
        )

    def full_pass(h):
        slot = full_slot(hops[2], h)
        return remote(
            slot, slot, full_send.at[2, h], full_recv.at[hops[2], h], sp, 2 * hops[1] + core
        )

    def gather_out(h):
        row = inner_rows[h]
        for peer in peers:
            slot = note_in.at[peer, h]
            remote(slot, slot, note_send.at[0, h], note_recv.at[peer, h], sp, peer).wait_recv()
            row = row + note_in[peer, h, 0:1]
        scale = inverse[h * half_rows : (h + 1) * half_rows]
        factor = scale * scale * to_column(row) / width
        full[core, chip, spans[h]] = (
            up_ref[spans[h]].astype(jnp.float32)
            + own_sum[spans[h]]
            - stream_ref[spans[h]].astype(jnp.float32) * factor
        ).astype(jnp.bfloat16)
        for step in (1, 2):
            go(full_copy(step, h))

        @pl.when(edge)
        def _():
            full_copy(3, h).start()

    def mate_copy(place, h, half=None):
        slot = full_slot(place, h, half)
        return remote(slot, slot, mate_send.at[place, h], mate_recv.at[place, h], sp, mate)

    def grad_copy(place, h):
        return remote(
            full_slot(place, h),
            grads.at[sp, core, spans[h]],
            grad_send.at[place, h],
            grad_recv.at[sp, h],
            place,
            tp,
        )

    def mixed_term(half, place, h):
        start = pl.multiple_of((2 * place + half) * columns, columns)
        return dot_nt(full[half, place, spans[h]], w_out[:, pl.ds(start, columns)])

    def fan(step, h):
        place = hops[step]
        if step > 0:
            slot = full_slot(place, h)
            remote(slot, slot, full_send.at[0, h], full_recv.at[place, h], sp, mate).wait_recv()
        if step == 2:

            @pl.when(middle)
            def _():
                full_pass(h).start()

        mate_copy(place, h).start()

        @pl.when(place != sp)
        def _():
            grad_copy(place, h).start()

        term = mixed_term(core, place, h)
        if step == 0:
            mixed_back[spans[h]] = term
        else:
            mixed_back[spans[h]] += term

    tails = []

    def norm_out(h):
        total = mixed_back[spans[h]]
        for step in range(4):
            place = hops[step]
            mate_copy(place, h, 1 - core).wait_recv()
            total = total + mixed_term(1 - core, place, h)
        norm_in = total * slope_ref[spans[h]]
        mixed_back[spans[h]] = norm_in
        sums = jnp.concatenate(
            [
                to_row(jnp.sum(norm_in, axis=1, keepdims=True)),
                to_row(jnp.sum(norm_in * centred_ref[spans[h]], axis=1, keepdims=True)),
                jnp.zeros((6, half_rows), jnp.float32),
            ],
            axis=0,
        )
        tails.append(sums)
        tail_out[h] = sums
        for i, peer in enumerate(peers):
            go(
                remote(
                    tail_out.at[h], tail_in.at[tp, h], tail_send.at[i, h], tail_recv.at[tp, h], sp, peer
                )
            )

    def norm_back(h):
        sums = tails[h]
        for peer in peers:
            slot = tail_in.at[peer, h]
            remote(slot, slot, tail_send.at[0, h], tail_recv.at[peer, h], sp, peer).wait_recv()
            sums = sums + tail_in[peer, h]
        conv_out[spans[h]] = inv_std[h * half_rows : (h + 1) * half_rows] * (
            mixed_back[spans[h]]
            - to_column(sums[0:1]) / channels
            - centred_ref[spans[h]] * (to_column(sums[1:2]) / channels)
        )

    def grads_in(h):
        for other in others:
            slot = grads.at[other, core, spans[h]]
            remote(slot, slot, grad_send.at[0, h], grad_recv.at[other, h], other, tp).wait_recv()
            go(
                remote(
                    slot, slot, gmate_send.at[other, h], gmate_recv.at[other, h], sp, mate
                )
            )

    rim = rim_in.shape[0]
    before = lax.rem(sp + 3, 4)
    reduce_out(0)
    reduce_out(1)
    reduce_over(0)
    reduce_over(1)
    reduce_in(0)
    gather_out(0)
    reduce_in(1)
    load.wait()
    fan(0, 0)
    fan(1, 0)
    gather_out(1)
    fan(2, 0)
    fan(3, 0)
    fan(0, 1)
    fan(1, 1)
    norm_out(0)
    fan(2, 1)
    norm_back(0)
    go(
        remote(
            conv_out.at[pl.ds(0, rim)], rim_in, rim_sems.at[0], rim_sems.at[1], before, tp
        )
    )
    grads_in(0)
    own_mixed.wait()
    for other in others:
        slot = mixed.at[other]
        remote(slot, slot, mix_send.at[0], mix_recv.at[other], other, tp).wait_recv()
    fan(3, 1)
    norm_out(1)
    for half in range(2):
        grads[sp, half] = full[half, sp]
    grads_in(1)
    norm_back(1)
    remote(rim_in, rim_in, rim_sems.at[0], rim_sems.at[1], before, tp).wait_recv()
    last = (sp < 3).astype(jnp.float32)
    conv_out[tokens : tokens + rim] = rim_in[...] * last
    for h in range(halves):
        for other in others:
            slot = grads.at[other, 1 - core, spans[h]]
            remote(
                slot, slot, gmate_send.at[other, h], gmate_recv.at[other, h], sp, mate
            ).wait_recv()
        for step in range(4):
            place = hops[step]
            mate_copy(place, h).wait_send()

            @pl.when(place != sp)
            def _(place=place, h=h):
                grad_copy(place, h).wait_send()

        @pl.when(edge)
        def _(h=h):
            over_copy(h).wait_send()
            full_copy(3, h).wait_send()

        @pl.when(middle)
        def _(h=h):
            z_copy(2, h).wait_send()
            full_pass(h).wait_send()

    for copy in pending:
        copy.wait_send()


def finish_kernel(conv, taps, value_in, gate_in, grads, mixed, grad_out, value_out, gate_out):
    tokens, part = value_in.shape
    tap_count = taps.shape[0]
    columns = grads.shape[3]
    for half in range(2):
        total = dot_tn(mixed[0], grads[0, half])
        for origin in range(1, 4):
            total = total + dot_tn(mixed[origin], grads[origin, half])
        grad_out[:, half * columns : (half + 1) * columns] = total
    glu = jnp.zeros((tokens, part), jnp.float32)
    for residue in range(8):
        rolled = None
        for offset in range(residue, tap_count, 8):
            base = offset - residue
            tap = taps[tap_count - 1 - offset : tap_count - offset]
            term = tap * conv[base : base + tokens + 8]
            rolled = term if rolled is None else rolled + term
        glu = glu + rolled[residue : residue + tokens]
    sigma = 1.0 / (1.0 + jnp.exp(-gate_in[...].astype(jnp.float32)))
    value_out[...] = (glu * sigma).astype(jnp.bfloat16)
    gate_out[...] = (
        glu * value_in[...].astype(jnp.float32) * sigma * (1.0 - sigma)
    ).astype(jnp.bfloat16)


def fused_device(
    upstream,
    stream,
    norm_gain,
    routes,
    route_weights,
    w_gate,
    w_up,
    w_down,
    value_in,
    gate_in,
    conv_pre,
    ln_gain,
    conv_taps,
    w_out,
):
    tokens, columns = stream.shape
    tp_count = lax.axis_size("tp")
    sp_count = lax.axis_size("sp")
    chips = tp_count // 2
    width = columns * tp_count
    part = w_gate.shape[2]
    channel_part = conv_pre.shape[1]
    channels = channel_part * tp_count
    bf16, f32 = jnp.bfloat16, jnp.float32
    vmem = pl.BlockSpec(memory_space=pltpu.VMEM)
    anywhere = pl.BlockSpec(memory_space=pl.ANY)
    dma = pltpu.SemaphoreType.DMA
    shape = jax.ShapeDtypeStruct

    piece = (chips, 2, columns, part)
    rows_shape = (sp_count, 2, chips, tokens, columns)
    outs = pl.pallas_call(
        functools.partial(expert_kernel, width),
        out_shape=(
            shape(rows_shape, bf16),
            shape(rows_shape, bf16),
            shape((sp_count, tokens, 2 * part), bf16),
            shape((sp_count, tokens, part), bf16),
            shape((2, 2, 2, tokens, columns), bf16),
            shape((2, tokens, columns), bf16),
            shape((2, tokens, columns), bf16),
            shape((2, tokens, columns), bf16),
            shape((2, tokens, columns), bf16),
            shape((8, tokens), f32),
        ),
        in_specs=[vmem] * 6 + [anywhere] * 3,
        out_specs=[anywhere] * 9 + [vmem],
        scratch_shapes=[
            pltpu.VMEM(rows_shape, bf16),
            pltpu.VMEM(rows_shape, bf16),
            pltpu.VMEM((sp_count, tokens, 2 * part), bf16),
            pltpu.VMEM((sp_count, tokens, part), bf16),
            pltpu.VMEM((2, 2, 2, tokens, columns), bf16),
            pltpu.VMEM((2, 2, tokens, columns), bf16),
            pltpu.VMEM((2, 2, tokens, columns), bf16),
            pltpu.VMEM((tokens, columns), bf16),
            pltpu.VMEM((8, tokens), f32),
            pltpu.VMEM((sp_count, 8, tokens), f32),
            pltpu.VMEM((chips, 2, columns, 2 * part), bf16),
            pltpu.VMEM((part, width), bf16),
            pltpu.VMEM((chips, columns, 2 * part), bf16),
            pltpu.VMEM((sp_count, tokens, 2 * part), bf16),
            pltpu.VMEM((sp_count, tokens, 2 * part), f32),
            pltpu.VMEM((sp_count, tokens, part), f32),
            pltpu.VMEM((tp_count, 8, tokens), f32),
            pltpu.VMEM((8, tokens), f32),
            pltpu.VMEM((sp_count, 8, tokens), f32),
            pltpu.VMEM((sp_count, 8, tokens), f32),
            dma((2, 3)),
            dma((2, sp_count, chips)),
            dma((2, chips, 2)),
            dma((2, chips)),
            dma((2, sp_count)),
            dma((2, sp_count)),
            dma((chips,)),
            dma((chips,)),
            dma((2, 3)),
            dma((2, 2)),
            dma((2, 2)),
            dma((tp_count - 1,)),
            dma((tp_count,)),
            dma((3,)),
            dma((sp_count,)),
            dma((3,)),
            dma((sp_count,)),
            dma((2,)),
            dma((sp_count,)),
            dma((sp_count,)),
            dma((5,)),
            dma((2, sp_count, 2)),
            dma((4, sp_count)),
        ],
        compiler_params=pltpu.CompilerParams(
            collective_id=3, has_side_effects=True, vmem_limit_bytes=VMEM_LIMIT
        ),
        cost_estimate=pl.CostEstimate(
            flops=10**10, bytes_accessed=10**8, transcendentals=0
        ),
        name="expert_gather",
    )(
        stream,
        upstream,
        norm_gain[None, :],
        routes.T,
        route_weights.T,
        conv_pre,
        w_gate[0].reshape(piece),
        w_up[0].reshape(piece),
        w_down[0],
    )
    rows_s, rows_u, hidden, active, keep, far_x, far_y, near_x, near_y, totals = outs

    def swap(block, step):
        route = [(i, i + step if (i // step) % 2 == 0 else i - step) for i in range(sp_count)]
        return lax.ppermute(block, "sp", route)

    got_x = swap(far_x, 1)
    got_y = swap(far_y, 2)

    grad_gate, grad_up, grad_down = pl.pallas_call(
        grads_kernel,
        out_shape=(shape((width, part), f32), shape((width, part), f32), shape((part, width), f32)),
        in_specs=[vmem] * 4,
        out_specs=[anywhere] * 3,
        scratch_shapes=[
            pltpu.VMEM((2, columns, 2 * part), f32),
            pltpu.VMEM((2, part, columns), f32),
            dma((2, 3)),
        ],
        compiler_params=pltpu.CompilerParams(vmem_limit_bytes=VMEM_LIMIT),
        cost_estimate=pl.CostEstimate(
            flops=6 * width * part * tokens * sp_count,
            bytes_accessed=40 * 2**20,
            transcendentals=0,
        ),
        name="weight_grads",
    )(rows_s, rows_u, hidden, active)

    rim = -(-(conv_taps.shape[0] - 1) // 8) * 8
    conv_back, grads, mixed = pl.pallas_call(
        functools.partial(return_kernel, width, channels),
        out_shape=(
            shape((tokens + rim, channel_part), f32),
            shape((sp_count, 2, tokens, columns), bf16),
            shape((sp_count, tokens, channel_part), bf16),
        ),
        in_specs=[anywhere] * 5 + [vmem] * 6 + [anywhere],
        out_specs=[vmem] * 3,
        scratch_shapes=[
            pltpu.VMEM(w_out.shape, bf16),
            pltpu.VMEM((2, 2, 2, tokens, columns), bf16),
            pltpu.VMEM((2, 2, tokens, columns), bf16),
            pltpu.VMEM((2, 2, tokens, columns), bf16),
            pltpu.VMEM((tokens, channel_part), bf16),
            pltpu.VMEM((tokens, channel_part), f32),
            pltpu.VMEM((tokens, channel_part), f32),
            pltpu.VMEM((2, 2, tokens, columns), bf16),
            pltpu.VMEM((2, 2, tokens, columns), bf16),
            pltpu.VMEM((chips, 2, tokens // 2, columns), bf16),
            pltpu.VMEM((chips, 2, tokens // 2, columns), bf16),
            pltpu.VMEM((2, tokens // 2, columns), bf16),
            pltpu.VMEM((2, tokens // 2, columns), f32),
            pltpu.VMEM((tokens, columns), f32),
            pltpu.VMEM((tokens, channel_part), f32),
            pltpu.VMEM((2, 8, tokens // 2), f32),
            pltpu.VMEM((tp_count, 2, 8, tokens // 2), f32),
            pltpu.VMEM((2, 8, tokens // 2), f32),
            pltpu.VMEM((tp_count, 2, 8, tokens // 2), f32),
            pltpu.VMEM((2, chips, tokens, columns), bf16),
            pltpu.VMEM((rim, channel_part), f32),
            dma((3,)),
            dma((sp_count,)),
            dma((2, 2, 2)),
            dma((2, 2, 2)),
            dma((chips, 2)),
            dma((chips, 2)),
            dma((2,)),
            dma((tp_count - 1, 2)),
            dma((tp_count, 2)),
            dma((tp_count - 1, 2)),
            dma((tp_count, 2)),
            dma((3, 2)),
            dma((chips, 2)),
            dma((chips, 2)),
            dma((chips, 2)),
            dma((sp_count, 2)),
            dma((sp_count, 2)),
            dma((sp_count, 2)),
            dma((sp_count, 2)),
            dma((2,)),
            dma((7,)),
        ],
        compiler_params=pltpu.CompilerParams(
            collective_id=4, has_side_effects=True, vmem_limit_bytes=VMEM_LIMIT
        ),
        cost_estimate=pl.CostEstimate(
            flops=10**10, bytes_accessed=10**8, transcendentals=0
        ),
        name="return_path",
    )(
        keep,
        got_x,
        got_y,
        near_x,
        near_y,
        upstream,
        stream,
        norm_gain[None, :],
        totals,
        conv_pre,
        ln_gain[None, :],
        w_out,
    )
    grad_out, value_grad, gate_grad = pl.pallas_call(
        finish_kernel,
        out_shape=(
            shape((channel_part, 2 * columns), f32),
            shape((tokens, channel_part), bf16),
            shape((tokens, channel_part), bf16),
        ),
        in_specs=[vmem] * 6,
        out_specs=[vmem] * 3,
        compiler_params=pltpu.CompilerParams(vmem_limit_bytes=VMEM_LIMIT),
        cost_estimate=pl.CostEstimate(
            flops=10**9, bytes_accessed=10**7, transcendentals=0
        ),
        name="finish",
    )(conv_back, conv_taps, value_in, gate_in, grads, mixed)
    return (grad_gate[None], grad_up[None], grad_down[None], grad_out, value_grad, gate_grad)


def solution(mesh):
    planar = mesh.shape["sp"] == 4 and mesh.shape["tp"] == 2 * mesh.shape["sp"]
    return jax.shard_map(
        fused_device if planar else per_device,
        mesh=mesh,
        in_specs=(
            P("sp", "tp"),
            P("sp", "tp"),
            P("tp"),
            P("sp", None),
            P("sp", None),
            P("sp", None, "tp"),
            P("sp", None, "tp"),
            P("sp", "tp", None),
            P("sp", "tp"),
            P("sp", "tp"),
            P("sp", "tp"),
            P("tp"),
            P(None, "tp"),
            P("tp", None),
        ),
        out_specs=(
            P("sp", None, "tp"),
            P("sp", None, "tp"),
            P("sp", "tp", None),
            P("tp", "sp"),
            P("sp", "tp"),
            P("sp", "tp"),
        ),
        check_vma=False,
    )
```

```python
import functools

import jax
import jax.numpy as jnp
from jax import lax
from jax.experimental import pallas as pl
from jax.experimental.pallas import tpu as pltpu
from jax.sharding import PartitionSpec as P


EPSILON = 1e-06
VMEM_LIMIT = 60 * 2**20


def shifted(block, axis, distance):
    devices = range(lax.axis_size(axis))
    route = [(i - distance, i) for i in devices if i - distance in devices]
    return lax.ppermute(block, axis, route)


def group_sum_kernel(axis, group, own_ref, out_ref, landed, send_sems, recv_sems):
    me = lax.axis_index(axis)
    barrier = pltpu.get_barrier_semaphore()
    for step in range(1, group):
        pl.semaphore_signal(
            barrier,
            inc=1,
            device_id={axis: lax.rem(me + step, group)},
            device_id_type=pl.DeviceIdType.MESH,
        )
    pl.semaphore_wait(barrier, group - 1)
    copies = []
    for step in range(1, group):
        copy = pltpu.make_async_remote_copy(
            src_ref=own_ref,
            dst_ref=landed.at[step - 1],
            send_sem=send_sems.at[step - 1],
            recv_sem=recv_sems.at[step - 1],
            device_id={axis: lax.rem(me + step, group)},
            device_id_type=pl.DeviceIdType.MESH,
        )
        copy.start()
        copies.append(copy)
    for copy in copies:
        copy.wait()
    total = own_ref[...]
    for step in range(1, group):
        total = total + landed[step - 1]
    out_ref[...] = total


def group_sum(vectors, axis, collective_id):
    block = jnp.stack(vectors, axis=0)
    group = lax.axis_size(axis)
    summed = pl.pallas_call(
        functools.partial(group_sum_kernel, axis, group),
        out_shape=jax.ShapeDtypeStruct(block.shape, block.dtype),
        in_specs=[pl.BlockSpec(memory_space=pltpu.VMEM)],
        out_specs=pl.BlockSpec(memory_space=pltpu.VMEM),
        scratch_shapes=[
            pltpu.VMEM((group - 1,) + block.shape, block.dtype),
            pltpu.SemaphoreType.DMA((group - 1,)),
            pltpu.SemaphoreType.DMA((group - 1,)),
        ],
        compiler_params=pltpu.CompilerParams(
            collective_id=collective_id, has_side_effects=True
        ),
        cost_estimate=pl.CostEstimate(
            flops=group * block.size, bytes_accessed=400 * block.size * 4, transcendentals=0
        ),
        name="group_sum",
    )(block)
    return tuple(summed[row] for row in range(len(vectors)))


def silu_slope(values):
    logistic = jax.nn.sigmoid(values)
    return logistic * (1.0 + values * (1.0 - logistic))


def per_device(
    upstream,
    stream,
    norm_gain,
    routes,
    route_weights,
    w_gate,
    w_up,
    w_down,
    value_in,
    gate_in,
    conv_pre,
    ln_gain,
    conv_taps,
    w_out,
):
    tok_rows, width_part = stream.shape
    token_groups = lax.axis_size("sp")
    width_groups = lax.axis_size("tp")
    model_width = width_part * width_groups
    channels = conv_pre.shape[1] * width_groups
    tap_count = conv_taps.shape[0]
    capacity = 3 * tok_rows // token_groups
    experts = w_gate.shape[0] * token_groups
    slot_count = experts * capacity
    expert_rows = token_groups * capacity
    flat_experts = routes.reshape(-1)
    one_hot = (flat_experts[:, None] == jnp.arange(experts, dtype=jnp.int32)[None, :]).astype(
        jnp.int32
    )
    slot_rank = jnp.sum((jnp.cumsum(one_hot, axis=0) - one_hot) * one_hot, axis=1)
    slot_index = (flat_experts * capacity + slot_rank).reshape(tok_rows, 2)
    slot_ids = jnp.arange(slot_count, dtype=jnp.int32)[:, None]
    first_hit = slot_ids == slot_index[None, :, 0]
    second_hit = slot_ids == slot_index[None, :, 1]
    any_hit = jnp.logical_or(first_hit, second_hit)
    picker = any_hit.astype(jnp.bfloat16)
    slot_weight = jnp.sum(
        jnp.where(first_hit, route_weights[None, :, 0], 0.0)
        + jnp.where(second_hit, route_weights[None, :, 1], 0.0),
        axis=1,
    )
    token_iota = jnp.arange(tok_rows, dtype=jnp.int32)[None, :]
    slot_token = jnp.where(
        jnp.any(any_hit, axis=1), jnp.sum(jnp.where(any_hit, token_iota, 0), axis=1), tok_rows
    )
    columns = stream.shape[1]
    spare = jnp.zeros((1, columns), jnp.bfloat16)
    upstream_pad = jnp.concatenate([upstream, spare], axis=0)
    cotangent = (upstream_pad[slot_token].astype(jnp.float32) * slot_weight[:, None]).astype(
        jnp.bfloat16
    )
    sent_cotangent = cotangent.reshape(experts, capacity, columns)
    part_cotangent = lax.all_to_all(
        sent_cotangent, "sp", split_axis=0, concat_axis=0, tiled=True
    ).reshape(expert_rows, width_part)
    part_cotangent, stream_late, conv_late = lax.optimization_barrier(
        (part_cotangent, stream, conv_pre)
    )
    cotangent = lax.all_gather(part_cotangent, "tp", axis=1, tiled=True)
    residual = stream_late.astype(jnp.float32)
    conv_vals = conv_late.astype(jnp.float32)
    row_squares, conv_total, conv_squares = group_sum(
        (
            jnp.sum(residual * residual, axis=1),
            jnp.sum(conv_vals, axis=1),
            jnp.sum(conv_vals * conv_vals, axis=1),
        ),
        "tp",
        0,
    )
    inverse = lax.rsqrt(row_squares / model_width + EPSILON)[:, None]
    normed = (norm_gain[None, :] * residual * inverse).astype(jnp.bfloat16)
    normed_pad = jnp.concatenate([normed, spare], axis=0)
    inputs = normed_pad[slot_token]
    sent_inputs = inputs.reshape(experts, capacity, columns)
    part_inputs = lax.all_to_all(sent_inputs, "sp", split_axis=0, concat_axis=0, tiled=True)
    inputs = lax.all_gather(
        part_inputs.reshape(expert_rows, width_part), "tp", axis=1, tiled=True
    )
    gate_mat = w_gate[0]
    upper_mat = w_up[0]
    down_mat = w_down[0]
    gate_pre = jnp.dot(inputs, gate_mat, preferred_element_type=jnp.float32)
    upper_pre = jnp.dot(inputs, upper_mat, preferred_element_type=jnp.float32)
    active = (jax.nn.silu(gate_pre) * upper_pre).astype(jnp.bfloat16)
    active_back = lax.dot_general(
        cotangent, down_mat, (((1,), (1,)), ((), ())), preferred_element_type=jnp.float32
    )
    gate_back = (active_back * upper_pre * silu_slope(gate_pre)).astype(jnp.bfloat16)
    upper_back = (active_back * jax.nn.silu(gate_pre)).astype(jnp.bfloat16)
    grad_gate = lax.dot_general(
        inputs, gate_back, (((0,), (0,)), ((), ())), preferred_element_type=jnp.float32
    )
    grad_up = lax.dot_general(
        inputs, upper_back, (((0,), (0,)), ((), ())), preferred_element_type=jnp.float32
    )
    grad_down = lax.dot_general(
        active, cotangent, (((0,), (0,)), ((), ())), preferred_element_type=jnp.float32
    )
    input_part = lax.dot_general(
        gate_back, gate_mat, (((1,), (1,)), ((), ())), preferred_element_type=jnp.float32
    ) + lax.dot_general(
        upper_back, upper_mat, (((1,), (1,)), ((), ())), preferred_element_type=jnp.float32
    )
    input_back = lax.psum_scatter(
        input_part.astype(jnp.bfloat16), "tp", scatter_dimension=1, tiled=True
    )
    input_back, grad_gate, grad_up, grad_down = lax.optimization_barrier(
        (input_back, grad_gate, grad_up, grad_down)
    )
    returned = lax.all_to_all(
        input_back.reshape(token_groups, capacity, width_part),
        "sp",
        split_axis=0,
        concat_axis=0,
        tiled=True,
    )
    returned = returned.reshape(slot_count, width_part)
    token_back = lax.dot_general(
        picker, returned, (((0,), (0,)), ((), ())), preferred_element_type=jnp.float32
    )
    gained = norm_gain[None, :] * token_back
    (inner_sum,) = group_sum((jnp.sum(gained * residual, axis=1),), "tp", 1)
    norm_back = inverse * gained - residual * inverse**3 * (inner_sum / model_width)[:, None]
    stream_grad = (upstream.astype(jnp.float32) + norm_back).astype(jnp.bfloat16)
    full_grad = lax.all_gather(stream_grad, "tp", axis=1, tiled=True)
    mean_val = (conv_total / channels)[:, None]
    variance = (conv_squares / channels)[:, None] - mean_val * mean_val
    inv_std = lax.rsqrt(variance + EPSILON)
    centred = (conv_vals - mean_val) * inv_std
    scaled = centred * ln_gain[None, :]
    mixed_out = jax.nn.silu(scaled).astype(jnp.bfloat16)
    grad_rows = lax.dot_general(
        full_grad, mixed_out, (((0,), (0,)), ((), ())), preferred_element_type=jnp.float32
    ).astype(jnp.bfloat16)
    grad_out = (
        lax.psum_scatter(grad_rows, "sp", scatter_dimension=0, tiled=True).astype(jnp.float32).T
    )
    mixed_back = lax.dot_general(
        full_grad, w_out, (((1,), (1,)), ((), ())), preferred_element_type=jnp.float32
    )
    norm_in = mixed_back * silu_slope(scaled) * ln_gain[None, :]
    norm_total, norm_cross = group_sum(
        (jnp.sum(norm_in, axis=1), jnp.sum(norm_in * centred, axis=1)), "tp", 2
    )
    conv_back = inv_std * (
        norm_in - (norm_total / channels)[:, None] - centred * (norm_cross / channels)[:, None]
    )
    next_rim = shifted(conv_back[: tap_count - 1], "sp", -1)
    padded = jnp.concatenate([conv_back, next_rim], axis=0)
    glu_back = jnp.zeros(conv_back.shape, jnp.float32)
    for tap_index in range(tap_count):
        offset = tap_count - 1 - tap_index
        glu_back = glu_back + conv_taps[tap_index][None, :] * padded[offset : offset + tok_rows]
    gate_sigma = jax.nn.sigmoid(gate_in.astype(jnp.float32))
    value_grad = (glu_back * gate_sigma).astype(jnp.bfloat16)
    gate_grad = (glu_back * value_in.astype(jnp.float32) * gate_sigma * (1.0 - gate_sigma)).astype(
        jnp.bfloat16
    )
    return (grad_gate[None], grad_up[None], grad_down[None], grad_out, value_grad, gate_grad)


MESH_ID = pl.DeviceIdType.MESH


def remote(src, dst, send_sem, recv_sem, sp_index, tp_index):
    return pltpu.make_async_remote_copy(
        src_ref=src,
        dst_ref=dst,
        send_sem=send_sem,
        recv_sem=recv_sem,
        device_id={"sp": sp_index, "tp": tp_index},
        device_id_type=MESH_ID,
    )


def signal(devices):
    barrier = pltpu.get_barrier_semaphore()
    for sp_index, tp_index in devices:
        pl.semaphore_signal(
            barrier,
            inc=1,
            device_id={"sp": sp_index, "tp": tp_index},
            device_id_type=MESH_ID,
        )


def await_signals(count):
    pl.semaphore_wait(pltpu.get_barrier_semaphore(), count)


def places():
    sp = lax.axis_index("sp")
    tp = lax.axis_index("tp")
    chip, core = tp // 2, tp % 2
    side = 1 - 2 * (sp % 2)
    lift = 2 - 4 * (sp // 2)
    across, along = sp + side, sp + lift
    corner = 3 - sp
    hops = (
        chip,
        chip + 1 - 2 * (chip % 2),
        2 - chip // 2,
        3 - 3 * (chip // 2),
    )
    return sp, tp, chip, core, across, along, corner, hops


def to_column(row):
    count = row.shape[1]
    down = lax.broadcasted_iota(jnp.int32, (count, count), 0)
    over = lax.broadcasted_iota(jnp.int32, (count, count), 1)
    return jnp.sum(jnp.where(down == over, row, 0.0), axis=1, keepdims=True)


def to_row(column):
    count = column.shape[0]
    down = lax.broadcasted_iota(jnp.int32, (count, count), 0)
    over = lax.broadcasted_iota(jnp.int32, (count, count), 1)
    return jnp.sum(jnp.where(down == over, column, 0.0), axis=0, keepdims=True)


def dot_nt(left, right):
    return lax.dot_general(
        left, right, (((1,), (1,)), ((), ())), preferred_element_type=jnp.float32
    )


def dot_tn(left, right):
    return lax.dot_general(
        left, right, (((0,), (0,)), ((), ())), preferred_element_type=jnp.float32
    )


def step_kernel(
    width,
    channels,
    stream_ref,
    up_ref,
    gain_ref,
    routes_ref,
    weights_ref,
    conv_ref,
    ln_ref,
    wg_hbm,
    wu_hbm,
    wd_hbm,
    w_hbm,
    rows_s_out,
    rows_u_out,
    hidden_out,
    active_out,
    conv_out,
    grads,
    mixed,
    rows_s,
    rows_u,
    hidden,
    active,
    keep,
    send_x,
    send_y,
    near,
    far,
    gs_ref,
    stat_ref,
    stat_out,
    wrow_ref,
    wgu,
    wd,
    mate_w,
    mate_h,
    acc,
    back,
    stat_in,
    inv_out,
    inv_in,
    w_in,
    w_out,
    mixed_ref,
    slope_ref,
    centred_ref,
    turn_out,
    turn_in,
    z_out,
    z_in,
    over_in,
    over_sum,
    own_sum,
    mixed_back,
    note_out,
    note_in,
    tail_out,
    tail_in,
    full,
    rim_in,
    z_send,
    piece_recv,
    xy_send,
    relay_send,
    mate_send,
    mate_recv,
    last_send,
    last_recv,
    c_send,
    near_send,
    near_recv,
    far_send,
    far_recv,
    stat_send,
    stat_recv,
    inv_send,
    inv_recv,
    w_send,
    w_recv,
    mw_sems,
    mh_send,
    mh_recv,
    local_sems,
    rows_sems,
    small_sems,
    mix_send,
    mix_recv,
    turn_send,
    turn_recv,
    r_send,
    r_recv,
    over_recv,
    note_send,
    note_recv,
    tail_send,
    tail_recv,
    full_send,
    full_recv,
    fm_send,
    fm_recv,
    grad_send,
    grad_recv,
    gmate_send,
    gmate_recv,
    rim_sems,
):
    sp, tp, chip, core, across, along, corner, hops = places()
    mate = tp + 1 - 2 * core
    tokens, columns = gs_ref.shape
    part = wd_hbm.shape[0]
    sp_count, tp_count = 4, 8
    row_of = sp // 2
    col_of = lax.rem(sp, 2)
    peers = [lax.rem(tp + step, tp_count) for step in range(1, tp_count)]
    others = (across, along, corner)
    owns = (gs_ref, up_ref)
    rows = (rows_s, rows_u)
    rows_out = (rows_s_out, rows_u_out)

    signal([(sp, peer) for peer in peers] + [(other, tp) for other in others])
    loads = [
        pltpu.make_async_copy(up_ref, rows_u.at[sp, core, chip], local_sems.at[3]),
        pltpu.make_async_copy(wg_hbm, wgu.at[:, :, :, pl.ds(0, part)], local_sems.at[0]),
        pltpu.make_async_copy(wu_hbm, wgu.at[:, :, :, pl.ds(part, part)], local_sems.at[1]),
        pltpu.make_async_copy(wd_hbm, wd, local_sems.at[2]),
    ]
    for load in loads:
        load.start()
    out_load = pltpu.make_async_copy(w_hbm, w_out, local_sems.at[5])
    out_load.start()
    own_rows = pltpu.make_async_copy(gs_ref, rows_s.at[sp, core, chip], local_sems.at[4])

    gain = gain_ref[...]
    squares = []
    for begin in range(0, tokens, 64):
        block = stream_ref[begin : begin + 64].astype(jnp.float32)
        gs_ref[begin : begin + 64] = (gain * block).astype(jnp.bfloat16)
        squares.append(jnp.sum(block * block, axis=1, keepdims=True))
    conv_vals = conv_ref[...].astype(jnp.float32)
    stat_ref[...] = jnp.concatenate(
        [
            to_row(jnp.concatenate(squares, axis=0)),
            to_row(jnp.sum(conv_vals, axis=1, keepdims=True)),
            to_row(jnp.sum(conv_vals * conv_vals, axis=1, keepdims=True)),
            jnp.zeros((5, tokens), jnp.float32),
        ],
        axis=0,
    )
    for expert in range(sp_count):
        row = jnp.sum(
            jnp.where(routes_ref[...] == expert, weights_ref[...], 0.0), axis=0, keepdims=True
        )
        wrow_ref[expert] = jnp.broadcast_to(row, (8, tokens))
    await_signals(len(peers) + len(others))
    own_rows.start()

    pending = []
    stores = []

    def go(copy):
        copy.start()
        pending.append(copy)

    def store(source, target, sem):
        copy = pltpu.make_async_copy(source, target, sem)
        copy.start()
        stores.append(copy)

    for i, peer in enumerate(peers):
        go(remote(stat_ref, stat_in.at[tp], stat_send.at[i], stat_recv.at[tp], sp, peer))
    for i, other in enumerate(others):
        go(remote(wrow_ref.at[other], w_in.at[sp], w_send.at[i], w_recv.at[sp], other, tp))

    def send_piece(kind, step, source, place):
        for way, target in enumerate((across, along)):
            go(
                remote(
                    source,
                    rows[kind].at[sp, core, place],
                    xy_send.at[kind, step, way],
                    piece_recv.at[kind, sp, place],
                    target,
                    tp,
                )
            )

    edge = lax.rem(chip + 1, 4) // 2 == 0
    middle = jnp.logical_not(edge)

    def z_copy(kind, origin, step, send_sem, source=None):
        slot = rows[kind].at[origin, core, chip]
        return remote(
            slot if source is None else source,
            slot,
            send_sem,
            piece_recv.at[kind, origin, chip],
            sp,
            2 * hops[step] + core,
        )

    def pass_copy(kind, origin, send_sem):
        slot = rows[kind].at[origin, core, hops[2]]
        return remote(
            slot,
            slot,
            send_sem,
            piece_recv.at[kind, origin, hops[2]],
            sp,
            2 * hops[1] + core,
        )

    for kind in (0, 1):
        for step in (1, 2):
            go(z_copy(kind, sp, step, z_send.at[kind, step - 1], owns[kind]))

        @pl.when(edge)
        def _(kind=kind):
            z_copy(kind, sp, 3, z_send.at[kind, 2], owns[kind]).start()

        send_piece(kind, 0, owns[kind], chip)

    def await_piece(kind, origin, step):
        slot = rows[kind].at[origin, core, hops[step]]
        remote(
            slot,
            slot,
            mate_send.at[kind, origin],
            piece_recv.at[kind, origin, hops[step]],
            sp,
            mate,
        ).wait_recv()

    def relay(kind, step):
        origin, target = (across, along) if step % 2 == 0 else (along, across)
        await_piece(kind, origin, step)
        slot = rows[kind].at[origin, core, hops[step]]
        go(
            remote(
                slot,
                slot,
                relay_send.at[kind, step],
                piece_recv.at[kind, origin, hops[step]],
                target,
                tp,
            )
        )

    def share(kind, origin):
        slot = rows[kind].at[origin, core]
        go(
            remote(
                slot, slot, mate_send.at[kind, origin], mate_recv.at[kind, origin], sp, mate
            )
        )
        store(slot, rows_out[kind].at[origin, core], rows_sems.at[kind, origin, 0])

    def await_share(kind, origin):
        slot = rows[kind].at[origin, 1 - core]
        remote(
            slot, slot, mate_send.at[kind, origin], mate_recv.at[kind, origin], sp, mate
        ).wait_recv()
        store(slot, rows_out[kind].at[origin, 1 - core], rows_sems.at[kind, origin, 1])

    acc[...] = jnp.zeros(acc.shape, jnp.float32)
    back[...] = jnp.zeros(back.shape, jnp.float32)
    w_in[sp] = wrow_ref[sp]

    total = stat_ref[...]
    for peer in peers:
        remote(
            stat_in.at[peer], stat_in.at[peer], stat_send.at[0], stat_recv.at[peer], sp, peer
        ).wait_recv()
        total = total + stat_in[peer]
    stat_out[...] = total
    halves = 2
    half_rows = tokens // halves
    spans = [pl.ds(h * half_rows, half_rows) for h in range(halves)]
    inverse_row = lax.rsqrt(total[0:1] / width + EPSILON)
    inv_out[...] = jnp.broadcast_to(inverse_row, inv_out.shape)
    inv_in[sp] = jnp.broadcast_to(inverse_row, inv_out.shape)
    for i, other in enumerate(others):
        go(remote(inv_out, inv_in.at[sp], inv_send.at[i], inv_recv.at[sp], other, tp))

    def forward(origin):
        def body(index, carry):
            half, place = index // 4, lax.rem(index, 4)
            acc[origin] += jnp.dot(
                rows_s[origin, half, place],
                wgu[place, half],
                preferred_element_type=jnp.float32,
            )
            return carry

        lax.fori_loop(0, tp_count, body, 0)

    def backward_piece(origin, half, place):
        start = pl.multiple_of((2 * place + half) * columns, columns)
        back[origin] += dot_nt(rows_u[origin, half, place], wd[:, pl.ds(start, columns)])

    def backward(origin):
        def body(index, carry):
            backward_piece(origin, index // 4, lax.rem(index, 4))
            return carry

        lax.fori_loop(0, tp_count, body, 0)

    chunk = 64

    def activate(origin):
        inverse = to_column(inv_in[origin, 0:1])
        weight = to_column(w_in[origin, 0:1])
        for begin in range(0, tokens, chunk):
            end = begin + chunk
            pre = acc[origin, begin:end] * inverse[begin:end]
            gate, upper = pre[:, :part], pre[:, part:]
            cot = back[origin, begin:end] * weight[begin:end]
            logistic = 1.0 / (1.0 + jnp.exp(-gate))
            silu = gate * logistic
            slope = logistic * (1.0 + gate * (1.0 - logistic))
            active[origin, begin:end] = (silu * upper * weight[begin:end]).astype(jnp.bfloat16)
            back_inv = cot * inverse[begin:end]
            hidden[origin, begin:end, :part] = (back_inv * upper * slope).astype(jnp.bfloat16)
            hidden[origin, begin:end, part:] = (back_inv * silu).astype(jnp.bfloat16)
        go(
            remote(
                hidden.at[origin],
                mate_h.at[origin],
                mh_send.at[origin],
                mh_recv.at[origin],
                sp,
                mate,
            )
        )

    def spread(origin, low, high):
        remote(
            mate_h.at[origin],
            mate_h.at[origin],
            mh_send.at[origin],
            mh_recv.at[origin],
            sp,
            mate,
        ).wait_recv()
        store(hidden.at[origin], hidden_out.at[origin], small_sems.at[0, origin])
        store(active.at[origin], active_out.at[origin], small_sems.at[1, origin])

        for target, first in ((low, 0), (high, 2)):

            def body(i, carry, target=target, first=first):
                place = first + i
                part_sum = dot_nt(hidden[origin], wgu[place, core]) + dot_nt(
                    mate_h[origin], mate_w[place]
                )
                target[i] = part_sum.astype(jnp.bfloat16)
                return carry

            lax.fori_loop(0, 2, body, 0)

    def pass_on(kind, origin, send_sem):
        @pl.when(middle)
        def _():
            pass_copy(kind, origin, send_sem).start()

    turn = lax.rem(chip + 1, 4) // 2
    orders = (
        chip,
        hops[1] + turn * (hops[2] - hops[1]),
        hops[2] + turn * (hops[1] - hops[2]),
        hops[3],
    )

    def arrive(kind, number):
        place = orders[number]
        slot = rows[kind].at[sp, core, place]
        remote(
            slot, slot, mate_send.at[kind, sp], piece_recv.at[kind, sp, place], sp, mate
        ).wait_recv()
        if number == 1:
            pass_on(kind, sp, z_send.at[kind, 2])
        send_piece(kind, number, slot, place)

    def corner_out(kind):
        await_piece(kind, corner, 0)
        go(z_copy(kind, corner, 1, c_send.at[kind, 0]))

        @pl.when(middle)
        def _():
            z_copy(kind, corner, 2, c_send.at[kind, 1]).start()

    def corner_over(kind):
        @pl.when(middle)
        def _():
            await_piece(kind, corner, 2)
            pass_copy(kind, corner, c_send.at[kind, 2]).start()

    def await_pieces(kind, origin, steps):
        for step in steps:
            await_piece(kind, origin, step)

    def await_corner(kind, steps):
        await_pieces(kind, corner, steps)

        @pl.when(edge)
        def _():
            await_piece(kind, corner, 2)

    def mix():
        sums = stat_out[...]
        mean_row = sums[1:2] / channels
        conv_std = to_column(lax.rsqrt(sums[2:3] / channels - mean_row * mean_row + EPSILON))
        mean_val = to_column(mean_row)
        ln_gain = ln_ref[...]
        for begin in range(0, tokens, 64):
            end = begin + 64
            block = (conv_ref[begin:end].astype(jnp.float32) - mean_val[begin:end]) * conv_std[
                begin:end
            ]
            scaled = block * ln_gain
            logistic = 1.0 / (1.0 + jnp.exp(-scaled))
            centred_ref[begin:end] = block
            mixed_ref[begin:end] = (scaled * logistic).astype(jnp.bfloat16)
            slope_ref[begin:end] = logistic * (1.0 + scaled * (1.0 - logistic)) * ln_gain
        return conv_std

    def turn_copy(group, i, h):
        return remote(
            turn_out.at[group, i, spans[h]],
            turn_in.at[group, i, spans[h]],
            turn_send.at[group, i, h],
            turn_recv.at[group, i, h],
            (along, across)[group],
            tp,
        )

    def near_copy(side, i, h):
        source, target = ((send_x, across), (send_y, along))[side]
        return remote(
            source.at[0, i, spans[h]],
            near.at[side, i, spans[h]],
            near_send.at[side, i, h],
            near_recv.at[side, i, h],
            target,
            tp,
        )

    def far_copy(side, i, h):
        source, target = ((send_x, across), (send_y, along))[side]
        return remote(
            source.at[1, i, spans[h]],
            far.at[side, i, spans[h]],
            far_send.at[side, i, h],
            far_recv.at[side, i, h],
            target,
            tp,
        )

    def near_out(side, h):
        for i in range(2):
            go(near_copy(side, i, h))

    def far_out(h):
        for i in range(2):
            for side in range(2):
                go(far_copy(side, i, h))

    def second_turn(h):
        for i in range(2):
            for group, off in ((0, 1 - row_of), (1, 1 - col_of)):
                far_copy(group, i, h).wait_recv()
                turn_out[group, i, spans[h]] = (
                    keep[group, off, i, spans[h]].astype(jnp.float32)
                    + far[group, i, spans[h]].astype(jnp.float32)
                ).astype(jnp.bfloat16)
                go(turn_copy(group, i, h))

    def plane_sum(place, h):
        group, i = place // 2, lax.rem(place, 2)
        own = row_of + group * (col_of - row_of)
        remote(
            turn_in.at[group, i, spans[h]],
            turn_in.at[group, i, spans[h]],
            turn_send.at[group, i, h],
            turn_recv.at[group, i, h],
            sp,
            mate,
        ).wait_recv()
        remote(
            near.at[group, i, spans[h]],
            near.at[group, i, spans[h]],
            near_send.at[group, i, h],
            near_recv.at[group, i, h],
            sp,
            mate,
        ).wait_recv()
        return (
            keep[group, own, i, spans[h]].astype(jnp.float32)
            + near[group, i, spans[h]].astype(jnp.float32)
            + turn_in[group, i, spans[h]].astype(jnp.float32)
        )

    def r_copy(step, h):
        return remote(
            z_out.at[step, h],
            z_in.at[chip, h],
            r_send.at[step, h],
            r_recv.at[chip, h],
            sp,
            2 * hops[step] + core,
        )

    def over_copy(h):
        return remote(
            z_out.at[2, h], over_in.at[h], r_send.at[2, h], over_recv.at[h], sp, 2 * hops[1] + core
        )

    def await_z(step, h):
        slot = z_in.at[hops[step], h]
        remote(slot, slot, r_send.at[0, h], r_recv.at[hops[step], h], sp, mate).wait_recv()

    inner_rows = {}

    def reduce_out(h):
        inner = None
        for step in (2, 3, 1, 0):
            place = hops[step]
            summed = plane_sum(place, h)
            term = jnp.sum(
                summed * rows_s[sp, core, place, spans[h]].astype(jnp.float32),
                axis=1,
                keepdims=True,
            )
            inner = term if inner is None else inner + term
            if step == 0:
                own_sum[spans[h]] = summed
            elif step == 2:
                over_sum[h] = summed
                z_out[step, h] = summed.astype(jnp.bfloat16)
            else:
                z_out[step, h] = summed.astype(jnp.bfloat16)
        row = to_row(inner)
        inner_rows[h] = row
        note_out[h] = jnp.broadcast_to(row, note_out.shape[1:])
        for i, peer in enumerate(peers):
            go(
                remote(
                    note_out.at[h], note_in.at[tp, h], note_send.at[i, h], note_recv.at[tp, h], sp, peer
                )
            )

        @pl.when(edge)
        def _():
            over_copy(h).start()

        for step in (3, 1):
            go(r_copy(step, h))

    def reduce_over(h):
        @pl.when(middle)
        def _():
            slot = over_in.at[h]
            remote(slot, slot, r_send.at[2, h], over_recv.at[h], sp, mate).wait_recv()
            z_out[2, h] = (over_sum[h] + over_in[h].astype(jnp.float32)).astype(jnp.bfloat16)
            r_copy(2, h).start()

    def reduce_in(h):
        for step in (1, 2):
            await_z(step, h)
        total = (
            own_sum[spans[h]]
            + z_in[hops[1], h].astype(jnp.float32)
            + z_in[hops[2], h].astype(jnp.float32)
        )
        own_sum[spans[h]] = total

        @pl.when(edge)
        def _():
            await_z(3, h)
            own_sum[spans[h]] += z_in[hops[3], h].astype(jnp.float32)


    def full_slot(place, h, half=None):
        return full.at[core if half is None else half, place, spans[h]]

    def full_copy(step, h):
        slot = full_slot(chip, h)
        return remote(
            slot, slot, full_send.at[step - 1, h], full_recv.at[chip, h], sp, 2 * hops[step] + core
        )

    def full_pass(h):
        slot = full_slot(hops[2], h)
        return remote(
            slot, slot, full_send.at[2, h], full_recv.at[hops[2], h], sp, 2 * hops[1] + core
        )

    def gather_out(h):
        row = inner_rows[h]
        for peer in peers:
            slot = note_in.at[peer, h]
            remote(slot, slot, note_send.at[0, h], note_recv.at[peer, h], sp, peer).wait_recv()
            row = row + note_in[peer, h, 0:1]
        scale = inv_col[h * half_rows : (h + 1) * half_rows]
        factor = scale * scale * to_column(row) / width
        full[core, chip, spans[h]] = (
            up_ref[spans[h]].astype(jnp.float32)
            + gain * own_sum[spans[h]]
            - stream_ref[spans[h]].astype(jnp.float32) * factor
        ).astype(jnp.bfloat16)

        @pl.when(edge)
        def _():
            full_copy(3, h).start()

        for step in (1, 2):
            go(full_copy(step, h))

    def mate_copy(place, h, half=None):
        slot = full_slot(place, h, half)
        return remote(slot, slot, fm_send.at[place, h], fm_recv.at[place, h], sp, mate)

    def grad_copy(place, h):
        return remote(
            full_slot(place, h),
            grads.at[sp, core, spans[h]],
            grad_send.at[place, h],
            grad_recv.at[sp, h],
            place,
            tp,
        )

    def mixed_term(half, place, h):
        start = pl.multiple_of((2 * place + half) * columns, columns)
        return dot_nt(full[half, place, spans[h]], w_out[:, pl.ds(start, columns)])

    def fan(step, h):
        place = hops[step]
        if step > 0:
            slot = full_slot(place, h)
            remote(slot, slot, full_send.at[0, h], full_recv.at[place, h], sp, mate).wait_recv()
        if step == 2:

            @pl.when(middle)
            def _():
                full_pass(h).start()

        mate_copy(place, h).start()

        @pl.when(place != sp)
        def _():
            grad_copy(place, h).start()

        term = mixed_term(core, place, h)
        if step == 0:
            mixed_back[spans[h]] = term
        else:
            mixed_back[spans[h]] += term

    tails = []

    def norm_out(h):
        total = mixed_back[spans[h]]
        for step in range(4):
            place = hops[step]
            mate_copy(place, h, 1 - core).wait_recv()
            total = total + mixed_term(1 - core, place, h)
        norm_in = total * slope_ref[spans[h]]
        mixed_back[spans[h]] = norm_in
        sums = jnp.concatenate(
            [
                to_row(jnp.sum(norm_in, axis=1, keepdims=True)),
                to_row(jnp.sum(norm_in * centred_ref[spans[h]], axis=1, keepdims=True)),
                jnp.zeros((6, half_rows), jnp.float32),
            ],
            axis=0,
        )
        tails.append(sums)
        tail_out[h] = sums
        for i, peer in enumerate(peers):
            go(
                remote(
                    tail_out.at[h], tail_in.at[tp, h], tail_send.at[i, h], tail_recv.at[tp, h], sp, peer
                )
            )

    def norm_back(h):
        sums = tails[h]
        for peer in peers:
            slot = tail_in.at[peer, h]
            remote(slot, slot, tail_send.at[0, h], tail_recv.at[peer, h], sp, peer).wait_recv()
            sums = sums + tail_in[peer, h]
        conv_out[spans[h]] = conv_std[h * half_rows : (h + 1) * half_rows] * (
            mixed_back[spans[h]]
            - to_column(sums[0:1]) / channels
            - centred_ref[spans[h]] * (to_column(sums[1:2]) / channels)
        )

    def grads_in(h):
        for other in others:
            slot = grads.at[other, core, spans[h]]
            remote(slot, slot, grad_send.at[0, h], grad_recv.at[other, h], other, tp).wait_recv()
            go(
                remote(
                    slot, slot, gmate_send.at[other, h], gmate_recv.at[other, h], sp, mate
                )
            )

    rim = rim_in.shape[0]
    before = lax.rem(sp + 3, 4)
    arrive(0, 1)
    relay(0, 0)
    relay(1, 0)
    arrive(1, 1)
    arrive(0, 2)
    corner_out(0)
    arrive(0, 3)
    arrive(1, 2)
    corner_out(1)
    own_rows.wait()
    for load in loads:
        load.wait()
    share(0, sp)
    go(remote(wgu.at[:, 1 - core], mate_w, mw_sems.at[0], mw_sems.at[1], sp, mate))
    await_share(0, sp)
    forward(sp)
    corner_over(0)
    await_pieces(0, across, (1, 2, 3))
    share(0, across)
    await_share(0, across)
    forward(across)
    conv_std = mix()
    own_mixed = pltpu.make_async_copy(mixed_ref, mixed.at[sp], local_sems.at[6])
    relay(0, 3)
    arrive(1, 3)
    share(1, sp)
    await_pieces(0, along, (0, 1, 2))
    share(0, along)
    for other in others:
        for sems, landing in ((inv_recv, inv_in), (w_recv, w_in)):
            remote(
                landing.at[other], landing.at[other], inv_send.at[0], sems.at[other], sp, mate
            ).wait_recv()
    await_share(0, along)
    forward(along)
    await_share(1, sp)
    backward(sp)
    corner_over(1)
    activate(sp)
    own_mixed.start()
    inv_col = to_column(lax.rsqrt(stat_out[0:1] / width + EPSILON))
    remote(mate_w, mate_w, mw_sems.at[0], mw_sems.at[1], sp, mate).wait_recv()
    await_corner(0, (1, 3))
    share(0, corner)
    await_share(0, corner)
    forward(corner)
    relay(1, 3)
    await_pieces(1, across, (1, 2, 3))
    share(1, across)
    await_share(1, across)
    backward(across)
    activate(across)
    await_pieces(1, along, (0, 1, 2))
    share(1, along)
    spread(across, send_x.at[0], keep.at[1, 1 - col_of])
    near_out(0, 0)
    await_share(1, along)
    backward(along)
    activate(along)
    spread(sp, keep.at[0, row_of], keep.at[1, col_of])
    spread(along, keep.at[0, 1 - row_of], send_y.at[0])
    near_out(1, 0)
    await_corner(1, ())
    for step in (0, 1, 2, 3):
        place = hops[step]
        if step in (1, 3):
            await_piece(1, corner, step)
        slot = rows_u.at[corner, core, place]
        go(remote(slot, slot, last_send.at[place], last_recv.at[place], sp, mate))
        backward_piece(corner, core, place)
    store(rows_u.at[corner, core], rows_u_out.at[corner, core], rows_sems.at[1, corner, 0])
    for step in (0, 1, 2, 3):
        place = hops[step]
        slot = rows_u.at[corner, 1 - core, place]
        remote(slot, slot, last_send.at[place], last_recv.at[place], sp, mate).wait_recv()
        backward_piece(corner, 1 - core, place)
    store(rows_u.at[corner, 1 - core], rows_u_out.at[corner, 1 - core], rows_sems.at[1, corner, 1])
    activate(corner)
    spread(corner, send_x.at[1], send_y.at[1])
    rim = rim_in.shape[0]
    before = lax.rem(sp + 3, 4)
    far_out(0)
    second_turn(0)
    for side in range(2):
        near_out(side, 1)
    far_out(1)
    reduce_out(0)
    second_turn(1)
    reduce_over(0)
    reduce_in(0)
    gather_out(0)
    out_load.wait()
    fan(0, 0)
    reduce_out(1)
    fan(2, 0)
    reduce_over(1)
    fan(1, 0)
    reduce_in(1)
    fan(3, 0)
    gather_out(1)
    own_mixed.wait()
    for i, other in enumerate(others):
        go(remote(mixed_ref, mixed.at[sp], mix_send.at[i], mix_recv.at[sp], other, tp))
    norm_out(0)
    grads_in(0)
    fan(0, 1)
    fan(2, 1)
    fan(1, 1)
    fan(3, 1)
    norm_back(0)
    go(
        remote(
            conv_out.at[pl.ds(0, rim)], rim_in, rim_sems.at[0], rim_sems.at[1], before, tp
        )
    )
    norm_out(1)
    grads_in(1)
    for half in range(2):
        grads[sp, half] = full[half, sp]
    norm_back(1)
    for other in others:
        slot = mixed.at[other]
        remote(slot, slot, mix_send.at[0], mix_recv.at[other], other, tp).wait_recv()
    remote(rim_in, rim_in, rim_sems.at[0], rim_sems.at[1], before, tp).wait_recv()
    last = (sp < 3).astype(jnp.float32)
    conv_out[tokens : tokens + rim] = rim_in[...] * last
    for h in range(halves):
        for other in others:
            slot = grads.at[other, 1 - core, spans[h]]
            remote(
                slot, slot, gmate_send.at[other, h], gmate_recv.at[other, h], sp, mate
            ).wait_recv()
        for step in range(4):
            place = hops[step]
            mate_copy(place, h).wait_send()

            @pl.when(place != sp)
            def _(place=place, h=h):
                grad_copy(place, h).wait_send()

        @pl.when(edge)
        def _(h=h):
            over_copy(h).wait_send()
            full_copy(3, h).wait_send()

        @pl.when(middle)
        def _(h=h):
            r_copy(2, h).wait_send()
            full_pass(h).wait_send()

    for copy in stores:
        copy.wait()
    for copy in pending:
        copy.wait_send()
    for kind in (0, 1):

        @pl.when(edge)
        def _(kind=kind):
            z_copy(kind, sp, 3, z_send.at[kind, 2], owns[kind]).wait_send()

        @pl.when(middle)
        def _(kind=kind):
            pass_copy(kind, sp, z_send.at[kind, 2]).wait_send()
            z_copy(kind, corner, 2, c_send.at[kind, 1]).wait_send()
            pass_copy(kind, corner, c_send.at[kind, 2]).wait_send()


def finish_kernel(
    rows_s,
    rows_u,
    hidden,
    active,
    conv,
    taps,
    value_in,
    gate_in,
    grads,
    mixed,
    grad_gate,
    grad_up,
    grad_down,
    grad_out,
    value_out,
    gate_out,
):
    step = pl.program_id(0)
    tokens, part = value_in.shape
    tap_count = taps.shape[0]
    tall = all_rows(hidden[...])
    term = dot_tn(all_rows(rows_s[:, 0, 0]), tall)
    half = term.shape[1] // 2
    grad_gate[...] = term[:, :half]
    grad_up[...] = term[:, half:]
    grad_down[...] = dot_tn(all_rows(active[...]), all_rows(rows_u[:, 0, 0]))

    @pl.when(lax.rem(step, 4) == 3)
    def _():
        grad_out[...] = dot_tn(all_rows(mixed[...]), all_rows(grads[:, 0]))

    @pl.when(step == 1)
    def _():
        glu = jnp.zeros((tokens, part), jnp.float32)
        for residue in range(8):
            rolled = None
            for offset in range(residue, tap_count, 8):
                base = offset - residue
                tap = taps[tap_count - 1 - offset : tap_count - offset]
                product = tap * conv[base : base + tokens + 8]
                rolled = product if rolled is None else rolled + product
            glu = glu + rolled[residue : residue + tokens]
        sigma = 1.0 / (1.0 + jnp.exp(-gate_in[...].astype(jnp.float32)))
        value_out[...] = (glu * sigma).astype(jnp.bfloat16)
        gate_out[...] = (
            glu * value_in[...].astype(jnp.float32) * sigma * (1.0 - sigma)
        ).astype(jnp.bfloat16)


def all_rows(blocks):
    return blocks.reshape(blocks.shape[0] * blocks.shape[1], blocks.shape[2])


def fused_device(
    upstream,
    stream,
    norm_gain,
    routes,
    route_weights,
    w_gate,
    w_up,
    w_down,
    value_in,
    gate_in,
    conv_pre,
    ln_gain,
    conv_taps,
    w_out,
):
    tokens, columns = stream.shape
    tp_count = lax.axis_size("tp")
    sp_count = lax.axis_size("sp")
    chips = tp_count // 2
    width = columns * tp_count
    part = w_gate.shape[2]
    channel_part = conv_pre.shape[1]
    channels = channel_part * tp_count
    bf16, f32 = jnp.bfloat16, jnp.float32
    vmem = pl.BlockSpec(memory_space=pltpu.VMEM)
    anywhere = pl.BlockSpec(memory_space=pl.ANY)
    dma = pltpu.SemaphoreType.DMA
    shape = jax.ShapeDtypeStruct

    piece = (chips, 2, columns, part)
    rows_shape = (sp_count, 2, chips, tokens, columns)
    rim = -(-(conv_taps.shape[0] - 1) // 8) * 8
    rows_s, rows_u, hidden, active, conv_back, grads, mixed = pl.pallas_call(
        functools.partial(step_kernel, width, channels),
        out_shape=(
            shape(rows_shape, bf16),
            shape(rows_shape, bf16),
            shape((sp_count, tokens, 2 * part), bf16),
            shape((sp_count, tokens, part), bf16),
            shape((tokens + rim, channel_part), f32),
            shape((sp_count, 2, tokens, columns), bf16),
            shape((sp_count, tokens, channel_part), bf16),
        ),
        in_specs=[vmem] * 7 + [anywhere] * 4,
        out_specs=[anywhere] * 4 + [vmem] * 3,
        scratch_shapes=[
            pltpu.VMEM(rows_shape, bf16),
            pltpu.VMEM(rows_shape, bf16),
            pltpu.VMEM((sp_count, tokens, 2 * part), bf16),
            pltpu.VMEM((sp_count, tokens, part), bf16),
            pltpu.VMEM((2, 2, 2, tokens, columns), bf16),
            pltpu.VMEM((2, 2, tokens, columns), bf16),
            pltpu.VMEM((2, 2, tokens, columns), bf16),
            pltpu.VMEM((2, 2, tokens, columns), bf16),
            pltpu.VMEM((2, 2, tokens, columns), bf16),
            pltpu.VMEM((tokens, columns), bf16),
            pltpu.VMEM((8, tokens), f32),
            pltpu.VMEM((8, tokens), f32),
            pltpu.VMEM((sp_count, 8, tokens), f32),
            pltpu.VMEM((chips, 2, columns, 2 * part), bf16),
            pltpu.VMEM((part, width), bf16),
            pltpu.VMEM((chips, columns, 2 * part), bf16),
            pltpu.VMEM((sp_count, tokens, 2 * part), bf16),
            pltpu.VMEM((sp_count, tokens, 2 * part), f32),
            pltpu.VMEM((sp_count, tokens, part), f32),
            pltpu.VMEM((tp_count, 8, tokens), f32),
            pltpu.VMEM((8, tokens), f32),
            pltpu.VMEM((sp_count, 8, tokens), f32),
            pltpu.VMEM((sp_count, 8, tokens), f32),
            pltpu.VMEM(w_out.shape, bf16),
            pltpu.VMEM((tokens, channel_part), bf16),
            pltpu.VMEM((tokens, channel_part), f32),
            pltpu.VMEM((tokens, channel_part), f32),
            pltpu.VMEM((2, 2, tokens, columns), bf16),
            pltpu.VMEM((2, 2, tokens, columns), bf16),
            pltpu.VMEM((chips, 2, tokens // 2, columns), bf16),
            pltpu.VMEM((chips, 2, tokens // 2, columns), bf16),
            pltpu.VMEM((2, tokens // 2, columns), bf16),
            pltpu.VMEM((2, tokens // 2, columns), f32),
            pltpu.VMEM((tokens, columns), f32),
            pltpu.VMEM((tokens, channel_part), f32),
            pltpu.VMEM((2, 8, tokens // 2), f32),
            pltpu.VMEM((tp_count, 2, 8, tokens // 2), f32),
            pltpu.VMEM((2, 8, tokens // 2), f32),
            pltpu.VMEM((tp_count, 2, 8, tokens // 2), f32),
            pltpu.VMEM((2, chips, tokens, columns), bf16),
            pltpu.VMEM((rim, channel_part), f32),
            dma((2, 3)),
            dma((2, sp_count, chips)),
            dma((2, chips, 2)),
            dma((2, chips)),
            dma((2, sp_count)),
            dma((2, sp_count)),
            dma((chips,)),
            dma((chips,)),
            dma((2, 3)),
            dma((2, 2, 2)),
            dma((2, 2, 2)),
            dma((2, 2, 2)),
            dma((2, 2, 2)),
            dma((tp_count - 1,)),
            dma((tp_count,)),
            dma((3,)),
            dma((sp_count,)),
            dma((3,)),
            dma((sp_count,)),
            dma((2,)),
            dma((sp_count,)),
            dma((sp_count,)),
            dma((7,)),
            dma((2, sp_count, 2)),
            dma((2, sp_count)),
            dma((3,)),
            dma((sp_count,)),
            dma((2, 2, 2)),
            dma((2, 2, 2)),
            dma((chips, 2)),
            dma((chips, 2)),
            dma((2,)),
            dma((tp_count - 1, 2)),
            dma((tp_count, 2)),
            dma((tp_count - 1, 2)),
            dma((tp_count, 2)),
            dma((3, 2)),
            dma((chips, 2)),
            dma((chips, 2)),
            dma((chips, 2)),
            dma((sp_count, 2)),
            dma((sp_count, 2)),
            dma((sp_count, 2)),
            dma((sp_count, 2)),
            dma((2,)),
        ],
        compiler_params=pltpu.CompilerParams(
            collective_id=3, has_side_effects=True, vmem_limit_bytes=VMEM_LIMIT
        ),
        cost_estimate=pl.CostEstimate(
            flops=10**10, bytes_accessed=10**8, transcendentals=0
        ),
        name="routed_step",
    )(
        stream,
        upstream,
        norm_gain[None, :],
        routes.T,
        route_weights.T,
        conv_pre,
        ln_gain[None, :],
        w_gate[0].reshape(piece),
        w_up[0].reshape(piece),
        w_down[0],
        w_out,
    )

    def fixed(count):
        return lambda step: (0,) * count

    piece_spec = pl.BlockSpec(
        (sp_count, 1, 1, tokens, columns), lambda step: (0, step % 2, step // 2, 0, 0)
    )
    grad_gate, grad_up, grad_down, grad_out, value_grad, gate_grad = pl.pallas_call(
        finish_kernel,
        grid=(tp_count,),
        out_shape=(
            shape((width, part), f32),
            shape((width, part), f32),
            shape((part, width), f32),
            shape((channel_part, 2 * columns), f32),
            shape((tokens, channel_part), bf16),
            shape((tokens, channel_part), bf16),
        ),
        in_specs=[
            piece_spec,
            piece_spec,
            pl.BlockSpec(hidden.shape, fixed(3)),
            pl.BlockSpec(active.shape, fixed(3)),
            pl.BlockSpec(conv_back.shape, fixed(2)),
            pl.BlockSpec(conv_taps.shape, fixed(2)),
            pl.BlockSpec(value_in.shape, fixed(2)),
            pl.BlockSpec(gate_in.shape, fixed(2)),
            pl.BlockSpec(
                (sp_count, 1, tokens, columns), lambda step: (0, step // 4, 0, 0)
            ),
            pl.BlockSpec(mixed.shape, fixed(3)),
        ],
        out_specs=[
            pl.BlockSpec((columns, part), lambda step: (step, 0)),
            pl.BlockSpec((columns, part), lambda step: (step, 0)),
            pl.BlockSpec((part, columns), lambda step: (0, step)),
            pl.BlockSpec((channel_part, columns), lambda step: (0, step // 4)),
            pl.BlockSpec((tokens, channel_part), fixed(2)),
            pl.BlockSpec((tokens, channel_part), fixed(2)),
        ],
        compiler_params=pltpu.CompilerParams(vmem_limit_bytes=VMEM_LIMIT),
        cost_estimate=pl.CostEstimate(
            flops=6 * width * part * tokens * sp_count,
            bytes_accessed=40 * 2**20,
            transcendentals=0,
        ),
        name="finish",
    )(
        rows_s,
        rows_u,
        hidden,
        active,
        conv_back,
        conv_taps,
        value_in,
        gate_in,
        grads,
        mixed,
    )
    return (grad_gate[None], grad_up[None], grad_down[None], grad_out, value_grad, gate_grad)


def solution(mesh):
    planar = mesh.shape["sp"] == 4 and mesh.shape["tp"] == 2 * mesh.shape["sp"]
    return jax.shard_map(
        fused_device if planar else per_device,
        mesh=mesh,
        in_specs=(
            P("sp", "tp"),
            P("sp", "tp"),
            P("tp"),
            P("sp", None),
            P("sp", None),
            P("sp", None, "tp"),
            P("sp", None, "tp"),
            P("sp", "tp", None),
            P("sp", "tp"),
            P("sp", "tp"),
            P("sp", "tp"),
            P("tp"),
            P(None, "tp"),
            P("tp", None),
        ),
        out_specs=(
            P("sp", None, "tp"),
            P("sp", None, "tp"),
            P("sp", "tp", None),
            P("tp", "sp"),
            P("sp", "tp"),
            P("sp", "tp"),
        ),
        check_vma=False,
    )
```

```python
import functools

import jax
import jax.numpy as jnp
from jax import lax
from jax.experimental import pallas as pl
from jax.experimental.pallas import tpu as pltpu
from jax.sharding import PartitionSpec as P


EPSILON = 1e-06
VMEM_LIMIT = 60 * 2**20
PARTS = 4


def shifted(block, axis, distance):
    devices = range(lax.axis_size(axis))
    route = [(i - distance, i) for i in devices if i - distance in devices]
    return lax.ppermute(block, axis, route)


def group_sum_kernel(axis, group, own_ref, out_ref, landed, send_sems, recv_sems):
    me = lax.axis_index(axis)
    barrier = pltpu.get_barrier_semaphore()
    for step in range(1, group):
        pl.semaphore_signal(
            barrier,
            inc=1,
            device_id={axis: lax.rem(me + step, group)},
            device_id_type=pl.DeviceIdType.MESH,
        )
    pl.semaphore_wait(barrier, group - 1)
    copies = []
    for step in range(1, group):
        copy = pltpu.make_async_remote_copy(
            src_ref=own_ref,
            dst_ref=landed.at[step - 1],
            send_sem=send_sems.at[step - 1],
            recv_sem=recv_sems.at[step - 1],
            device_id={axis: lax.rem(me + step, group)},
            device_id_type=pl.DeviceIdType.MESH,
        )
        copy.start()
        copies.append(copy)
    for copy in copies:
        copy.wait()
    total = own_ref[...]
    for step in range(1, group):
        total = total + landed[step - 1]
    out_ref[...] = total


def group_sum(vectors, axis, collective_id):
    block = jnp.stack(vectors, axis=0)
    group = lax.axis_size(axis)
    summed = pl.pallas_call(
        functools.partial(group_sum_kernel, axis, group),
        out_shape=jax.ShapeDtypeStruct(block.shape, block.dtype),
        in_specs=[pl.BlockSpec(memory_space=pltpu.VMEM)],
        out_specs=pl.BlockSpec(memory_space=pltpu.VMEM),
        scratch_shapes=[
            pltpu.VMEM((group - 1,) + block.shape, block.dtype),
            pltpu.SemaphoreType.DMA((group - 1,)),
            pltpu.SemaphoreType.DMA((group - 1,)),
        ],
        compiler_params=pltpu.CompilerParams(
            collective_id=collective_id, has_side_effects=True
        ),
        cost_estimate=pl.CostEstimate(
            flops=group * block.size, bytes_accessed=400 * block.size * 4, transcendentals=0
        ),
        name="group_sum",
    )(block)
    return tuple(summed[row] for row in range(len(vectors)))


def silu_slope(values):
    logistic = jax.nn.sigmoid(values)
    return logistic * (1.0 + values * (1.0 - logistic))


def per_device(
    upstream,
    stream,
    norm_gain,
    routes,
    route_weights,
    w_gate,
    w_up,
    w_down,
    value_in,
    gate_in,
    conv_pre,
    ln_gain,
    conv_taps,
    w_out,
):
    tok_rows, width_part = stream.shape
    token_groups = lax.axis_size("sp")
    width_groups = lax.axis_size("tp")
    model_width = width_part * width_groups
    channels = conv_pre.shape[1] * width_groups
    tap_count = conv_taps.shape[0]
    capacity = 3 * tok_rows // token_groups
    experts = w_gate.shape[0] * token_groups
    slot_count = experts * capacity
    expert_rows = token_groups * capacity
    flat_experts = routes.reshape(-1)
    one_hot = (flat_experts[:, None] == jnp.arange(experts, dtype=jnp.int32)[None, :]).astype(
        jnp.int32
    )
    slot_rank = jnp.sum((jnp.cumsum(one_hot, axis=0) - one_hot) * one_hot, axis=1)
    slot_index = (flat_experts * capacity + slot_rank).reshape(tok_rows, 2)
    slot_ids = jnp.arange(slot_count, dtype=jnp.int32)[:, None]
    first_hit = slot_ids == slot_index[None, :, 0]
    second_hit = slot_ids == slot_index[None, :, 1]
    any_hit = jnp.logical_or(first_hit, second_hit)
    picker = any_hit.astype(jnp.bfloat16)
    slot_weight = jnp.sum(
        jnp.where(first_hit, route_weights[None, :, 0], 0.0)
        + jnp.where(second_hit, route_weights[None, :, 1], 0.0),
        axis=1,
    )
    token_iota = jnp.arange(tok_rows, dtype=jnp.int32)[None, :]
    slot_token = jnp.where(
        jnp.any(any_hit, axis=1), jnp.sum(jnp.where(any_hit, token_iota, 0), axis=1), tok_rows
    )
    columns = stream.shape[1]
    spare = jnp.zeros((1, columns), jnp.bfloat16)
    upstream_pad = jnp.concatenate([upstream, spare], axis=0)
    cotangent = (upstream_pad[slot_token].astype(jnp.float32) * slot_weight[:, None]).astype(
        jnp.bfloat16
    )
    sent_cotangent = cotangent.reshape(experts, capacity, columns)
    part_cotangent = lax.all_to_all(
        sent_cotangent, "sp", split_axis=0, concat_axis=0, tiled=True
    ).reshape(expert_rows, width_part)
    part_cotangent, stream_late, conv_late = lax.optimization_barrier(
        (part_cotangent, stream, conv_pre)
    )
    cotangent = lax.all_gather(part_cotangent, "tp", axis=1, tiled=True)
    residual = stream_late.astype(jnp.float32)
    conv_vals = conv_late.astype(jnp.float32)
    row_squares, conv_total, conv_squares = group_sum(
        (
            jnp.sum(residual * residual, axis=1),
            jnp.sum(conv_vals, axis=1),
            jnp.sum(conv_vals * conv_vals, axis=1),
        ),
        "tp",
        0,
    )
    inverse = lax.rsqrt(row_squares / model_width + EPSILON)[:, None]
    normed = (norm_gain[None, :] * residual * inverse).astype(jnp.bfloat16)
    normed_pad = jnp.concatenate([normed, spare], axis=0)
    inputs = normed_pad[slot_token]
    sent_inputs = inputs.reshape(experts, capacity, columns)
    part_inputs = lax.all_to_all(sent_inputs, "sp", split_axis=0, concat_axis=0, tiled=True)
    inputs = lax.all_gather(
        part_inputs.reshape(expert_rows, width_part), "tp", axis=1, tiled=True
    )
    gate_mat = w_gate[0]
    upper_mat = w_up[0]
    down_mat = w_down[0]
    gate_pre = jnp.dot(inputs, gate_mat, preferred_element_type=jnp.float32)
    upper_pre = jnp.dot(inputs, upper_mat, preferred_element_type=jnp.float32)
    active = (jax.nn.silu(gate_pre) * upper_pre).astype(jnp.bfloat16)
    active_back = lax.dot_general(
        cotangent, down_mat, (((1,), (1,)), ((), ())), preferred_element_type=jnp.float32
    )
    gate_back = (active_back * upper_pre * silu_slope(gate_pre)).astype(jnp.bfloat16)
    upper_back = (active_back * jax.nn.silu(gate_pre)).astype(jnp.bfloat16)
    grad_gate = lax.dot_general(
        inputs, gate_back, (((0,), (0,)), ((), ())), preferred_element_type=jnp.float32
    )
    grad_up = lax.dot_general(
        inputs, upper_back, (((0,), (0,)), ((), ())), preferred_element_type=jnp.float32
    )
    grad_down = lax.dot_general(
        active, cotangent, (((0,), (0,)), ((), ())), preferred_element_type=jnp.float32
    )
    input_part = lax.dot_general(
        gate_back, gate_mat, (((1,), (1,)), ((), ())), preferred_element_type=jnp.float32
    ) + lax.dot_general(
        upper_back, upper_mat, (((1,), (1,)), ((), ())), preferred_element_type=jnp.float32
    )
    input_back = lax.psum_scatter(
        input_part.astype(jnp.bfloat16), "tp", scatter_dimension=1, tiled=True
    )
    input_back, grad_gate, grad_up, grad_down = lax.optimization_barrier(
        (input_back, grad_gate, grad_up, grad_down)
    )
    returned = lax.all_to_all(
        input_back.reshape(token_groups, capacity, width_part),
        "sp",
        split_axis=0,
        concat_axis=0,
        tiled=True,
    )
    returned = returned.reshape(slot_count, width_part)
    token_back = lax.dot_general(
        picker, returned, (((0,), (0,)), ((), ())), preferred_element_type=jnp.float32
    )
    gained = norm_gain[None, :] * token_back
    (inner_sum,) = group_sum((jnp.sum(gained * residual, axis=1),), "tp", 1)
    norm_back = inverse * gained - residual * inverse**3 * (inner_sum / model_width)[:, None]
    stream_grad = (upstream.astype(jnp.float32) + norm_back).astype(jnp.bfloat16)
    full_grad = lax.all_gather(stream_grad, "tp", axis=1, tiled=True)
    mean_val = (conv_total / channels)[:, None]
    variance = (conv_squares / channels)[:, None] - mean_val * mean_val
    inv_std = lax.rsqrt(variance + EPSILON)
    centred = (conv_vals - mean_val) * inv_std
    scaled = centred * ln_gain[None, :]
    mixed_out = jax.nn.silu(scaled).astype(jnp.bfloat16)
    grad_rows = lax.dot_general(
        full_grad, mixed_out, (((0,), (0,)), ((), ())), preferred_element_type=jnp.float32
    ).astype(jnp.bfloat16)
    grad_out = (
        lax.psum_scatter(grad_rows, "sp", scatter_dimension=0, tiled=True).astype(jnp.float32).T
    )
    mixed_back = lax.dot_general(
        full_grad, w_out, (((1,), (1,)), ((), ())), preferred_element_type=jnp.float32
    )
    norm_in = mixed_back * silu_slope(scaled) * ln_gain[None, :]
    norm_total, norm_cross = group_sum(
        (jnp.sum(norm_in, axis=1), jnp.sum(norm_in * centred, axis=1)), "tp", 2
    )
    conv_back = inv_std * (
        norm_in - (norm_total / channels)[:, None] - centred * (norm_cross / channels)[:, None]
    )
    next_rim = shifted(conv_back[: tap_count - 1], "sp", -1)
    padded = jnp.concatenate([conv_back, next_rim], axis=0)
    glu_back = jnp.zeros(conv_back.shape, jnp.float32)
    for tap_index in range(tap_count):
        offset = tap_count - 1 - tap_index
        glu_back = glu_back + conv_taps[tap_index][None, :] * padded[offset : offset + tok_rows]
    gate_sigma = jax.nn.sigmoid(gate_in.astype(jnp.float32))
    value_grad = (glu_back * gate_sigma).astype(jnp.bfloat16)
    gate_grad = (glu_back * value_in.astype(jnp.float32) * gate_sigma * (1.0 - gate_sigma)).astype(
        jnp.bfloat16
    )
    return (grad_gate[None], grad_up[None], grad_down[None], grad_out, value_grad, gate_grad)


MESH_ID = pl.DeviceIdType.MESH


def remote(src, dst, send_sem, recv_sem, sp_index, tp_index):
    return pltpu.make_async_remote_copy(
        src_ref=src,
        dst_ref=dst,
        send_sem=send_sem,
        recv_sem=recv_sem,
        device_id={"sp": sp_index, "tp": tp_index},
        device_id_type=MESH_ID,
    )


def signal(devices):
    barrier = pltpu.get_barrier_semaphore()
    for sp_index, tp_index in devices:
        pl.semaphore_signal(
            barrier,
            inc=1,
            device_id={"sp": sp_index, "tp": tp_index},
            device_id_type=MESH_ID,
        )


def await_signals(count):
    pl.semaphore_wait(pltpu.get_barrier_semaphore(), count)


def places():
    sp = lax.axis_index("sp")
    tp = lax.axis_index("tp")
    chip, core = tp // 2, tp % 2
    side = 1 - 2 * (sp % 2)
    lift = 2 - 4 * (sp // 2)
    across, along = sp + side, sp + lift
    corner = 3 - sp
    hops = (
        chip,
        chip + 1 - 2 * (chip % 2),
        2 - chip // 2,
        3 - 3 * (chip // 2),
    )
    return sp, tp, chip, core, across, along, corner, hops


def to_column(row):
    count = row.shape[1]
    down = lax.broadcasted_iota(jnp.int32, (count, count), 0)
    over = lax.broadcasted_iota(jnp.int32, (count, count), 1)
    return jnp.sum(jnp.where(down == over, row, 0.0), axis=1, keepdims=True)


def to_row(column):
    count = column.shape[0]
    down = lax.broadcasted_iota(jnp.int32, (count, count), 0)
    over = lax.broadcasted_iota(jnp.int32, (count, count), 1)
    return jnp.sum(jnp.where(down == over, column, 0.0), axis=0, keepdims=True)


def dot_nt(left, right):
    return lax.dot_general(
        left, right, (((1,), (1,)), ((), ())), preferred_element_type=jnp.float32
    )


def dot_tn(left, right):
    return lax.dot_general(
        left, right, (((0,), (0,)), ((), ())), preferred_element_type=jnp.float32
    )


def step_kernel(
    width,
    channels,
    stream_ref,
    up_ref,
    gain_ref,
    routes_ref,
    weights_ref,
    conv_ref,
    ln_ref,
    wg_hbm,
    wu_hbm,
    wd_hbm,
    w_hbm,
    tall_out,
    wide_out,
    conv_out,
    grads,
    mixed,
    rows_s,
    rows_u,
    hidden,
    active,
    hidden_t,
    active_t,
    tall,
    wide,
    keep,
    send_x,
    send_y,
    near,
    far,
    gs_ref,
    stat_ref,
    stat_out,
    wrow_ref,
    wgu,
    wd,
    mate_w,
    mate_h,
    acc,
    back,
    stat_in,
    inv_out,
    inv_in,
    w_in,
    w_out,
    mixed_ref,
    slope_ref,
    centred_ref,
    turn_out,
    turn_in,
    z_out,
    z_in,
    over_in,
    over_sum,
    own_sum,
    mixed_back,
    note_out,
    note_in,
    tail_out,
    tail_in,
    full,
    rim_in,
    z_send,
    piece_recv,
    xy_send,
    relay_send,
    mate_send,
    mate_recv,
    last_send,
    last_recv,
    c_send,
    near_send,
    near_recv,
    far_send,
    far_recv,
    stat_send,
    stat_recv,
    inv_send,
    inv_recv,
    w_send,
    w_recv,
    mw_sems,
    mh_send,
    mh_recv,
    local_sems,
    rows_sems,
    mix_send,
    mix_recv,
    turn_send,
    turn_recv,
    r_send,
    r_recv,
    over_recv,
    note_send,
    note_recv,
    tail_send,
    tail_recv,
    full_send,
    full_recv,
    fm_send,
    fm_recv,
    grad_send,
    grad_recv,
    gmate_send,
    gmate_recv,
    rim_sems,
):
    sp, tp, chip, core, across, along, corner, hops = places()
    mate = tp + 1 - 2 * core
    tokens, columns = gs_ref.shape
    part = wd_hbm.shape[0]
    sp_count, tp_count = 4, 8
    row_of = sp // 2
    col_of = lax.rem(sp, 2)
    peers = [lax.rem(tp + step, tp_count) for step in range(1, tp_count)]
    others = (across, along, corner)
    owns = (gs_ref, up_ref)
    rows = (rows_s, rows_u)

    signal([(sp, peer) for peer in peers] + [(other, tp) for other in others])
    loads = [
        pltpu.make_async_copy(up_ref, rows_u.at[sp, core, chip], local_sems.at[3]),
        pltpu.make_async_copy(wg_hbm, wgu.at[:, :, :, pl.ds(0, part)], local_sems.at[0]),
        pltpu.make_async_copy(wu_hbm, wgu.at[:, :, :, pl.ds(part, part)], local_sems.at[1]),
        pltpu.make_async_copy(wd_hbm, wd, local_sems.at[2]),
    ]
    for load in loads:
        load.start()
    out_load = pltpu.make_async_copy(w_hbm, w_out, local_sems.at[5])
    out_load.start()
    own_rows = pltpu.make_async_copy(gs_ref, rows_s.at[sp, core, chip], local_sems.at[4])

    gain = gain_ref[...]
    squares = []
    for begin in range(0, tokens, 64):
        block = stream_ref[begin : begin + 64].astype(jnp.float32)
        gs_ref[begin : begin + 64] = (gain * block).astype(jnp.bfloat16)
        squares.append(jnp.sum(block * block, axis=1, keepdims=True))
    conv_vals = conv_ref[...].astype(jnp.float32)
    stat_ref[...] = jnp.concatenate(
        [
            to_row(jnp.concatenate(squares, axis=0)),
            to_row(jnp.sum(conv_vals, axis=1, keepdims=True)),
            to_row(jnp.sum(conv_vals * conv_vals, axis=1, keepdims=True)),
            jnp.zeros((5, tokens), jnp.float32),
        ],
        axis=0,
    )
    for expert in range(sp_count):
        row = jnp.sum(
            jnp.where(routes_ref[...] == expert, weights_ref[...], 0.0), axis=0, keepdims=True
        )
        wrow_ref[expert] = jnp.broadcast_to(row, (8, tokens))
    await_signals(len(peers) + len(others))
    own_rows.start()

    pending = []
    stores = []

    def go(copy):
        copy.start()
        pending.append(copy)

    def store(source, target, sem):
        copy = pltpu.make_async_copy(source, target, sem)
        copy.start()
        stores.append(copy)

    for i, peer in enumerate(peers):
        go(remote(stat_ref, stat_in.at[tp], stat_send.at[i], stat_recv.at[tp], sp, peer))
    for i, other in enumerate(others):
        go(remote(wrow_ref.at[other], w_in.at[sp], w_send.at[i], w_recv.at[sp], other, tp))

    def send_piece(kind, step, source, place):
        for way, target in enumerate((across, along)):
            go(
                remote(
                    source,
                    rows[kind].at[sp, core, place],
                    xy_send.at[kind, step, way],
                    piece_recv.at[kind, sp, place],
                    target,
                    tp,
                )
            )

    edge = lax.rem(chip + 1, 4) // 2 == 0
    middle = jnp.logical_not(edge)

    def z_copy(kind, origin, step, send_sem, source=None):
        slot = rows[kind].at[origin, core, chip]
        return remote(
            slot if source is None else source,
            slot,
            send_sem,
            piece_recv.at[kind, origin, chip],
            sp,
            2 * hops[step] + core,
        )

    def pass_copy(kind, origin, send_sem):
        slot = rows[kind].at[origin, core, hops[2]]
        return remote(
            slot,
            slot,
            send_sem,
            piece_recv.at[kind, origin, hops[2]],
            sp,
            2 * hops[1] + core,
        )

    for kind in (0, 1):
        for step in (1, 2):
            go(z_copy(kind, sp, step, z_send.at[kind, step - 1], owns[kind]))

        @pl.when(edge)
        def _(kind=kind):
            z_copy(kind, sp, 3, z_send.at[kind, 2], owns[kind]).start()

        send_piece(kind, 0, owns[kind], chip)

    def await_piece(kind, origin, step):
        slot = rows[kind].at[origin, core, hops[step]]
        remote(
            slot,
            slot,
            mate_send.at[kind, origin],
            piece_recv.at[kind, origin, hops[step]],
            sp,
            mate,
        ).wait_recv()

    def relay(kind, step):
        origin, target = (across, along) if step % 2 == 0 else (along, across)
        await_piece(kind, origin, step)
        slot = rows[kind].at[origin, core, hops[step]]
        go(
            remote(
                slot,
                slot,
                relay_send.at[kind, step],
                piece_recv.at[kind, origin, hops[step]],
                target,
                tp,
            )
        )

    def share(kind, origin):
        slot = rows[kind].at[origin, core]
        go(
            remote(
                slot, slot, mate_send.at[kind, origin], mate_recv.at[kind, origin], sp, mate
            )
        )

    def await_share(kind, origin):
        slot = rows[kind].at[origin, 1 - core]
        remote(
            slot, slot, mate_send.at[kind, origin], mate_recv.at[kind, origin], sp, mate
        ).wait_recv()

    acc[...] = jnp.zeros(acc.shape, jnp.float32)
    back[...] = jnp.zeros(back.shape, jnp.float32)
    w_in[sp] = wrow_ref[sp]

    total = stat_ref[...]
    for peer in peers:
        remote(
            stat_in.at[peer], stat_in.at[peer], stat_send.at[0], stat_recv.at[peer], sp, peer
        ).wait_recv()
        total = total + stat_in[peer]
    stat_out[...] = total
    halves = PARTS
    half_rows = tokens // halves
    spans = [pl.ds(h * half_rows, half_rows) for h in range(halves)]
    inverse_row = lax.rsqrt(total[0:1] / width + EPSILON)
    inv_out[...] = jnp.broadcast_to(inverse_row, inv_out.shape)
    inv_in[sp] = jnp.broadcast_to(inverse_row, inv_out.shape)
    for i, other in enumerate(others):
        go(remote(inv_out, inv_in.at[sp], inv_send.at[i], inv_recv.at[sp], other, tp))

    def forward(origin):
        def body(index, carry):
            half, place = index // 4, lax.rem(index, 4)
            acc[origin] += jnp.dot(
                rows_s[origin, half, place],
                wgu[place, half],
                preferred_element_type=jnp.float32,
            )
            return carry

        lax.fori_loop(0, tp_count, body, 0)

    def backward_piece(origin, half, place):
        start = pl.multiple_of((2 * place + half) * columns, columns)
        back[origin] += dot_nt(rows_u[origin, half, place], wd[:, pl.ds(start, columns)])

    def backward(origin):
        def body(index, carry):
            backward_piece(origin, index // 4, lax.rem(index, 4))
            return carry

        lax.fori_loop(0, tp_count, body, 0)

    chunk = 64

    def activate(origin):
        inverse = to_column(inv_in[origin, 0:1])
        weight = to_column(w_in[origin, 0:1])
        for begin in range(0, tokens, chunk):
            end = begin + chunk
            pre = acc[origin, begin:end] * inverse[begin:end]
            gate, upper = pre[:, :part], pre[:, part:]
            cot = back[origin, begin:end] * weight[begin:end]
            logistic = 1.0 / (1.0 + jnp.exp(-gate))
            silu = gate * logistic
            slope = logistic * (1.0 + gate * (1.0 - logistic))
            active[origin, begin:end] = (silu * upper * weight[begin:end]).astype(jnp.bfloat16)
            back_inv = cot * inverse[begin:end]
            hidden[origin, begin:end, :part] = (back_inv * upper * slope).astype(jnp.bfloat16)
            hidden[origin, begin:end, part:] = (back_inv * silu).astype(jnp.bfloat16)
        go(
            remote(
                hidden.at[origin],
                mate_h.at[origin],
                mh_send.at[origin],
                mh_recv.at[origin],
                sp,
                mate,
            )
        )

    def spread(origin, low, high):
        remote(
            mate_h.at[origin],
            mate_h.at[origin],
            mh_send.at[origin],
            mh_recv.at[origin],
            sp,
            mate,
        ).wait_recv()

        for target, first in ((low, 0), (high, 2)):

            def body(i, carry, target=target, first=first):
                place = first + i
                part_sum = dot_nt(hidden[origin], wgu[place, core]) + dot_nt(
                    mate_h[origin], mate_w[place]
                )
                target[i] = part_sum.astype(jnp.bfloat16)
                return carry

            lax.fori_loop(0, 2, body, 0)

    def pass_on(kind, origin, send_sem):
        @pl.when(middle)
        def _():
            pass_copy(kind, origin, send_sem).start()

    turn = lax.rem(chip + 1, 4) // 2
    orders = (
        chip,
        hops[1] + turn * (hops[2] - hops[1]),
        hops[2] + turn * (hops[1] - hops[2]),
        hops[3],
    )

    def arrive(kind, number):
        place = orders[number]
        slot = rows[kind].at[sp, core, place]
        remote(
            slot, slot, mate_send.at[kind, sp], piece_recv.at[kind, sp, place], sp, mate
        ).wait_recv()
        if number == 1:
            pass_on(kind, sp, z_send.at[kind, 2])
        send_piece(kind, number, slot, place)

    def corner_out(kind):
        await_piece(kind, corner, 0)
        go(z_copy(kind, corner, 1, c_send.at[kind, 0]))

        @pl.when(middle)
        def _():
            z_copy(kind, corner, 2, c_send.at[kind, 1]).start()

    def corner_over(kind):
        @pl.when(middle)
        def _():
            await_piece(kind, corner, 2)
            pass_copy(kind, corner, c_send.at[kind, 2]).start()

    def await_pieces(kind, origin, steps):
        for step in steps:
            await_piece(kind, origin, step)

    def await_corner(kind, steps):
        await_pieces(kind, corner, steps)

        @pl.when(edge)
        def _():
            await_piece(kind, corner, 2)

    def mix():
        sums = stat_out[...]
        mean_row = sums[1:2] / channels
        conv_std = to_column(lax.rsqrt(sums[2:3] / channels - mean_row * mean_row + EPSILON))
        mean_val = to_column(mean_row)
        ln_gain = ln_ref[...]
        for begin in range(0, tokens, 64):
            end = begin + 64
            block = (conv_ref[begin:end].astype(jnp.float32) - mean_val[begin:end]) * conv_std[
                begin:end
            ]
            scaled = block * ln_gain
            logistic = 1.0 / (1.0 + jnp.exp(-scaled))
            centred_ref[begin:end] = block
            mixed_ref[begin:end] = (scaled * logistic).astype(jnp.bfloat16)
            slope_ref[begin:end] = logistic * (1.0 + scaled * (1.0 - logistic)) * ln_gain
        return conv_std

    def turn_copy(group, h):
        return remote(
            turn_out.at[group, :, spans[h]],
            turn_in.at[group, :, spans[h]],
            turn_send.at[group, h],
            turn_recv.at[group, h],
            (along, across)[group],
            tp,
        )

    def near_copy(side, h):
        source, target = ((send_x, across), (send_y, along))[side]
        return remote(
            source.at[0, :, spans[h]],
            near.at[side, :, spans[h]],
            near_send.at[side, h],
            near_recv.at[side, h],
            target,
            tp,
        )

    def far_copy(side, h):
        source, target = ((send_x, across), (send_y, along))[side]
        return remote(
            source.at[1, :, spans[h]],
            far.at[side, :, spans[h]],
            far_send.at[side, h],
            far_recv.at[side, h],
            target,
            tp,
        )

    def turn_hidden(origin):
        span = slice(origin * tokens, (origin + 1) * tokens)
        hidden_t[:, span] = hidden[origin].T
        active_t[:, span] = active[origin].T

    def weight_grads(first, count):
        def body(piece, carry):
            half, place = lax.rem(piece, 2), piece // 2
            tall[piece] = jnp.dot(
                hidden_t[...], all_rows(rows_s[:, half, place]), preferred_element_type=jnp.float32
            ).astype(jnp.bfloat16)
            wide[piece] = jnp.dot(
                active_t[...], all_rows(rows_u[:, half, place]), preferred_element_type=jnp.float32
            ).astype(jnp.bfloat16)
            return carry

        lax.fori_loop(first, first + count, body, 0)
        for piece in range(first, first + count):
            store(tall.at[piece], tall_out.at[piece], rows_sems.at[piece, 0])
            store(wide.at[piece], wide_out.at[piece], rows_sems.at[piece, 1])

    def near_out(side, h):
        go(near_copy(side, h))

    def far_out(h):
        for side in range(2):
            go(far_copy(side, h))

    def second_turn(h):
        for group, off in ((0, 1 - row_of), (1, 1 - col_of)):
            far_copy(group, h).wait_recv()
            for i in range(2):
                turn_out[group, i, spans[h]] = (
                    keep[group, off, i, spans[h]].astype(jnp.float32)
                    + far[group, i, spans[h]].astype(jnp.float32)
                ).astype(jnp.bfloat16)
            go(turn_copy(group, h))

    def plane_in(h):
        for side in range(2):
            near_copy(side, h).wait_recv()
            turn_copy(side, h).wait_recv()

    def plane_sum(place, h):
        group, i = place // 2, lax.rem(place, 2)
        own = row_of + group * (col_of - row_of)
        return (
            keep[group, own, i, spans[h]].astype(jnp.float32)
            + near[group, i, spans[h]].astype(jnp.float32)
            + turn_in[group, i, spans[h]].astype(jnp.float32)
        )

    def r_copy(step, h):
        return remote(
            z_out.at[step, h],
            z_in.at[chip, h],
            r_send.at[step, h],
            r_recv.at[chip, h],
            sp,
            2 * hops[step] + core,
        )

    def over_copy(h):
        return remote(
            z_out.at[2, h], over_in.at[h], r_send.at[2, h], over_recv.at[h], sp, 2 * hops[1] + core
        )

    def await_z(step, h):
        slot = z_in.at[hops[step], h]
        remote(slot, slot, r_send.at[0, h], r_recv.at[hops[step], h], sp, mate).wait_recv()

    inner_rows = {}

    def reduce_out(h):
        plane_in(h)
        inner = None
        for step in (2, 3, 1, 0):
            place = hops[step]
            summed = plane_sum(place, h)
            term = jnp.sum(
                summed * rows_s[sp, core, place, spans[h]].astype(jnp.float32),
                axis=1,
                keepdims=True,
            )
            inner = term if inner is None else inner + term
            if step == 0:
                own_sum[spans[h]] = summed
            elif step == 2:
                over_sum[h] = summed
                z_out[step, h] = summed.astype(jnp.bfloat16)
            else:
                z_out[step, h] = summed.astype(jnp.bfloat16)
        row = to_row(inner)
        inner_rows[h] = row
        note_out[h] = jnp.broadcast_to(row, note_out.shape[1:])
        for i, peer in enumerate(peers):
            go(
                remote(
                    note_out.at[h], note_in.at[tp, h], note_send.at[i, h], note_recv.at[tp, h], sp, peer
                )
            )

        @pl.when(edge)
        def _():
            over_copy(h).start()

        for step in (3, 1):
            go(r_copy(step, h))

    def reduce_over(h):
        @pl.when(middle)
        def _():
            slot = over_in.at[h]
            remote(slot, slot, r_send.at[2, h], over_recv.at[h], sp, mate).wait_recv()
            z_out[2, h] = (over_sum[h] + over_in[h].astype(jnp.float32)).astype(jnp.bfloat16)
            r_copy(2, h).start()

    def reduce_in(h):
        for step in (1, 2):
            await_z(step, h)
        total = (
            own_sum[spans[h]]
            + z_in[hops[1], h].astype(jnp.float32)
            + z_in[hops[2], h].astype(jnp.float32)
        )
        own_sum[spans[h]] = total

        @pl.when(edge)
        def _():
            await_z(3, h)
            own_sum[spans[h]] += z_in[hops[3], h].astype(jnp.float32)


    def full_slot(place, h, half=None):
        return full.at[core if half is None else half, place, spans[h]]

    def full_copy(step, h):
        slot = full_slot(chip, h)
        return remote(
            slot, slot, full_send.at[step - 1, h], full_recv.at[chip, h], sp, 2 * hops[step] + core
        )

    def full_pass(h):
        slot = full_slot(hops[2], h)
        return remote(
            slot, slot, full_send.at[2, h], full_recv.at[hops[2], h], sp, 2 * hops[1] + core
        )

    def gather_out(h):
        row = inner_rows[h]
        for peer in peers:
            slot = note_in.at[peer, h]
            remote(slot, slot, note_send.at[0, h], note_recv.at[peer, h], sp, peer).wait_recv()
            row = row + note_in[peer, h, 0:1]
        scale = inv_col[h * half_rows : (h + 1) * half_rows]
        factor = scale * scale * to_column(row) / width
        full[core, chip, spans[h]] = (
            up_ref[spans[h]].astype(jnp.float32)
            + gain * own_sum[spans[h]]
            - stream_ref[spans[h]].astype(jnp.float32) * factor
        ).astype(jnp.bfloat16)
        for step in (1, 2):
            go(full_copy(step, h))

        @pl.when(edge)
        def _():
            full_copy(3, h).start()

    def mate_copy(place, h, half=None):
        slot = full_slot(place, h, half)
        return remote(slot, slot, fm_send.at[place, h], fm_recv.at[place, h], sp, mate)

    def grad_copy(place, h):
        return remote(
            full_slot(place, h),
            grads.at[sp, core, spans[h]],
            grad_send.at[place, h],
            grad_recv.at[sp, h],
            place,
            tp,
        )

    def mixed_term(half, place, h):
        start = pl.multiple_of((2 * place + half) * columns, columns)
        return dot_nt(full[half, place, spans[h]], w_out[:, pl.ds(start, columns)])

    def fan(step, h):
        place = hops[step]
        if step > 0:
            slot = full_slot(place, h)
            remote(slot, slot, full_send.at[0, h], full_recv.at[place, h], sp, mate).wait_recv()
        if step == 2:

            @pl.when(middle)
            def _():
                full_pass(h).start()

        mate_copy(place, h).start()

        @pl.when(place != sp)
        def _():
            grad_copy(place, h).start()

        term = mixed_term(core, place, h)
        if step == 0:
            mixed_back[spans[h]] = term
        else:
            mixed_back[spans[h]] += term

    tails = {}

    def norm_out(h):
        total = mixed_back[spans[h]]
        for step in range(4):
            place = hops[step]
            mate_copy(place, h, 1 - core).wait_recv()
            total = total + mixed_term(1 - core, place, h)
        norm_in = total * slope_ref[spans[h]]
        mixed_back[spans[h]] = norm_in
        sums = jnp.concatenate(
            [
                to_row(jnp.sum(norm_in, axis=1, keepdims=True)),
                to_row(jnp.sum(norm_in * centred_ref[spans[h]], axis=1, keepdims=True)),
                jnp.zeros((6, half_rows), jnp.float32),
            ],
            axis=0,
        )
        tails[h] = sums
        tail_out[h] = sums
        for i, peer in enumerate(peers):
            go(
                remote(
                    tail_out.at[h], tail_in.at[tp, h], tail_send.at[i, h], tail_recv.at[tp, h], sp, peer
                )
            )

    def norm_back(h):
        sums = tails[h]
        for peer in peers:
            slot = tail_in.at[peer, h]
            remote(slot, slot, tail_send.at[0, h], tail_recv.at[peer, h], sp, peer).wait_recv()
            sums = sums + tail_in[peer, h]
        conv_out[spans[h]] = conv_std[h * half_rows : (h + 1) * half_rows] * (
            mixed_back[spans[h]]
            - to_column(sums[0:1]) / channels
            - centred_ref[spans[h]] * (to_column(sums[1:2]) / channels)
        )

    def grads_in(h):
        for other in others:
            slot = grads.at[other, core, spans[h]]
            remote(slot, slot, grad_send.at[0, h], grad_recv.at[other, h], other, tp).wait_recv()
            go(
                remote(
                    slot, slot, gmate_send.at[other, h], gmate_recv.at[other, h], sp, mate
                )
            )

    rim = rim_in.shape[0]
    before = lax.rem(sp + 3, 4)
    arrive(0, 1)
    relay(0, 0)
    relay(1, 0)
    arrive(1, 1)
    arrive(0, 2)
    corner_out(0)
    arrive(0, 3)
    arrive(1, 2)
    corner_out(1)
    own_rows.wait()
    for load in loads:
        load.wait()
    share(0, sp)
    go(remote(wgu.at[:, 1 - core], mate_w, mw_sems.at[0], mw_sems.at[1], sp, mate))
    await_share(0, sp)
    forward(sp)
    corner_over(0)
    await_pieces(0, across, (1, 2, 3))
    share(0, across)
    await_share(0, across)
    forward(across)
    conv_std = mix()
    own_mixed = pltpu.make_async_copy(mixed_ref, mixed.at[sp], local_sems.at[6])
    relay(0, 3)
    arrive(1, 3)
    share(1, sp)
    await_pieces(0, along, (0, 1, 2))
    share(0, along)
    for other in others:
        for sems, landing in ((inv_recv, inv_in), (w_recv, w_in)):
            remote(
                landing.at[other], landing.at[other], inv_send.at[0], sems.at[other], sp, mate
            ).wait_recv()
    await_share(0, along)
    forward(along)
    await_share(1, sp)
    backward(sp)
    corner_over(1)
    activate(sp)
    own_mixed.start()
    inv_col = to_column(lax.rsqrt(stat_out[0:1] / width + EPSILON))
    remote(mate_w, mate_w, mw_sems.at[0], mw_sems.at[1], sp, mate).wait_recv()
    await_corner(0, (1, 3))
    share(0, corner)
    await_share(0, corner)
    forward(corner)
    relay(1, 3)
    await_pieces(1, across, (1, 2, 3))
    share(1, across)
    await_share(1, across)
    backward(across)
    activate(across)
    await_pieces(1, along, (0, 1, 2))
    share(1, along)
    spread(across, send_x.at[0], keep.at[1, 1 - col_of])
    for h in range(halves // 2):
        near_out(0, h)
    await_share(1, along)
    backward(along)
    activate(along)
    spread(along, keep.at[0, 1 - row_of], send_y.at[0])
    for h in range(halves // 2):
        near_out(1, h)
    spread(sp, keep.at[0, row_of], keep.at[1, col_of])
    await_corner(1, ())
    for step in (0, 1, 2, 3):
        place = hops[step]
        if step in (1, 3):
            await_piece(1, corner, step)
        slot = rows_u.at[corner, core, place]
        go(remote(slot, slot, last_send.at[place], last_recv.at[place], sp, mate))
        backward_piece(corner, core, place)
    for step in (0, 1, 2, 3):
        place = hops[step]
        slot = rows_u.at[corner, 1 - core, place]
        remote(slot, slot, last_send.at[place], last_recv.at[place], sp, mate).wait_recv()
        backward_piece(corner, 1 - core, place)
    activate(corner)
    spread(corner, send_x.at[1], send_y.at[1])
    rim = rim_in.shape[0]
    before = lax.rem(sp + 3, 4)
    far_out(0)
    far_out(1)
    for origin in range(sp_count):
        turn_hidden(origin)
    second_turn(0)
    second_turn(1)
    far_out(2)
    far_out(3)
    weight_grads(0, 2)
    reduce_out(0)
    reduce_over(0)
    second_turn(2)
    weight_grads(2, 1)
    reduce_out(1)
    reduce_in(0)
    near_out(0, 3)
    near_out(1, 3)
    near_out(0, 2)
    near_out(1, 2)
    second_turn(3)
    reduce_over(1)
    gather_out(0)
    weight_grads(3, 1)
    reduce_in(1)
    reduce_out(2)
    reduce_over(2)
    reduce_out(3)
    weight_grads(4, 1)
    reduce_in(2)
    gather_out(1)
    out_load.wait()
    fan(0, 0)
    fan(2, 0)
    fan(3, 0)
    fan(1, 0)
    gather_out(2)
    fan(0, 1)
    fan(0, 2)
    weight_grads(5, 1)
    reduce_over(3)
    fan(2, 1)
    fan(1, 1)
    norm_out(0)
    weight_grads(6, 1)
    reduce_in(3)
    gather_out(3)
    fan(3, 1)
    grads_in(0)
    weight_grads(7, 1)
    fan(2, 2)
    fan(1, 2)
    fan(0, 3)
    grads_in(1)
    own_mixed.wait()
    for i, other in enumerate(others):
        go(remote(mixed_ref, mixed.at[sp], mix_send.at[i], mix_recv.at[sp], other, tp))
    fan(3, 2)
    fan(2, 3)
    fan(1, 3)
    norm_out(1)
    norm_back(0)
    go(
        remote(
            conv_out.at[pl.ds(0, rim)], rim_in, rim_sems.at[0], rim_sems.at[1], before, tp
        )
    )
    norm_out(2)
    fan(3, 3)
    norm_out(3)
    norm_back(1)
    grads_in(2)
    grads_in(3)
    for half in range(2):
        grads[sp, half] = full[half, sp]
    norm_back(2)
    norm_back(3)
    for other in others:
        slot = mixed.at[other]
        remote(slot, slot, mix_send.at[0], mix_recv.at[other], other, tp).wait_recv()
    remote(rim_in, rim_in, rim_sems.at[0], rim_sems.at[1], before, tp).wait_recv()
    last = (sp < 3).astype(jnp.float32)
    conv_out[tokens : tokens + rim] = rim_in[...] * last
    for h in range(halves):
        for other in others:
            slot = grads.at[other, 1 - core, spans[h]]
            remote(
                slot, slot, gmate_send.at[other, h], gmate_recv.at[other, h], sp, mate
            ).wait_recv()
        for step in range(4):
            place = hops[step]
            mate_copy(place, h).wait_send()

            @pl.when(place != sp)
            def _(place=place, h=h):
                grad_copy(place, h).wait_send()

        @pl.when(edge)
        def _(h=h):
            over_copy(h).wait_send()
            full_copy(3, h).wait_send()

        @pl.when(middle)
        def _(h=h):
            r_copy(2, h).wait_send()
            full_pass(h).wait_send()

    for copy in stores:
        copy.wait()
    for copy in pending:
        copy.wait_send()
    for kind in (0, 1):

        @pl.when(edge)
        def _(kind=kind):
            z_copy(kind, sp, 3, z_send.at[kind, 2], owns[kind]).wait_send()

        @pl.when(middle)
        def _(kind=kind):
            pass_copy(kind, sp, z_send.at[kind, 2]).wait_send()
            z_copy(kind, corner, 2, c_send.at[kind, 1]).wait_send()
            pass_copy(kind, corner, c_send.at[kind, 2]).wait_send()


def finish_kernel(
    tall,
    wide,
    conv,
    taps,
    value_in,
    gate_in,
    grads,
    mixed,
    grad_gate,
    grad_up,
    grad_down,
    grad_out,
    value_out,
    gate_out,
):
    step = pl.program_id(0)
    tokens, part = value_in.shape
    tap_count = taps.shape[0]
    turned = tall[0].astype(jnp.float32)
    half = turned.shape[0] // 2
    grad_gate[...] = turned[:half].T
    grad_up[...] = turned[half:].T
    grad_down[...] = wide[0].astype(jnp.float32)

    @pl.when(lax.rem(step, 4) == 3)
    def _():
        grad_out[...] = dot_tn(all_rows(mixed[...]), all_rows(grads[:, 0]))

    @pl.when(step == 1)
    def _():
        glu = jnp.zeros((tokens, part), jnp.float32)
        for residue in range(8):
            rolled = None
            for offset in range(residue, tap_count, 8):
                base = offset - residue
                tap = taps[tap_count - 1 - offset : tap_count - offset]
                product = tap * conv[base : base + tokens + 8]
                rolled = product if rolled is None else rolled + product
            glu = glu + rolled[residue : residue + tokens]
        sigma = 1.0 / (1.0 + jnp.exp(-gate_in[...].astype(jnp.float32)))
        value_out[...] = (glu * sigma).astype(jnp.bfloat16)
        gate_out[...] = (
            glu * value_in[...].astype(jnp.float32) * sigma * (1.0 - sigma)
        ).astype(jnp.bfloat16)


def all_rows(blocks):
    return blocks.reshape(blocks.shape[0] * blocks.shape[1], blocks.shape[2])


def fused_device(
    upstream,
    stream,
    norm_gain,
    routes,
    route_weights,
    w_gate,
    w_up,
    w_down,
    value_in,
    gate_in,
    conv_pre,
    ln_gain,
    conv_taps,
    w_out,
):
    tokens, columns = stream.shape
    tp_count = lax.axis_size("tp")
    sp_count = lax.axis_size("sp")
    chips = tp_count // 2
    width = columns * tp_count
    part = w_gate.shape[2]
    channel_part = conv_pre.shape[1]
    channels = channel_part * tp_count
    bf16, f32 = jnp.bfloat16, jnp.float32
    vmem = pl.BlockSpec(memory_space=pltpu.VMEM)
    anywhere = pl.BlockSpec(memory_space=pl.ANY)
    dma = pltpu.SemaphoreType.DMA
    shape = jax.ShapeDtypeStruct

    piece = (chips, 2, columns, part)
    rows_shape = (sp_count, 2, chips, tokens, columns)
    rim = -(-(conv_taps.shape[0] - 1) // 8) * 8
    tall, wide, conv_back, grads, mixed = pl.pallas_call(
        functools.partial(step_kernel, width, channels),
        out_shape=(
            shape((tp_count, 2 * part, columns), bf16),
            shape((tp_count, part, columns), bf16),
            shape((tokens + rim, channel_part), f32),
            shape((sp_count, 2, tokens, columns), bf16),
            shape((sp_count, tokens, channel_part), bf16),
        ),
        in_specs=[vmem] * 7 + [anywhere] * 4,
        out_specs=[anywhere] * 2 + [vmem] * 3,
        scratch_shapes=[
            pltpu.VMEM(rows_shape, bf16),
            pltpu.VMEM(rows_shape, bf16),
            pltpu.VMEM((sp_count, tokens, 2 * part), bf16),
            pltpu.VMEM((sp_count, tokens, part), bf16),
            pltpu.VMEM((2 * part, sp_count * tokens), bf16),
            pltpu.VMEM((part, sp_count * tokens), bf16),
            pltpu.VMEM((tp_count, 2 * part, columns), bf16),
            pltpu.VMEM((tp_count, part, columns), bf16),
            pltpu.VMEM((2, 2, 2, tokens, columns), bf16),
            pltpu.VMEM((2, 2, tokens, columns), bf16),
            pltpu.VMEM((2, 2, tokens, columns), bf16),
            pltpu.VMEM((2, 2, tokens, columns), bf16),
            pltpu.VMEM((2, 2, tokens, columns), bf16),
            pltpu.VMEM((tokens, columns), bf16),
            pltpu.VMEM((8, tokens), f32),
            pltpu.VMEM((8, tokens), f32),
            pltpu.VMEM((sp_count, 8, tokens), f32),
            pltpu.VMEM((chips, 2, columns, 2 * part), bf16),
            pltpu.VMEM((part, width), bf16),
            pltpu.VMEM((chips, columns, 2 * part), bf16),
            pltpu.VMEM((sp_count, tokens, 2 * part), bf16),
            pltpu.VMEM((sp_count, tokens, 2 * part), f32),
            pltpu.VMEM((sp_count, tokens, part), f32),
            pltpu.VMEM((tp_count, 8, tokens), f32),
            pltpu.VMEM((8, tokens), f32),
            pltpu.VMEM((sp_count, 8, tokens), f32),
            pltpu.VMEM((sp_count, 8, tokens), f32),
            pltpu.VMEM(w_out.shape, bf16),
            pltpu.VMEM((tokens, channel_part), bf16),
            pltpu.VMEM((tokens, channel_part), f32),
            pltpu.VMEM((tokens, channel_part), f32),
            pltpu.VMEM((2, 2, tokens, columns), bf16),
            pltpu.VMEM((2, 2, tokens, columns), bf16),
            pltpu.VMEM((chips, PARTS, tokens // PARTS, columns), bf16),
            pltpu.VMEM((chips, PARTS, tokens // PARTS, columns), bf16),
            pltpu.VMEM((PARTS, tokens // PARTS, columns), bf16),
            pltpu.VMEM((PARTS, tokens // PARTS, columns), f32),
            pltpu.VMEM((tokens, columns), f32),
            pltpu.VMEM((tokens, channel_part), f32),
            pltpu.VMEM((PARTS, 8, tokens // PARTS), f32),
            pltpu.VMEM((tp_count, PARTS, 8, tokens // PARTS), f32),
            pltpu.VMEM((PARTS, 8, tokens // PARTS), f32),
            pltpu.VMEM((tp_count, PARTS, 8, tokens // PARTS), f32),
            pltpu.VMEM((2, chips, tokens, columns), bf16),
            pltpu.VMEM((rim, channel_part), f32),
            dma((2, 3)),
            dma((2, sp_count, chips)),
            dma((2, chips, 2)),
            dma((2, chips)),
            dma((2, sp_count)),
            dma((2, sp_count)),
            dma((chips,)),
            dma((chips,)),
            dma((2, 3)),
            dma((2, PARTS)),
            dma((2, PARTS)),
            dma((2, PARTS)),
            dma((2, PARTS)),
            dma((tp_count - 1,)),
            dma((tp_count,)),
            dma((3,)),
            dma((sp_count,)),
            dma((3,)),
            dma((sp_count,)),
            dma((2,)),
            dma((sp_count,)),
            dma((sp_count,)),
            dma((7,)),
            dma((tp_count, 2)),
            dma((3,)),
            dma((sp_count,)),
            dma((2, PARTS)),
            dma((2, PARTS)),
            dma((chips, PARTS)),
            dma((chips, PARTS)),
            dma((PARTS,)),
            dma((tp_count - 1, PARTS)),
            dma((tp_count, PARTS)),
            dma((tp_count - 1, PARTS)),
            dma((tp_count, PARTS)),
            dma((3, PARTS)),
            dma((chips, PARTS)),
            dma((chips, PARTS)),
            dma((chips, PARTS)),
            dma((sp_count, PARTS)),
            dma((sp_count, PARTS)),
            dma((sp_count, PARTS)),
            dma((sp_count, PARTS)),
            dma((2,)),
        ],
        compiler_params=pltpu.CompilerParams(
            collective_id=3, has_side_effects=True, vmem_limit_bytes=VMEM_LIMIT
        ),
        cost_estimate=pl.CostEstimate(
            flops=10**10, bytes_accessed=10**8, transcendentals=0
        ),
        name="routed_step",
    )(
        stream,
        upstream,
        norm_gain[None, :],
        routes.T,
        route_weights.T,
        conv_pre,
        ln_gain[None, :],
        w_gate[0].reshape(piece),
        w_up[0].reshape(piece),
        w_down[0],
        w_out,
    )

    def fixed(count):
        return lambda step: (0,) * count

    grad_gate, grad_up, grad_down, grad_out, value_grad, gate_grad = pl.pallas_call(
        finish_kernel,
        grid=(tp_count,),
        out_shape=(
            shape((width, part), f32),
            shape((width, part), f32),
            shape((part, width), f32),
            shape((channel_part, 2 * columns), f32),
            shape((tokens, channel_part), bf16),
            shape((tokens, channel_part), bf16),
        ),
        in_specs=[
            pl.BlockSpec((1, 2 * part, columns), lambda step: (step, 0, 0)),
            pl.BlockSpec((1, part, columns), lambda step: (step, 0, 0)),
            pl.BlockSpec(conv_back.shape, fixed(2)),
            pl.BlockSpec(conv_taps.shape, fixed(2)),
            pl.BlockSpec(value_in.shape, fixed(2)),
            pl.BlockSpec(gate_in.shape, fixed(2)),
            pl.BlockSpec(
                (sp_count, 1, tokens, columns), lambda step: (0, step // 4, 0, 0)
            ),
            pl.BlockSpec(mixed.shape, fixed(3)),
        ],
        out_specs=[
            pl.BlockSpec((columns, part), lambda step: (step, 0)),
            pl.BlockSpec((columns, part), lambda step: (step, 0)),
            pl.BlockSpec((part, columns), lambda step: (0, step)),
            pl.BlockSpec((channel_part, columns), lambda step: (0, step // 4)),
            pl.BlockSpec((tokens, channel_part), fixed(2)),
            pl.BlockSpec((tokens, channel_part), fixed(2)),
        ],
        compiler_params=pltpu.CompilerParams(vmem_limit_bytes=VMEM_LIMIT),
        cost_estimate=pl.CostEstimate(
            flops=6 * width * part * tokens * sp_count,
            bytes_accessed=40 * 2**20,
            transcendentals=0,
        ),
        name="finish",
    )(
        tall,
        wide,
        conv_back,
        conv_taps,
        value_in,
        gate_in,
        grads,
        mixed,
    )
    return (grad_gate[None], grad_up[None], grad_down[None], grad_out, value_grad, gate_grad)


def solution(mesh):
    planar = mesh.shape["sp"] == 4 and mesh.shape["tp"] == 2 * mesh.shape["sp"]
    return jax.shard_map(
        fused_device if planar else per_device,
        mesh=mesh,
        in_specs=(
            P("sp", "tp"),
            P("sp", "tp"),
            P("tp"),
            P("sp", None),
            P("sp", None),
            P("sp", None, "tp"),
            P("sp", None, "tp"),
            P("sp", "tp", None),
            P("sp", "tp"),
            P("sp", "tp"),
            P("sp", "tp"),
            P("tp"),
            P(None, "tp"),
            P("tp", None),
        ),
        out_specs=(
            P("sp", None, "tp"),
            P("sp", None, "tp"),
            P("sp", "tp", None),
            P("tp", "sp"),
            P("sp", "tp"),
            P("sp", "tp"),
        ),
        check_vma=False,
    )
```
